32 devices in a mesh: sp: 8 (over z, x), tp: 4 (over y, core).
Axes of the slice: x: 2, y: 2, z: 4, core: 2. Of those that a mesh axis runs over, the one named last changes fastest.
Arguments:
- residual_signal: bfloat16 [1024, 2048], P('sp', 'tp'), may hold values from -90 to 90
- lifted_signal: bfloat16 [1024, 1024], P('sp', 'tp'), may hold values from -6 to 6
- discrete_timestep: float32 [64, 1024], P('tp', 'sp'), may hold values from 0.17 to 4.2
- additional_log_fading: float32 [64, 1024], P('tp', 'sp'), may hold values from -2.1 to 0
- paired_fading: float32 [2, 32, 64], replicated, may hold values from 1.953125e-05 to 0.0625
- unpaired_fading: float32 [2, 32, 32], replicated, may hold values from 1.953125e-05 to 0.0625
- paired_twist: float32 [2, 32, 64], replicated, may hold values from -3.140625 to 3.140625
- unpaired_twist: float32 [2, 32, 32], replicated, may hold values from -3.140625 to 3.140625
- paired_latent_linears: float32 [2, 2, 2, 32, 64, 16], replicated, may hold values from -1 to 1
- unpaired_latent_linears: float32 [2, 2, 2, 32, 32, 16], replicated, may hold values from -1 to 1
- skip_coefficient: float32 [1024], replicated, may hold values from -4 to 4
- closing_norm_multiplier: float32 [1024], replicated, may hold values from 0.1 to 1.9
- emitted_linear: bfloat16 [1024, 2048], replicated, may hold values from -0.1875 to 0.1875
- leading_norm_multiplier: float32 [2048], replicated, may hold values from 0.1 to 1.9
- raising_linear: bfloat16 [2048, 8192], P('sp', 'tp'), may hold values from -0.125 to 0.125
- lowering_linear: bfloat16 [8192, 2048], P('tp', 'sp'), may hold values from -0.0625 to 0.0625
Outputs:
- layer_out: bfloat16 [1024, 2048], P('sp', 'tp')
The draws below stay inside these ranges and needn't reach their ends.
All inputs are finite; a program needn't handle non-finite values.
Results may differ from the reference program's by a relative error of at most 0.008.
Values may be sent and summed in bfloat16 or wider, within the bound.
A program may use at most 128 MiB of HBM per device.

```python
import math
import jax
import jax.numpy as jnp
from jax import lax

D = 2048
FF = 8192
MIXER_BANDS = 64
CHAN = 16
STATE_LONG = 64
STATE_SHORT = 32
NORM_W = 128
TOK_DEV = 128
SSM_W = 1024
TOKENS = 1024
N_TP = 4


def draw_residual_signal(key, part):
    keys = jax.random.split(jax.random.fold_in(key, 5), 3)
    column = 0.4 * 10.0 ** (jnp.arange(D, dtype=jnp.float32) / D)
    column = column * jax.random.uniform(keys[0], (D,), jnp.float32, 0.7, 1.4)
    base = jnp.clip(jax.random.normal(keys[1], (TOKENS, D), jnp.float32), -4.0, 4.0)
    row_scale = jnp.exp(jax.random.uniform(keys[2], (TOKENS,), jnp.float32, math.log(0.5), math.log(4.0)))
    return (base * row_scale[:, None] * column[None, :]).astype(jnp.bfloat16)


def draw_discrete_timestep(key, part):
    keys = jax.random.split(jax.random.fold_in(key, 7), 2)
    span = TOK_DEV // 2
    count = TOKENS // span
    lowest, highest, rough_low, rough_high = (0.5, 2.0, 0.5, 1.5)
    factor = jnp.exp(jax.random.uniform(keys[0], (count,), jnp.float32, math.log(lowest), math.log(highest)))
    along = jnp.repeat(factor, span)
    rough = jax.random.uniform(keys[1], (MIXER_BANDS, TOKENS), jnp.float32, rough_low, rough_high)
    return along[None, :] * rough


def draw_additional_log_fading(key, part):
    keys = jax.random.split(jax.random.fold_in(key, 9), 2)
    places = jax.random.randint(keys[0], (MIXER_BANDS, 3), 0, TOKENS)
    values = jax.random.uniform(keys[1], (MIXER_BANDS, 3), jnp.float32, math.log(0.5), math.log(0.8))
    hits = (jnp.arange(TOKENS)[None, None, :] == places[:, :, None]).astype(jnp.float32)
    return jnp.sum(hits * values[:, :, None], axis=1)


def draw_rates(key, states):
    keys = jax.random.split(key, 4)
    share = 8
    quick = jax.random.randint(keys[0], (2, MIXER_BANDS // 2), 0, 16) < share
    quick_rate = jnp.exp(jax.random.uniform(keys[1], (2, MIXER_BANDS // 2), jnp.float32, math.log(0.01), math.log(0.025)))
    slow_rate = jnp.exp(jax.random.uniform(keys[2], (2, MIXER_BANDS // 2), jnp.float32, math.log(0.02), math.log(0.12))) / TOKENS
    base = jnp.where(quick, quick_rate, slow_rate)
    spread = jnp.exp(jax.random.uniform(keys[3], (2, MIXER_BANDS // 2, states), jnp.float32, 0.0, math.log(2.5)))
    return base[:, :, None] * spread


def draw_paired_fading(key, part):
    return draw_rates(jax.random.fold_in(key, 11), STATE_LONG)


def draw_unpaired_fading(key, part):
    return draw_rates(jax.random.fold_in(key, 12), STATE_SHORT)


def level_of(key, dims, cuts, least, high):
    def one(axis_at, parts):
        heights = jax.random.uniform(jax.random.fold_in(jax.random.fold_in(key, 6), axis_at), (parts,), jnp.float32, least / len(cuts), high / len(cuts))
        return jnp.repeat(jnp.exp(heights), dims[axis_at] // parts).reshape((-1,) + (1,) * (len(dims) - axis_at - 1))

    level = one(*cuts[0])
    for cut in cuts[1:]:
        level = level * one(*cut)
    return level


def scatter_about(stream_key, shape, deviation, most, cuts=(), kind=jnp.bfloat16):
    drawn = jax.random.normal(stream_key, shape, jnp.float32) * deviation
    if len(cuts) > 0:
        drawn = level_of(stream_key, shape, cuts, -0.22, 0.18) * drawn
    return jnp.clip(drawn, min=-most, max=most).astype(kind)


def setup_inputs(seed: int = 0) -> dict:
    seeds = jax.random.split(jax.random.key(seed), 17)
    residual_signal = draw_residual_signal(jax.random.fold_in(seeds[16], 71), 0)
    lifted_signal = scatter_about(seeds[1], (TOKENS, SSM_W), 1.0, 6.0, ((0, 8), (1, 4)))
    discrete_timestep = draw_discrete_timestep(jax.random.fold_in(seeds[16], 71), 0)
    additional_log_fading = draw_additional_log_fading(jax.random.fold_in(seeds[16], 71), 0)
    paired_fading = draw_paired_fading(jax.random.fold_in(seeds[16], 71), 0)
    unpaired_fading = draw_unpaired_fading(jax.random.fold_in(seeds[16], 71), 0)
    paired_twist = jnp.clip(jax.random.uniform(seeds[6], (2, MIXER_BANDS // 2, STATE_LONG), jnp.float32, -3.140625, 3.140625), -3.140625, 3.140625)
    unpaired_twist = jnp.clip(jax.random.uniform(seeds[7], (2, MIXER_BANDS // 2, STATE_SHORT), jnp.float32, -3.140625, 3.140625), -3.140625, 3.140625)
    paired_latent_linears = scatter_about(seeds[8], (2, 2, 2, MIXER_BANDS // 2, STATE_LONG, CHAN), (2 * CHAN) ** -0.5, 1.0, (), jnp.float32)
    unpaired_latent_linears = scatter_about(seeds[9], (2, 2, 2, MIXER_BANDS // 2, STATE_SHORT, CHAN), (2 * CHAN) ** -0.5, 1.0, (), jnp.float32)
    skip_coefficient = scatter_about(seeds[10], (SSM_W,), 1.0, 4.0, (), jnp.float32)
    closing_norm_multiplier = jnp.clip(1.0 + 0.18 * jax.random.normal(seeds[11], (SSM_W,), jnp.float32), 0.1, 1.9)
    emitted_linear = scatter_about(seeds[12], (SSM_W, D), SSM_W ** -0.5, 0.1875)
    leading_norm_multiplier = jnp.clip(1.0 + 0.18 * jax.random.normal(seeds[13], (D,), jnp.float32), 0.1, 1.9)
    raising_linear = scatter_about(seeds[14], (D, FF), D ** -0.5, 0.125, ((0, 8), (1, 4)))
    lowering_linear = scatter_about(seeds[15], (FF, D), FF ** -0.5, 0.0625, ((0, 4), (1, 8)))
    return {"residual_signal": residual_signal, "lifted_signal": lifted_signal, "discrete_timestep": discrete_timestep, "additional_log_fading": additional_log_fading, "paired_fading": paired_fading, "unpaired_fading": unpaired_fading, "paired_twist": paired_twist, "unpaired_twist": unpaired_twist, "paired_latent_linears": paired_latent_linears, "unpaired_latent_linears": unpaired_latent_linears, "skip_coefficient": skip_coefficient, "closing_norm_multiplier": closing_norm_multiplier, "emitted_linear": emitted_linear, "leading_norm_multiplier": leading_norm_multiplier, "raising_linear": raising_linear, "lowering_linear": lowering_linear}


EPSILON = 1e-06

def combine_maps(early, later):
    first_re, first_im, base_re, base_im = early
    next_re, next_im, add_re, add_im = later
    return (next_re * first_re - next_im * first_im, next_re * first_im + next_im * first_re, next_re * base_re - next_im * base_im + add_re, next_re * base_im + next_im * base_re + add_im)

def step_maps(group_inputs, pace, surge_entries, decay_rate, turn_rate, input_re, input_im):
    scaled = pace[:, :, None]
    magnitude = jnp.exp(-decay_rate[None] * scaled + surge_entries[:, :, None])
    angle = turn_rate[None] * scaled
    weight_in = jnp.sqrt(-jnp.expm1(-2.0 * decay_rate[None] * scaled))
    drive_re = jnp.einsum('ngj,gpj->ngp', group_inputs, input_re, precision=lax.Precision.HIGHEST) * weight_in
    drive_im = jnp.einsum('ngj,gpj->ngp', group_inputs, input_im, precision=lax.Precision.HIGHEST) * weight_in
    return (magnitude * jnp.cos(angle), magnitude * jnp.sin(angle), drive_re, drive_im)

def readout(state_re, state_im, read_re, read_im):
    return jnp.einsum('ngp,gpj->ngj', state_re, read_re, precision=lax.Precision.HIGHEST) - jnp.einsum('ngp,gpj->ngj', state_im, read_im, precision=lax.Precision.HIGHEST)

def kind_output(group_inputs, pace, surge_entries, decay_rate, turn_rate, projection):
    batch_number = group_inputs.shape[0]
    count = batch_number // TOK_DEV
    width = group_inputs.shape[1]
    states = decay_rate.shape[-1]
    input_blocks = group_inputs.reshape(count, TOK_DEV, width, CHAN)
    pace_blocks = pace.reshape(count, TOK_DEV, width)
    jolt_blocks = surge_entries.reshape(count, TOK_DEV, width)
    result = jnp.zeros((count, TOK_DEV, width, CHAN), jnp.float32)
    for direction in range(2):
        backward = direction == 1
        edge = 0 if backward else -1

        def each_block(carry, pieces, direction=direction, backward=backward, edge=edge):
            block_inputs, block_pace, block_jolts = pieces
            maps = step_maps(block_inputs, block_pace, block_jolts, decay_rate[direction], turn_rate[direction], projection[direction, 0, 0], projection[direction, 0, 1])
            prefix_re, prefix_im, state_re, state_im = lax.associative_scan(combine_maps, maps, reverse=backward, axis=0)
            carry_re, carry_im = carry
            state_re = state_re + prefix_re * carry_re[None] - prefix_im * carry_im[None]
            state_im = state_im + prefix_re * carry_im[None] + prefix_im * carry_re[None]
            values = readout(state_re, state_im, projection[direction, 1, 0], projection[direction, 1, 1])
            return ((state_re[edge], state_im[edge]), values)
        start = (jnp.zeros((width, states), jnp.float32), jnp.zeros((width, states), jnp.float32))
        _, values = lax.scan(each_block, start, (input_blocks, pace_blocks, jolt_blocks), reverse=backward)
        result = result + values
    return result.reshape(batch_number, width, CHAN)

def reference(residual_signal, lifted_signal, discrete_timestep, additional_log_fading, paired_fading, unpaired_fading, paired_twist, unpaired_twist, paired_latent_linears, unpaired_latent_linears, skip_coefficient, closing_norm_multiplier, emitted_linear, leading_norm_multiplier, raising_linear, lowering_linear):
    batch_number = residual_signal.shape[0]
    grouped = lifted_signal.astype(jnp.float32).reshape(batch_number, MIXER_BANDS // 2, 2, CHAN)
    pace = discrete_timestep.T.reshape(batch_number, MIXER_BANDS // 2, 2)
    surge_entries = additional_log_fading.T.reshape(batch_number, MIXER_BANDS // 2, 2)
    long_out = kind_output(grouped[:, :, 0], pace[:, :, 0], surge_entries[:, :, 0], paired_fading, paired_twist, paired_latent_linears)
    short_out = kind_output(grouped[:, :, 1], pace[:, :, 1], surge_entries[:, :, 1], unpaired_fading, unpaired_twist, unpaired_latent_linears)
    ssm_out = jnp.stack([long_out, short_out], axis=2).reshape(batch_number, SSM_W)
    activated = jax.nn.gelu(ssm_out + skip_coefficient[None] * grouped.reshape(batch_number, SSM_W))
    heads = activated.reshape(batch_number, SSM_W // NORM_W, NORM_W)
    heads = heads * lax.rsqrt(lax.optimization_barrier(jnp.mean(heads * heads, axis=2, keepdims=True)) + EPSILON)
    combined_result = (heads.reshape(batch_number, SSM_W) * closing_norm_multiplier[None]).astype(jnp.bfloat16)
    inner_activity = residual_signal.astype(jnp.float32) + jnp.dot(combined_result, emitted_linear, preferred_element_type=jnp.float32)
    scale = lax.rsqrt(lax.optimization_barrier(jnp.mean(inner_activity * inner_activity, axis=1, keepdims=True)) + EPSILON)
    normed = (inner_activity * scale * leading_norm_multiplier[None]).astype(jnp.bfloat16)
    block_width = FF // N_TP
    feed = jnp.zeros((batch_number, D), jnp.float32)
    for member in range(N_TP):
        upward = jnp.dot(normed, raising_linear[:, member * block_width:(member + 1) * block_width], preferred_element_type=jnp.float32)
        hidden = jnp.square(jax.nn.relu(upward)).astype(jnp.bfloat16)
        product = jnp.dot(hidden, lowering_linear[member * block_width:(member + 1) * block_width], preferred_element_type=jnp.float32).astype(jnp.bfloat16)
        feed = feed + product.astype(jnp.float32)
    return (inner_activity + feed).astype(jnp.bfloat16)
```

```python
import functools

import jax
import jax.numpy as jnp
from jax import lax
from jax.experimental import pallas as pl
from jax.experimental.pallas import tpu as pltpu
from jax.sharding import PartitionSpec as P

CHAN = 16
NORM_W = 128
EPSILON = 1e-06
SUB = 8
F32, BF16 = jnp.float32, jnp.bfloat16


def sincos(a):
    k = jnp.floor(a * 0.6366197723675814 + 0.5)
    r = a - k * 1.5703125
    r = r - k * 4.8351287841796875e-4
    r = r - k * 3.138556210e-7
    z = r * r
    s = r + r * z * (-1.6666654611e-1 + z * (8.3321608736e-3 + z * -1.9515295891e-4))
    c = 1.0 - 0.5 * z + z * z * (
        4.166664568298827e-2 + z * (-1.388731625493765e-3 + z * 2.443315711809948e-5)
    )
    half = jnp.floor(k * 0.5)
    odd = (k - 2.0 * half) > 0.5
    half_odd = (half - 2.0 * jnp.floor(half * 0.5)) > 0.5
    cos_v = jnp.where(odd, -s, c)
    sin_v = jnp.where(odd, c, s)
    return jnp.where(half_odd, -cos_v, cos_v), jnp.where(half_odd, -sin_v, sin_v)


def one_minus_exp_neg(u):
    t = jnp.full_like(u, 1.0)
    for m in range(10, 1, -1):
        t = 1.0 - u * (1.0 / m) * t
    return u * t


def cmul(ar, ai, br, bi):
    return ar * br - ai * bi, ar * bi + ai * br


def mixer_body(cfg, x_ref, dt_ref, lf_ref, long_rate, short_rate, long_freq, short_freq,
               skip_ref, gain_ref, resid_ref, lead_ref, long_hbm, short_hbm, emit_hbm, up_hbm, down_hbm,
               out_ref, lin_l, lin_s, lin_sem,
               pace, surge, pre, st, blk, ends, ends_all, cin, mg, rows_in, mrg, emit, resid_in,
               mid_out, wup, wdn, nrm, hid, part, rs_in, fin, fin_in,
               copy_sem, s_ends, r_ends, s_rows, r_rows, s_res, r_res,
               s_u1, r_u1, s_d1, r_d1, s_u2, r_u2, s_d2, r_d2, s_u3, r_u3, s_d3, r_d3,
               s_nrm, r_nrm, s_rs, r_rs, s_fin, r_fin):
    nsp, ntp, n, S, W, G, PL, PS, D, c_ff, F = cfg
    M = ntp // 2
    L = n // SUB
    half = G // 2
    SL = half * PL
    sp = lax.axis_index("sp")
    tp = lax.axis_index("tp")
    q = n // ntp
    Dl = D // ntp
    MESH = pl.DeviceIdType.MESH

    emit_copy = pltpu.make_async_copy(emit_hbm, emit, copy_sem.at[0])
    lin_copies = []
    for at in range(8):
        for kind, (src, dst) in enumerate(((long_hbm, lin_l), (short_hbm, lin_s))):
            lin_copies.append(pltpu.make_async_copy(
                src.at[at // 4, at // 2 % 2, at % 2, pl.ds(tp * half, half)], dst.at[at],
                lin_sem.at[kind, at]))
    for copy in lin_copies:
        copy.start()
    emit_copy.start()
    chunk = lax.rem(sp, c_ff)
    partner = tp + 1 - 2 * lax.rem(tp, 2)

    def cols(of):
        return pl.ds(pl.multiple_of(of * F, 128), F)

    own_up = pltpu.make_async_copy(up_hbm.at[:, cols(chunk)], wup.at[tp, sp], copy_sem.at[1])
    own_down = pltpu.make_async_copy(down_hbm.at[cols(chunk), :], wdn.at[tp, sp], copy_sem.at[2])
    own_up.start()
    own_down.start()

    def spread_copy(k, up):
        to = lax.rem(sp + k, nsp)
        src = up_hbm.at[:, cols(lax.rem(to, c_ff))] if up else down_hbm.at[cols(lax.rem(to, c_ff)), :]
        return pltpu.make_async_remote_copy(
            src_ref=src, dst_ref=(wup if up else wdn).at[tp, sp],
            send_sem=(s_u1 if up else s_d1).at[k - 1], recv_sem=(r_u1 if up else r_d1).at[k - 1],
            device_id=(to, tp), device_id_type=MESH)

    def across_copy(m, k, up):
        piece = (wup if up else wdn).at[tp, lax.rem(sp - k + nsp, nsp)]
        return pltpu.make_async_remote_copy(
            src_ref=piece, dst_ref=piece,
            send_sem=(s_u2 if up else s_d2).at[m - 1, k], recv_sem=(r_u2 if up else r_d2).at[m - 1, k],
            device_id=(sp, lax.rem(tp + 2 * m, ntp)), device_id_type=MESH)

    def pair_copy(m, up):
        piece = (wup if up else wdn).at[lax.rem(tp + 2 * m, ntp)]
        return pltpu.make_async_remote_copy(
            src_ref=piece, dst_ref=piece,
            send_sem=(s_u3 if up else s_d3).at[m], recv_sem=(r_u3 if up else r_d3).at[m],
            device_id=(sp, partner), device_id_type=MESH)

    def pass_on(first, last, up):
        for k in range(first, last):
            if k == 0:
                (own_up if up else own_down).wait()
            else:
                spread_copy(k, up).wait_recv()
            for m in range(1, M):
                across_copy(m, k, up).start()

    barrier = pltpu.get_barrier_semaphore()
    for k in range(1, nsp):
        pl.semaphore_signal(barrier, inc=1, device_id=(lax.rem(sp + k, nsp), tp), device_id_type=MESH)
    for k in range(1, ntp):
        pl.semaphore_signal(barrier, inc=1, device_id=(sp, lax.rem(tp + k, ntp)), device_id_type=MESH)
    pl.semaphore_wait(barrier, nsp + ntp - 2)

    def res_copy(k):
        to = lax.rem(tp + k, ntp)
        return pltpu.make_async_remote_copy(
            src_ref=resid_ref.at[pl.ds(to * q, q), :], dst_ref=resid_in.at[k - 1],
            send_sem=s_res.at[k - 1], recv_sem=r_res.at[k - 1],
            device_id=(sp, to), device_id_type=MESH)

    for k in range(1, nsp):
        spread_copy(k, True).start()
    for k in range(1, ntp):
        res_copy(k).start()

    lane = lax.broadcasted_iota(jnp.int32, (G, S), 1)
    group = jnp.where(lane < SL, 2 * (lane // PL), 2 * ((lane - SL) // PS) + 1)
    spread = (group == lax.broadcasted_iota(jnp.int32, (G, S), 0)).astype(F32)
    r = lax.broadcasted_iota(jnp.int32, (n, n), 0)
    t = lax.broadcasted_iota(jnp.int32, (n, n), 1)
    mix = (t == (r % SUB) * L + r // SUB).astype(F32)

    def per_state(ref):
        moved = lax.dot_general(ref[...], mix, (((1,), (1,)), ((), ())),
                                precision=lax.Precision.HIGHEST, preferred_element_type=F32)
        return lax.dot_general(moved, spread, (((0,), (0,)), ((), ())),
                               precision=lax.Precision.HIGHEST, preferred_element_type=F32)

    pace[...] = per_state(dt_ref)
    surge[...] = per_state(lf_ref)

    def flat_kind(ref, e):
        many, states = ref.shape[1:]
        width = half * states
        repeat = (lax.broadcasted_iota(jnp.int32, (states, width), 1) % states
                  == lax.broadcasted_iota(jnp.int32, (states, width), 0)).astype(F32)
        wide = jnp.dot(ref[e], repeat, precision=lax.Precision.HIGHEST, preferred_element_type=F32)
        owner = tp * half + lax.broadcasted_iota(jnp.int32, (many, width), 1) // states
        mine = owner == lax.broadcasted_iota(jnp.int32, (many, width), 0)
        return jnp.sum(jnp.where(mine, wide, 0.0), axis=0, keepdims=True)

    def flat(long_ref, short_ref, e):
        return jnp.concatenate([flat_kind(long_ref, e), flat_kind(short_ref, e)], axis=1)

    def widened(ref, index, states, sign):
        rows, width = half * CHAN, half * states
        repeat = (lax.broadcasted_iota(jnp.int32, (states, width), 1) % states
                  == lax.broadcasted_iota(jnp.int32, (states, width), 0)).astype(BF16)
        wide = jnp.dot(ref[index].reshape(rows, states).astype(BF16), repeat, preferred_element_type=F32)
        own_block = (lax.broadcasted_iota(jnp.int32, (rows, width), 0) // CHAN
                     == lax.broadcasted_iota(jnp.int32, (rows, width), 1) // states)
        return jnp.where(own_block, sign * wide, 0.0).astype(BF16)

    def block_map(index, sign=1.0):
        long_part = widened(lin_l, index, PL, sign)
        short_part = widened(lin_s, index, PS, sign)
        no_long, no_short = jnp.zeros((CHAN, SL), BF16), jnp.zeros((CHAN, S - SL), BF16)
        bands = []
        for g in range(half):
            band = slice(g * CHAN, (g + 1) * CHAN)
            bands.append(jnp.concatenate([long_part[band], no_short], axis=1))
            bands.append(jnp.concatenate([no_long, short_part[band]], axis=1))
        return jnp.concatenate(bands, axis=0)

    xv = jnp.dot(mix.astype(BF16), x_ref[...], preferred_element_type=F32).astype(BF16)
    for copy in lin_copies:
        copy.wait()
    for e in range(2):
        for c in range(2):
            st[:, pl.ds((2 * e + c) * S, S)] = jnp.dot(
                xv, block_map(4 * e + c), preferred_element_type=F32)

    for e in range(2):
        rate = flat(long_rate, short_rate, e)
        freq = flat(long_freq, short_freq, e)

        def step(i, carry):
            pr, pi, sr, si = carry
            at = i if e == 0 else L - 1 - i
            rows = pl.ds(pl.multiple_of(at * SUB, SUB), SUB)
            d = pace[rows, :]
            rd = rate * d
            m = jnp.exp(surge[rows, :] - rd)
            cos_v, sin_v = sincos(freq * d)
            w = jnp.sqrt(one_minus_exp_neg(2.0 * rd))
            ar, ai = m * cos_v, m * sin_v
            pr, pi = cmul(ar, ai, pr, pi)
            sr, si = cmul(ar, ai, sr, si)
            sr = sr + w * st[rows, pl.ds(2 * e * S, S)]
            si = si + w * st[rows, pl.ds((2 * e + 1) * S, S)]
            pre[rows, pl.ds(2 * e * S, S)] = pr
            pre[rows, pl.ds((2 * e + 1) * S, S)] = pi
            st[rows, pl.ds(2 * e * S, S)] = sr
            st[rows, pl.ds((2 * e + 1) * S, S)] = si
            return pr, pi, sr, si

        zero = jnp.zeros((SUB, S), F32)
        total = lax.fori_loop(0, L, step, (zero + 1.0, zero, zero, zero))
        for c in range(4):
            blk[4 * e + c] = total[c]
        order = range(SUB) if e == 0 else range(SUB - 1, -1, -1)
        run = None
        for b in order:
            now = tuple(blk[4 * e + c, b : b + 1, :] for c in range(4))
            if run is None:
                run = now
            else:
                p = cmul(now[0], now[1], run[0], run[1])
                s = cmul(now[0], now[1], run[2], run[3])
                run = (p[0], p[1], s[0] + now[2], s[1] + now[3])
        for c in range(4):
            ends[4 * e + c : 4 * e + c + 1, :] = run[c]

    def ends_copy(k):
        return pltpu.make_async_remote_copy(
            src_ref=ends, dst_ref=ends_all.at[k - 1],
            send_sem=s_ends.at[k - 1], recv_sem=r_ends.at[k - 1],
            device_id=(lax.rem(sp + k, nsp), tp), device_id_type=MESH)

    for k in range(1, nsp):
        ends_copy(k).start()
    for k in range(1, nsp):
        spread_copy(k, False).start()

    read = jnp.concatenate(
        [block_map(2), block_map(3, -1.0), block_map(6), block_map(7, -1.0)], axis=1)

    pass_on(0, nsp // 2, True)
    for k in range(1, nsp):
        ends_copy(k).wait_recv()
    blank = jnp.zeros((1, S), F32)

    def fold(j, carry, e):
        cr, ci = carry
        k = nsp - 1 - j if e == 0 else j + 1
        reached = k <= sp if e == 0 else nsp - k <= nsp - 1 - sp
        got = ends_all[k - 1]
        nr, ni = cmul(got[4 * e : 4 * e + 1], got[4 * e + 1 : 4 * e + 2], cr, ci)
        nr = nr + got[4 * e + 2 : 4 * e + 3]
        ni = ni + got[4 * e + 3 : 4 * e + 4]
        return jnp.where(reached, nr, cr), jnp.where(reached, ni, ci)

    for e in range(2):
        cr, ci = lax.fori_loop(0, nsp - 1, functools.partial(fold, e=e), (blank, blank))
        order = range(SUB) if e == 0 else range(SUB - 1, -1, -1)
        for b in order:
            cin[2 * e, b : b + 1, :] = cr
            cin[2 * e + 1, b : b + 1, :] = ci
            now = tuple(blk[4 * e + c, b : b + 1, :] for c in range(4))
            nr, ni = cmul(now[0], now[1], cr, ci)
            cr, ci = nr + now[2], ni + now[3]

        inr, ini = cin[2 * e], cin[2 * e + 1]

        def settle(i, _):
            rows = pl.ds(pl.multiple_of(i * SUB, SUB), SUB)
            re, im = pl.ds(2 * e * S, S), pl.ds((2 * e + 1) * S, S)
            ar, ai = cmul(pre[rows, re], pre[rows, im], inr, ini)
            st[rows, re] = st[rows, re] + ar
            st[rows, im] = st[rows, im] + ai
            return 0

        lax.fori_loop(0, L, settle, 0)

    y = lax.dot_general(st[...].astype(BF16), read, (((1,), (1,)), ((), ())),
                        preferred_element_type=F32)
    own = pl.ds(pl.multiple_of(tp * W, 128), W)
    skip_row, gain_row = skip_ref[:, own], gain_ref[:, own]
    y = y + skip_row * xv.astype(F32)
    y = 0.5 * y * (1.0 + jnp.tanh(0.7978845608028654 * (y + 0.044715 * y * y * y)))
    heads = []
    for h in range(W // NORM_W):
        head = y[:, h * NORM_W : (h + 1) * NORM_W]
        scale = lax.rsqrt(jnp.mean(head * head, axis=1, keepdims=True) + EPSILON)
        heads.append(head * scale * gain_row[:, h * NORM_W : (h + 1) * NORM_W])
    merged = jnp.concatenate(heads, axis=1).astype(BF16)
    t = lax.broadcasted_iota(jnp.int32, (n, n), 0)
    r = lax.broadcasted_iota(jnp.int32, (n, n), 1)
    unmix = (r == (t % L) * SUB + t // L).astype(BF16)
    mg[...] = jnp.dot(unmix, merged, preferred_element_type=F32).astype(BF16).reshape(ntp, q, W)

    def row_copy(k):
        to = lax.rem(tp + k, ntp)
        return pltpu.make_async_remote_copy(
            src_ref=mg.at[to], dst_ref=rows_in.at[k - 1],
            send_sem=s_rows.at[k - 1], recv_sem=r_rows.at[k - 1],
            device_id=(sp, to), device_id_type=MESH)

    for k in range(1, ntp):
        row_copy(k).start()
    pass_on(nsp // 2, nsp, True)
    emit_copy.wait()
    mrg[:, pl.ds(pl.multiple_of(tp * W, 128), W)] = mg[tp]
    mid_out[:, pl.ds(pl.multiple_of(tp * Dl, 128), Dl)] = resid_ref[pl.ds(pl.multiple_of(tp * q, q), q), :].astype(F32)
    for k in range(1, ntp):
        src = lax.rem(tp - k + ntp, ntp)
        res_copy(k).wait_recv()
        mid_out[:, pl.ds(pl.multiple_of(src * Dl, 128), Dl)] = resid_in[k - 1].astype(F32)
        row_copy(k).wait_recv()
        mrg[:, pl.ds(pl.multiple_of(src * W, 128), W)] = rows_in[k - 1]
    mid = mid_out[...] + jnp.dot(mrg[...], emit[...], preferred_element_type=F32)
    mid_out[...] = mid
    scale = lax.rsqrt(jnp.mean(mid * mid, axis=1, keepdims=True) + EPSILON)
    base, q_all = sp - chunk, c_ff * q
    nrm[chunk] = (mid * scale * lead_ref[...]).astype(BF16)

    def peer(k):
        return lax.rem(chunk + k, c_ff)

    H = c_ff // 2

    def nrm_across(m):
        return pltpu.make_async_remote_copy(
            src_ref=nrm.at[chunk], dst_ref=nrm.at[chunk],
            send_sem=s_nrm.at[0, m], recv_sem=r_nrm.at[0, m],
            device_id=(base + peer(2 * m), tp), device_id_type=MESH)

    def nrm_pair(m):
        return pltpu.make_async_remote_copy(
            src_ref=nrm.at[peer(2 * m)], dst_ref=nrm.at[peer(2 * m)],
            send_sem=s_nrm.at[1, m], recv_sem=r_nrm.at[1, m],
            device_id=(base + chunk + 1 - 2 * lax.rem(chunk, 2), tp), device_id_type=MESH)

    def rs_copy(k):
        return pltpu.make_async_remote_copy(
            src_ref=part.at[peer(k)], dst_ref=rs_in.at[k - 1],
            send_sem=s_rs.at[k - 1], recv_sem=r_rs.at[k - 1],
            device_id=(base + peer(k), tp), device_id_type=MESH)

    def fin_copy(k):
        to = lax.rem(tp + k, ntp)
        return pltpu.make_async_remote_copy(
            src_ref=fin.at[to], dst_ref=fin_in.at[k - 1],
            send_sem=s_fin.at[k - 1], recv_sem=r_fin.at[k - 1],
            device_id=(sp, to), device_id_type=MESH)

    for m in range(1, H):
        nrm_across(m).start()
    nrm_pair(0).start()
    pair_copy(0, True).start()
    pass_on(0, nsp, False)
    pair_copy(0, False).start()
    for m in range(1, H):
        nrm_across(m).wait_recv()
        nrm_pair(H - m).start()
    for up in (True, False):
        for m in range(1, M):
            for k in range(nsp):
                across_copy(m, k, up).wait_recv()
            pair_copy(M - m, up).start()
        if up:
            for m in range(M):
                pair_copy(m, True).wait_recv()
            for m in range(H):
                nrm_pair(m).wait_recv()
            rows = nrm[...].reshape(q_all, D)

            def raise_step(t, _):
                upward = jnp.dot(rows, wup[t].reshape(D, F), preferred_element_type=F32)
                hid[t] = jnp.square(jnp.maximum(upward, 0.0)).astype(BF16)
                return 0

            lax.fori_loop(0, ntp, raise_step, 0)
    for m in range(M):
        pair_copy(m, False).wait_recv()
    Dc = D // nsp
    for j in range(nsp):
        total = jnp.dot(hid[0], wdn[0, j], preferred_element_type=F32)
        for t in range(1, ntp):
            total = total + jnp.dot(hid[t], wdn[t, j], preferred_element_type=F32)
        part[:, :, j * Dc : (j + 1) * Dc] = total.astype(BF16).reshape(c_ff, q, Dc)
    for k in range(1, c_ff):
        rs_copy(k).start()
    result = mid_out[...] + part[chunk].astype(F32)
    for k in range(1, c_ff):
        rs_copy(k).wait_recv()
        result = result + rs_in[k - 1].astype(F32)
    result = result.astype(BF16)
    for t in range(ntp):
        fin[t] = result[:, t * Dl : (t + 1) * Dl]
    for k in range(1, ntp):
        fin_copy(k).start()
    out_ref[pl.ds(pl.multiple_of(tp * q, q), q), :] = fin[tp]
    for k in range(1, ntp):
        fin_copy(k).wait_recv()
        src = lax.rem(tp - k + ntp, ntp)
        out_ref[pl.ds(pl.multiple_of(src * q, q), q), :] = fin_in[k - 1]
    for k in range(1, c_ff):
        rs_copy(k).wait_send()
    for m in range(H):
        if m > 0:
            nrm_across(m).wait_send()
        nrm_pair(m).wait_send()
    for k in range(1, ntp):
        fin_copy(k).wait_send()
    for up in (True, False):
        for k in range(1, nsp):
            spread_copy(k, up).wait_send()
        for m in range(1, M):
            for k in range(nsp):
                across_copy(m, k, up).wait_send()
        for m in range(M):
            pair_copy(m, up).wait_send()
    for k in range(1, nsp):
        ends_copy(k).wait_send()
    for k in range(1, ntp):
        res_copy(k).wait_send()
        row_copy(k).wait_send()


def mesh_split(nsp, ntp):
    Y = ntp // 2
    X = Y if Y > 0 and nsp % Y == 0 else 1
    return nsp // X, X, Y


def paired_body(cfg, x_ref, dt_ref, lf_ref, long_rate, short_rate, long_freq, short_freq,
                skip_ref, gain_ref, resid_ref, lead_ref, long_hbm, short_hbm, emit_hbm, up_hbm, down_hbm,
                out_ref, lin_l, lin_s, lin_sem,
                pace, surge, pre, st, blk, ends, ends_all, cin, mg, rows_in, mrg, emit, resid_in,
                mid_out, wup, wdn, nrm, hid, loc, a_out, a_in, b_out, b_in, c_out, c_in, fin, fin_in,
                copy_sem, own_sem, s_ends, r_ends, s_rows, r_rows, s_res, r_res,
                s_z, r_z, s_x, r_x, s_d, r_d, s_t, r_t, s_y, r_y,
                s_a, r_a, s_b, r_b, s_c, r_c, s_fin, r_fin):
    nsp, ntp, n, S, W, G, PL, PS, D, Fz = cfg
    Z, X, Y = mesh_split(nsp, ntp)
    L = n // SUB
    half = G // 2
    SL = half * PL
    sp = lax.axis_index("sp")
    tp = lax.axis_index("tp")
    q = n // ntp
    Dl = D // ntp
    Dh = D // nsp // 2
    Rh = D // nsp // 2
    MESH = pl.DeviceIdType.MESH
    z, x, y, c = sp // X, lax.rem(sp, X), tp // 2, lax.rem(tp, 2)
    side = z // 2
    half_in, half_out = 1 + side, 3 * side
    far_in, far_out = 2 - side, 3 - 3 * side
    far0 = 2 - 2 * side
    mate = z + 1 - 2 * lax.rem(z, 2)
    inner, outer = z == half_in, z == half_out
    kinds = (z, mate, far_in, far_out)
    as_seen = 2 + jnp.where(outer, 1, 0)

    def dev(z_, x_, y_, c_):
        return (z_ * X + x_, y_ * 2 + c_)

    x_mate, y_mate, c_mate = dev(z, 1 - x, y, c), dev(z, x, 1 - y, c), dev(z, x, y, 1 - c)

    def remote(src, dst, ssem, rsem, to):
        return pltpu.make_async_remote_copy(src_ref=src, dst_ref=dst, send_sem=ssem, recv_sem=rsem,
                                            device_id=to, device_id_type=MESH)

    emit_copy = pltpu.make_async_copy(emit_hbm, emit, copy_sem.at[0])
    lin_copies = []
    for at in range(8):
        for kind, (src, dst) in enumerate(((long_hbm, lin_l), (short_hbm, lin_s))):
            lin_copies.append(pltpu.make_async_copy(
                src.at[at // 4, at // 2 % 2, at % 2, pl.ds(tp * half, half)], dst.at[at],
                lin_sem.at[kind, at]))

    def bank(up):
        return wup if up else wdn

    def shard(up, h, to):
        part = pl.ds(pl.multiple_of(to * Fz, 128), Fz)
        if up:
            return up_hbm.at[pl.ds(h * Rh, Rh), part]
        return down_hbm.at[part, pl.ds(h * Dh, Dh)]

    def own_copy(up, h):
        return pltpu.make_async_copy(shard(up, h, z), bank(up).at[c, sp, h], own_sem.at[1 - up, h])

    def z_copy(up, h, k):
        to = kinds[k]
        return remote(shard(up, h, to), bank(up).at[c, sp, h], s_z.at[1 - up, h, k],
                      r_z.at[1 - up, h, 1 if k == 1 else as_seen], dev(to, x, y, c))

    def z_wait(up, h, k):
        piece = bank(up).at[c, kinds[k] * X + x, h]
        remote(piece, piece, s_z.at[1 - up, h, k], r_z.at[1 - up, h, k], x_mate).wait_recv()

    def x_copy(up, h, k):
        piece = bank(up).at[c, kinds[k] * X + x, h]
        return remote(shard(up, h, z) if k == 0 else piece, piece,
                      s_x.at[1 - up, h, k], r_x.at[1 - up, h, k], x_mate)

    def d_copy(up, h, k, other):
        piece = bank(up).at[c, kinds[k] * X + (1 - x if other else x), h]
        return remote(shard(up, h, z) if k == 0 and not other else piece, piece,
                      s_d.at[1 - up, h, k, other], r_d.at[1 - up, h, k, other], c_mate)

    def hop1(up, h, k):
        z_wait(up, h, k)
        x_copy(up, h, k).start()
        d_copy(up, h, k, 0).start()

    def hop2(up, h, k):
        x_copy(up, h, k).wait_recv()
        d_copy(up, h, k, 1).start()

    def hop3(up, h, k):
        d_copy(up, h, k, 0).wait_recv()
        d_copy(up, h, k, 1).wait_recv()

    def res_copy(k):
        to = lax.rem(tp + k, ntp)
        return remote(resid_ref.at[pl.ds(to * q, q), :], resid_in.at[k - 1], s_res.at[k - 1], r_res.at[k - 1],
                      (sp, to))

    barrier = pltpu.get_barrier_semaphore()
    for k in range(1, nsp):
        pl.semaphore_signal(barrier, inc=1, device_id=(lax.rem(sp + k, nsp), tp), device_id_type=MESH)
    for k in range(1, ntp):
        pl.semaphore_signal(barrier, inc=1, device_id=(sp, lax.rem(tp + k, ntp)), device_id_type=MESH)
    for copy in lin_copies:
        copy.start()
    emit_copy.start()
    for up in (1, 0):
        for h in range(2):
            own_copy(up, h).start()

    lane = lax.broadcasted_iota(jnp.int32, (G, S), 1)
    group = jnp.where(lane < SL, 2 * (lane // PL), 2 * ((lane - SL) // PS) + 1)
    spread = (group == lax.broadcasted_iota(jnp.int32, (G, S), 0)).astype(F32)
    r = lax.broadcasted_iota(jnp.int32, (n, n), 0)
    t = lax.broadcasted_iota(jnp.int32, (n, n), 1)
    mix = (t == (r % SUB) * L + r // SUB).astype(F32)

    def per_state(ref):
        moved = lax.dot_general(ref[...], mix, (((1,), (1,)), ((), ())),
                                precision=lax.Precision.HIGHEST, preferred_element_type=F32)
        return lax.dot_general(moved, spread, (((0,), (0,)), ((), ())),
                               precision=lax.Precision.HIGHEST, preferred_element_type=F32)

    pace[...] = per_state(dt_ref)
    surge[...] = per_state(lf_ref)

    pl.semaphore_wait(barrier, nsp + ntp - 2)

    @pl.when(inner)
    def _():
        for k in (2, 3):
            z_copy(1, 0, k).start()

    for h in range(2):
        z_copy(1, h, 1).start()
        x_copy(1, h, 0).start()
        d_copy(1, h, 0, 0).start()
    for k in range(1, ntp):
        res_copy(k).start()

    def flat_kind(ref, e):
        many, states = ref.shape[1:]
        width = half * states
        repeat = (lax.broadcasted_iota(jnp.int32, (states, width), 1) % states
                  == lax.broadcasted_iota(jnp.int32, (states, width), 0)).astype(F32)
        wide = jnp.dot(ref[e], repeat, precision=lax.Precision.HIGHEST, preferred_element_type=F32)
        owner = tp * half + lax.broadcasted_iota(jnp.int32, (many, width), 1) // states
        mine = owner == lax.broadcasted_iota(jnp.int32, (many, width), 0)
        return jnp.sum(jnp.where(mine, wide, 0.0), axis=0, keepdims=True)

    def flat(long_ref, short_ref, e):
        return jnp.concatenate([flat_kind(long_ref, e), flat_kind(short_ref, e)], axis=1)

    def widened(ref, index, states, sign):
        rows, width = half * CHAN, half * states
        repeat = (lax.broadcasted_iota(jnp.int32, (states, width), 1) % states
                  == lax.broadcasted_iota(jnp.int32, (states, width), 0)).astype(BF16)
        wide = jnp.dot(ref[index].reshape(rows, states).astype(BF16), repeat, preferred_element_type=F32)
        own_block = (lax.broadcasted_iota(jnp.int32, (rows, width), 0) // CHAN
                     == lax.broadcasted_iota(jnp.int32, (rows, width), 1) // states)
        return jnp.where(own_block, sign * wide, 0.0).astype(BF16)

    def block_map(index, sign=1.0):
        long_part = widened(lin_l, index, PL, sign)
        short_part = widened(lin_s, index, PS, sign)
        no_long, no_short = jnp.zeros((CHAN, SL), BF16), jnp.zeros((CHAN, S - SL), BF16)
        bands = []
        for g in range(half):
            band = slice(g * CHAN, (g + 1) * CHAN)
            bands.append(jnp.concatenate([long_part[band], no_short], axis=1))
            bands.append(jnp.concatenate([no_long, short_part[band]], axis=1))
        return jnp.concatenate(bands, axis=0)

    xv = jnp.dot(mix.astype(BF16), x_ref[...], preferred_element_type=F32).astype(BF16)
    for copy in lin_copies:
        copy.wait()
    for e in range(2):
        for part in range(2):
            st[:, pl.ds((2 * e + part) * S, S)] = jnp.dot(
                xv, block_map(4 * e + part), preferred_element_type=F32)

    for e in range(2):
        rate = flat(long_rate, short_rate, e)
        freq = flat(long_freq, short_freq, e)

        def step(i, carry):
            pr, pi, sr, si = carry
            at = i if e == 0 else L - 1 - i
            rows = pl.ds(pl.multiple_of(at * SUB, SUB), SUB)
            d = pace[rows, :]
            rd = rate * d
            m = jnp.exp(surge[rows, :] - rd)
            cos_v, sin_v = sincos(freq * d)
            w = jnp.sqrt(one_minus_exp_neg(2.0 * rd))
            ar, ai = m * cos_v, m * sin_v
            pr, pi = cmul(ar, ai, pr, pi)
            sr, si = cmul(ar, ai, sr, si)
            sr = sr + w * st[rows, pl.ds(2 * e * S, S)]
            si = si + w * st[rows, pl.ds((2 * e + 1) * S, S)]
            pre[rows, pl.ds(2 * e * S, S)] = pr
            pre[rows, pl.ds((2 * e + 1) * S, S)] = pi
            st[rows, pl.ds(2 * e * S, S)] = sr
            st[rows, pl.ds((2 * e + 1) * S, S)] = si
            return pr, pi, sr, si

        zero = jnp.zeros((SUB, S), F32)
        total = lax.fori_loop(0, L, step, (zero + 1.0, zero, zero, zero))
        for part in range(4):
            blk[4 * e + part] = total[part]
        order = range(SUB) if e == 0 else range(SUB - 1, -1, -1)
        run = None
        for b in order:
            now = tuple(blk[4 * e + part, b : b + 1, :] for part in range(4))
            if run is None:
                run = now
            else:
                p = cmul(now[0], now[1], run[0], run[1])
                s = cmul(now[0], now[1], run[2], run[3])
                run = (p[0], p[1], s[0] + now[2], s[1] + now[3])
        for part in range(4):
            ends[e, part : part + 1, :] = run[part]

    def ends_copy(e, k):
        return remote(ends.at[e], ends_all.at[e, k - 1], s_ends.at[e, k - 1], r_ends.at[e, k - 1],
                      (sp + k if e == 0 else sp - k, tp))

    def has_after(e, k):
        return sp + k < nsp if e == 0 else sp >= k

    def has_before(e, k):
        return has_after(1 - e, k)

    def ends_do(e, k, send, act):
        @pl.when(has_after(e, k) if send else has_before(e, k))
        def _():
            act(ends_copy(e, k))

    for k in range(1, nsp):
        for e in range(2):
            ends_do(e, k, True, lambda copy: copy.start())

    @pl.when(inner)
    def _():
        for k in (2, 3):
            z_copy(1, 1, k).start()

    @pl.when(outer)
    def _():
        for k in (2, 3):
            z_copy(1, 0, k).start()

    read = jnp.concatenate(
        [block_map(2), block_map(3, -1.0), block_map(6), block_map(7, -1.0)], axis=1)

    for h in range(2):
        hop1(1, h, 1)
    for h in range(2):
        hop2(1, h, 0)
    hop1(1, 0, 2)

    @pl.when(inner)
    def _():
        for h in range(2):
            z_copy(0, h, 1).start()

    for h in range(2):
        x_copy(0, h, 0).start()
        d_copy(0, h, 0, 0).start()
    for k in range(nsp - 1, 0, -1):
        for e in range(2):
            ends_do(e, k, False, lambda copy: copy.wait_recv())
    blank = jnp.zeros((1, S), F32)

    def fold(j, carry, e):
        cr, ci = carry
        k = nsp - 1 - j
        got = ends_all[e, k - 1]
        nr, ni = cmul(got[0:1], got[1:2], cr, ci)
        reached = has_before(e, k)
        return jnp.where(reached, nr + got[2:3], cr), jnp.where(reached, ni + got[3:4], ci)

    for e in range(2):
        cr, ci = lax.fori_loop(0, nsp - 1, functools.partial(fold, e=e), (blank, blank))
        order = range(SUB) if e == 0 else range(SUB - 1, -1, -1)
        for b in order:
            cin[2 * e, b : b + 1, :] = cr
            cin[2 * e + 1, b : b + 1, :] = ci
            now = tuple(blk[4 * e + part, b : b + 1, :] for part in range(4))
            nr, ni = cmul(now[0], now[1], cr, ci)
            cr, ci = nr + now[2], ni + now[3]

        inr, ini = cin[2 * e], cin[2 * e + 1]

        def settle(i, _):
            rows = pl.ds(pl.multiple_of(i * SUB, SUB), SUB)
            re, im = pl.ds(2 * e * S, S), pl.ds((2 * e + 1) * S, S)
            ar, ai = cmul(pre[rows, re], pre[rows, im], inr, ini)
            st[rows, re] = st[rows, re] + ar
            st[rows, im] = st[rows, im] + ai
            return 0

        lax.fori_loop(0, L, settle, 0)

    v = lax.dot_general(st[...].astype(BF16), read, (((1,), (1,)), ((), ())),
                        preferred_element_type=F32)
    own = pl.ds(pl.multiple_of(tp * W, 128), W)
    skip_row, gain_row = skip_ref[:, own], gain_ref[:, own]
    v = v + skip_row * xv.astype(F32)
    v = 0.5 * v * (1.0 + jnp.tanh(0.7978845608028654 * (v + 0.044715 * v * v * v)))
    heads = []
    for h in range(W // NORM_W):
        head = v[:, h * NORM_W : (h + 1) * NORM_W]
        scale = lax.rsqrt(jnp.mean(head * head, axis=1, keepdims=True) + EPSILON)
        heads.append(head * scale * gain_row[:, h * NORM_W : (h + 1) * NORM_W])
    merged = jnp.concatenate(heads, axis=1).astype(BF16)
    t = lax.broadcasted_iota(jnp.int32, (n, n), 0)
    r = lax.broadcasted_iota(jnp.int32, (n, n), 1)
    unmix = (r == (t % L) * SUB + t // L).astype(BF16)
    mg[...] = jnp.dot(unmix, merged, preferred_element_type=F32).astype(BF16).reshape(ntp, q, W)

    def row_copy(k):
        to = lax.rem(tp + k, ntp)
        return remote(mg.at[to], rows_in.at[k - 1], s_rows.at[k - 1], r_rows.at[k - 1], (sp, to))

    for k in range(1, ntp):
        row_copy(k).start()
    emit_copy.wait()
    mrg[:, pl.ds(pl.multiple_of(tp * W, 128), W)] = mg[tp]
    mid_out[:, pl.ds(pl.multiple_of(tp * Dl, 128), Dl)] = resid_ref[pl.ds(pl.multiple_of(tp * q, q), q), :].astype(F32)
    for k in range(1, ntp):
        src = lax.rem(tp - k + ntp, ntp)
        res_copy(k).wait_recv()
        mid_out[:, pl.ds(pl.multiple_of(src * Dl, 128), Dl)] = resid_in[k - 1].astype(F32)
        row_copy(k).wait_recv()
        mrg[:, pl.ds(pl.multiple_of(src * W, 128), W)] = rows_in[k - 1]
    mid = mid_out[...] + jnp.dot(mrg[...], emit[...], preferred_element_type=F32)
    mid_out[...] = mid
    scale = lax.rsqrt(jnp.mean(mid * mid, axis=1, keepdims=True) + EPSILON)
    nrm[0, z] = (mid * scale * lead_ref[...]).astype(BF16)

    def t_far():
        return remote(nrm.at[0, z], nrm.at[0, z], s_t.at[0], r_t.at[as_seen], dev(far_in, x, y, c))

    def t_mate(k):
        block = nrm.at[0, kinds[k]]
        return remote(block, block, s_t.at[max(k, 1)], r_t.at[max(k, 1)], dev(mate, x, y, c))

    def t_wait(k):
        t_mate(k).wait_recv()

    def y_copy(k):
        return remote(nrm.at[0, kinds[k]], nrm.at[1, kinds[k]], s_y.at[k], r_y.at[k], y_mate)

    t_far().start()
    t_mate(0).start()
    y_copy(0).start()

    @pl.when(outer)
    def _():
        for k in (2, 3):
            z_copy(1, 1, k).start()
        for h in range(2):
            z_copy(0, h, 1).start()

    for h in range(2):
        hop2(1, h, 1)
    hop2(1, 0, 2)
    hop1(1, 1, 2)
    hop1(1, 0, 3)
    t_wait(1)
    y_copy(1).start()

    @pl.when(outer)
    def _():
        for h in range(2):
            hop1(0, h, 1)

    for h in range(2):
        hop2(0, h, 0)
    hop2(1, 1, 2)
    for k in (2, 3):
        t_wait(k)

        @pl.when(inner)
        def _():
            t_mate(k).start()

        y_copy(k).start()

    @pl.when(inner)
    def _():
        z_copy(0, 0, 3).start()

    @pl.when(outer)
    def _():
        for h in range(2):
            for k in (2, 3):
                z_copy(0, h, k).start()

    hop2(1, 0, 3)
    hop1(1, 1, 3)

    @pl.when(inner)
    def _():
        z_copy(0, 0, 2).start()
        for k in (2, 3):
            z_copy(0, 1, k).start()

    hop2(1, 1, 3)
    for k in range(4):
        y_copy(k).wait_recv()
    for h in range(2):
        own_copy(1, h).wait()
        for k in range(4):
            hop3(1, h, k)
    rows = nrm[...].reshape(2 * Z * q, D)
    for b in range(2):
        upward = jnp.dot(rows, wup[b].reshape(D, Fz), preferred_element_type=F32)
        hid[b] = jnp.square(jnp.maximum(upward, 0.0)).astype(BF16)

    def cols(zs, x_, h):
        return pl.ds(pl.multiple_of((zs * X + x_) * 2 * Dh + h * Dh, 128), Dh)

    def a_copy(zs, h):
        g = zs * 2 + h
        return remote(a_out.at[g], a_in.at[g], s_a.at[g], r_a.at[g], y_mate)

    def b_copy(zs, h):
        g = zs * 2 + h
        return remote(b_out.at[g, mate], b_in.at[g, mate], s_b.at[0, g], r_b.at[0, g], dev(mate, x, y, c))

    def b_far(zs, h):
        g = zs * 2 + h
        blocks = pl.ds(far0, 2)
        return remote(b_out.at[g, blocks], b_in.at[g, blocks], s_b.at[1, g], r_b.at[1, g], dev(mate, x, y, c))

    def c_copy(zs, h, i):
        g = zs * 2 + h
        return remote(c_out.at[g, i], c_in.at[g], s_c.at[i, g], r_c.at[g], dev(far0 + i, x, y, c))

    def stage_a(zs, h):
        g = zs * 2 + h
        for x_ in range(X):
            total = jnp.dot(hid[0], wdn[0, zs * X + x_, h], preferred_element_type=F32)
            total = total + jnp.dot(hid[1], wdn[1, zs * X + x_, h], preferred_element_type=F32)
            total = total.reshape(2, Z, q, Dh)
            a_out[g, :, x_] = total[1].astype(BF16)
            loc[g, :, x_] = total[0]
        a_copy(zs, h).start()

    def stage_b(zs, h):
        g = zs * 2 + h
        a_copy(zs, h).wait_recv()
        total = loc[g] + a_in[g].astype(F32)
        loc[g] = total
        b_out[g] = total.astype(BF16)

        @pl.when(outer)
        def _():
            b_far(zs, h).start()

        b_copy(zs, h).start()

    def stage_c(zs, h):
        g = zs * 2 + h

        @pl.when(inner)
        def _():
            b_far(zs, h).wait_recv()
            blocks = pl.ds(far0, 2)
            c_out[g] = (loc[g, blocks] + b_in[g, blocks].astype(F32)).astype(BF16)
            for i in range(2):
                c_copy(zs, h, i).start()

        b_copy(zs, h).wait_recv()
        own_sum = loc[g, z] + b_in[g, z].astype(F32)
        for x_ in range(X):
            mid_out[:, cols(zs, x_, h)] = mid_out[:, cols(zs, x_, h)] + own_sum[x_]

    def stage_d(zs, h):
        g = zs * 2 + h
        c_copy(zs, h, 0).wait_recv()
        for x_ in range(X):
            mid_out[:, cols(zs, x_, h)] = mid_out[:, cols(zs, x_, h)] + c_in[g, x_].astype(F32)

    def fin_copy(to, at):
        return remote(fin.at[to], fin_in.at[at], s_fin.at[to], r_fin.at[at], (sp, to))

    def stage_e(zs):
        fin[zs] = mid_out[:, pl.ds(pl.multiple_of(zs * Dl, 128), Dl)].astype(BF16)

        @pl.when(zs != tp)
        def _():
            fin_copy(zs, tp).start()

    for h in range(2):
        own_copy(0, h).wait()
        hop3(0, h, 0)

    @pl.when(outer)
    def _():
        for h in range(2):
            hop2(0, h, 1)
            hop3(0, h, 1)

    def mate_hops(hop):
        @pl.when(inner)
        def _():
            for h in range(2):
                hop(0, h, 1)

    turns = [(half_in, 0), (half_in, 1), (far_in, 0), (half_out, 0), (half_out, 1),
             (far_in, 1), (far_out, 0), (far_out, 1)]
    stage_a(*turns[0])
    hop1(0, 0, 2)
    stage_a(*turns[1])
    mate_hops(hop1)
    stage_b(*turns[0])
    stage_b(*turns[1])
    hop2(0, 0, 2)
    hop1(0, 1, 2)
    mate_hops(hop2)
    hop3(0, 0, 2)
    stage_a(*turns[2])
    stage_c(*turns[0])
    stage_c(*turns[1])
    mate_hops(hop3)
    stage_a(*turns[3])
    stage_b(*turns[2])
    hop1(0, 0, 3)
    stage_a(*turns[4])
    stage_b(*turns[3])
    hop2(0, 1, 2)
    hop3(0, 1, 2)
    stage_a(*turns[5])
    stage_b(*turns[4])
    stage_c(*turns[2])
    stage_c(*turns[3])
    hop2(0, 0, 3)
    hop1(0, 1, 3)
    hop3(0, 0, 3)
    stage_a(*turns[6])
    stage_b(*turns[5])
    stage_c(*turns[4])
    stage_b(*turns[6])
    stage_c(*turns[5])
    hop2(0, 1, 3)
    hop3(0, 1, 3)
    stage_a(*turns[7])
    stage_c(*turns[6])
    stage_b(*turns[7])
    stage_c(*turns[7])
    for k, zs in enumerate((half_in, half_out, far_in, far_out)):
        for h in range(2):
            stage_d(zs, h)
        stage_e(zs)
    out_ref[pl.ds(pl.multiple_of(tp * q, q), q), :] = fin[tp]
    for k in range(1, ntp):
        src = lax.rem(tp + k, ntp)
        fin_copy(src, src).wait_recv()
        out_ref[pl.ds(pl.multiple_of(src * q, q), q), :] = fin_in[src]

    for up in (1, 0):
        for h in range(2):
            for k in range(4):
                if k > 0:
                    z_copy(up, h, k).wait_send()
                x_copy(up, h, k).wait_send()
                for other in range(2):
                    d_copy(up, h, k, other).wait_send()
    for e in range(2):
        for k in range(1, nsp):
            ends_do(e, k, True, lambda copy: copy.wait_send())
    t_far().wait_send()
    t_mate(0).wait_send()

    @pl.when(inner)
    def _():
        for k in (2, 3):
            t_mate(k).wait_send()

    for k in range(4):
        y_copy(k).wait_send()
    for zs in range(Z):
        for h in range(2):
            a_copy(zs, h).wait_send()
            b_copy(zs, h).wait_send()

            @pl.when(outer)
            def _():
                b_far(zs, h).wait_send()

            @pl.when(inner)
            def _():
                for i in range(2):
                    c_copy(zs, h, i).wait_send()

        @pl.when(zs != tp)
        def _():
            fin_copy(zs, tp).wait_send()
    for k in range(1, ntp):
        res_copy(k).wait_send()
        row_copy(k).wait_send()


def paired_call(nsp, ntp, residual, lifted, dts, long_rate, short_rate, emitted, raising):
    n, W = lifted.shape
    G = dts.shape[0]
    half = G // 2
    PL, PS = long_rate.shape[2], short_rate.shape[2]
    S = half * (PL + PS)
    D = emitted.shape[1]
    Dl = residual.shape[1]
    q = n // ntp
    Z, X, Y = mesh_split(nsp, ntp)
    Fz = raising.shape[1] // Z
    Dh = D // nsp // 2
    groups = 2 * Z
    cfg = (nsp, ntp, n, S, W, G, PL, PS, D, Fz)
    vm = pl.BlockSpec(memory_space=pltpu.VMEM)
    dma = pltpu.SemaphoreType.DMA
    return pl.pallas_call(
        functools.partial(paired_body, cfg),
        out_shape=jax.ShapeDtypeStruct((n, Dl), BF16),
        in_specs=[vm] * 11 + [pl.BlockSpec(memory_space=pl.ANY)] * 5,
        out_specs=vm,
        scratch_shapes=[
            pltpu.VMEM((8, half, CHAN, PL), F32), pltpu.VMEM((8, half, CHAN, PS), F32), dma((2, 8)),
            pltpu.VMEM((n, S), F32), pltpu.VMEM((n, S), F32),
            pltpu.VMEM((n, 4 * S), F32), pltpu.VMEM((n, 4 * S), F32),
            pltpu.VMEM((8, SUB, S), F32), pltpu.VMEM((2, 4, S), F32), pltpu.VMEM((2, nsp - 1, 4, S), F32),
            pltpu.VMEM((4, SUB, S), F32),
            pltpu.VMEM((ntp, q, W), BF16), pltpu.VMEM((ntp - 1, q, W), BF16),
            pltpu.VMEM((q, ntp * W), BF16), pltpu.VMEM(emitted.shape, BF16),
            pltpu.VMEM((ntp - 1, q, Dl), BF16),
            pltpu.VMEM((q, D), F32),
            pltpu.VMEM((2, nsp, 2, D // nsp // 2, Fz), BF16), pltpu.VMEM((2, nsp, 2, Fz, Dh), BF16),
            pltpu.VMEM((2, Z, q, D), BF16), pltpu.VMEM((2, 2 * Z * q, Fz), BF16),
            pltpu.VMEM((groups, Z, X, q, Dh), F32),
            *[pltpu.VMEM((groups, Z, X, q, Dh), BF16)] * 4,
            pltpu.VMEM((groups, 2, X, q, Dh), BF16), pltpu.VMEM((groups, X, q, Dh), BF16),
            pltpu.VMEM((ntp, q, Dl), BF16), pltpu.VMEM((ntp, q, Dl), BF16),
            dma((1,)), dma((2, 2)), *[dma((2, nsp - 1))] * 2, *[dma((ntp - 1,))] * 4,
            *[dma((2, 2, 4))] * 4, *[dma((2, 2, 4, 2))] * 2, *[dma((4,))] * 4,
            *[dma((groups,))] * 2, *[dma((2, groups))] * 2, dma((2, groups)), dma((groups,)),
            *[dma((ntp,))] * 2,
        ],
        compiler_params=pltpu.CompilerParams(collective_id=0, has_side_effects=True),
        cost_estimate=pl.CostEstimate(flops=10**9, bytes_accessed=3 * 10**7, transcendentals=10**6),
    )


def on_device(residual, lifted, dts, fades, long_rate, short_rate, long_freq, short_freq,
              long_lin, short_lin, skip, closing, emitted, leading, raising, lowering):
    nsp, ntp = lax.axis_size("sp"), lax.axis_size("tp")
    operands = (lifted, dts, fades, long_rate, short_rate, long_freq, short_freq, skip[None], closing[None],
                residual, leading[None], long_lin.swapaxes(4, 5), short_lin.swapaxes(4, 5), emitted, raising, lowering)
    Z, X, Y = mesh_split(nsp, ntp)
    if X == 2 and Y == 2 and Z == ntp:
        return paired_call(nsp, ntp, residual, lifted, dts, long_rate, short_rate, emitted, raising)(*operands)
    n, W = lifted.shape
    G = dts.shape[0]
    half = G // 2
    PL, PS = long_rate.shape[2], short_rate.shape[2]
    S = half * (PL + PS)
    D = emitted.shape[1]
    Dl = residual.shape[1]
    q = n // ntp
    c_ff = min(nsp, raising.shape[1] // 128)
    F = raising.shape[1] // c_ff
    q_all, M = c_ff * q, ntp // 2
    cfg = (nsp, ntp, n, S, W, G, PL, PS, D, c_ff, F)
    vm = pl.BlockSpec(memory_space=pltpu.VMEM)
    dma = pltpu.SemaphoreType.DMA
    return pl.pallas_call(
        functools.partial(mixer_body, cfg),
        out_shape=jax.ShapeDtypeStruct((n, Dl), BF16),
        in_specs=[vm] * 11 + [pl.BlockSpec(memory_space=pl.ANY)] * 5,
        out_specs=vm,
        scratch_shapes=[
            pltpu.VMEM((8, half, CHAN, PL), F32), pltpu.VMEM((8, half, CHAN, PS), F32), dma((2, 8)),
            pltpu.VMEM((n, S), F32), pltpu.VMEM((n, S), F32),
            pltpu.VMEM((n, 4 * S), F32), pltpu.VMEM((n, 4 * S), F32),
            pltpu.VMEM((8, SUB, S), F32), pltpu.VMEM((8, S), F32), pltpu.VMEM((nsp - 1, 8, S), F32),
            pltpu.VMEM((4, SUB, S), F32),
            pltpu.VMEM((ntp, q, W), BF16), pltpu.VMEM((ntp - 1, q, W), BF16),
            pltpu.VMEM((q, ntp * W), BF16), pltpu.VMEM(emitted.shape, BF16),
            pltpu.VMEM((ntp - 1, q, Dl), BF16),
            pltpu.VMEM((q, D), F32),
            pltpu.VMEM((ntp, nsp, D // nsp, F), BF16), pltpu.VMEM((ntp, nsp, F, D // nsp), BF16),
            pltpu.VMEM((c_ff, q, D), BF16), pltpu.VMEM((ntp, q_all, F), BF16),
            pltpu.VMEM((c_ff, q, D), BF16), pltpu.VMEM((c_ff - 1, q, D), BF16),
            pltpu.VMEM((ntp, q, Dl), BF16), pltpu.VMEM((ntp - 1, q, Dl), BF16),
            dma((3,)), dma((nsp - 1,)), dma((nsp - 1,)), dma((ntp - 1,)), dma((ntp - 1,)),
            dma((ntp - 1,)), dma((ntp - 1,)),
            *[dma((nsp - 1,))] * 4, *[dma((M - 1, nsp))] * 4, *[dma((M,))] * 4,
            *[dma((2, c_ff // 2))] * 2, *[dma((c_ff - 1,))] * 2, *[dma((ntp - 1,))] * 2,
        ],
        compiler_params=pltpu.CompilerParams(collective_id=0, has_side_effects=True),
        cost_estimate=pl.CostEstimate(flops=10**9, bytes_accessed=3 * 10**7, transcendentals=10**6),
    )(*operands)


def solution(mesh):
    both, swapped = P("sp", "tp"), P("tp", "sp")
    in_specs = (both, both, swapped, swapped) + (P(),) * 10 + (both, swapped)
    return jax.shard_map(on_device, mesh=mesh, in_specs=in_specs, out_specs=both, check_vma=False)
```

```python
import functools

import jax
import jax.numpy as jnp
from jax import lax
from jax.experimental import pallas as pl
from jax.experimental.pallas import tpu as pltpu
from jax.sharding import PartitionSpec as P

CHAN = 16
NORM_W = 128
EPSILON = 1e-06
SUB = 8
F32, BF16 = jnp.float32, jnp.bfloat16


def sincos(a):
    k = jnp.floor(a * 0.6366197723675814 + 0.5)
    r = a - k * 1.5703125
    r = r - k * 4.8351287841796875e-4
    r = r - k * 3.138556210e-7
    z = r * r
    s = r + r * z * (-1.6666654611e-1 + z * (8.3321608736e-3 + z * -1.9515295891e-4))
    c = 1.0 - 0.5 * z + z * z * (
        4.166664568298827e-2 + z * (-1.388731625493765e-3 + z * 2.443315711809948e-5)
    )
    half = jnp.floor(k * 0.5)
    odd = (k - 2.0 * half) > 0.5
    half_odd = (half - 2.0 * jnp.floor(half * 0.5)) > 0.5
    cos_v = jnp.where(odd, -s, c)
    sin_v = jnp.where(odd, c, s)
    return jnp.where(half_odd, -cos_v, cos_v), jnp.where(half_odd, -sin_v, sin_v)


def one_minus_exp_neg(u):
    t = jnp.full_like(u, 1.0)
    for m in range(10, 1, -1):
        t = 1.0 - u * (1.0 / m) * t
    return u * t


def cmul(ar, ai, br, bi):
    return ar * br - ai * bi, ar * bi + ai * br


def mixer_body(cfg, x_ref, dt_ref, lf_ref, long_rate, short_rate, long_freq, short_freq,
               skip_ref, gain_ref, resid_ref, lead_ref, long_hbm, short_hbm, emit_hbm, up_hbm, down_hbm,
               out_ref, lin_l, lin_s, lin_sem,
               pace, surge, pre, st, blk, ends, ends_all, cin, mg, rows_in, mrg, emit, resid_in,
               mid_out, wup, wdn, nrm, hid, part, rs_in, fin, fin_in,
               copy_sem, s_ends, r_ends, s_rows, r_rows, s_res, r_res,
               s_u1, r_u1, s_d1, r_d1, s_u2, r_u2, s_d2, r_d2, s_u3, r_u3, s_d3, r_d3,
               s_nrm, r_nrm, s_rs, r_rs, s_fin, r_fin):
    nsp, ntp, n, S, W, G, PL, PS, D, c_ff, F = cfg
    M = ntp // 2
    L = n // SUB
    half = G // 2
    SL = half * PL
    sp = lax.axis_index("sp")
    tp = lax.axis_index("tp")
    q = n // ntp
    Dl = D // ntp
    MESH = pl.DeviceIdType.MESH

    emit_copy = pltpu.make_async_copy(emit_hbm, emit, copy_sem.at[0])
    lin_copies = []
    for at in range(8):
        for kind, (src, dst) in enumerate(((long_hbm, lin_l), (short_hbm, lin_s))):
            lin_copies.append(pltpu.make_async_copy(
                src.at[at // 4, at // 2 % 2, at % 2, pl.ds(tp * half, half)], dst.at[at],
                lin_sem.at[kind, at]))
    for copy in lin_copies:
        copy.start()
    emit_copy.start()
    chunk = lax.rem(sp, c_ff)
    partner = tp + 1 - 2 * lax.rem(tp, 2)

    def cols(of):
        return pl.ds(pl.multiple_of(of * F, 128), F)

    own_up = pltpu.make_async_copy(up_hbm.at[:, cols(chunk)], wup.at[tp, sp], copy_sem.at[1])
    own_down = pltpu.make_async_copy(down_hbm.at[cols(chunk), :], wdn.at[tp, sp], copy_sem.at[2])
    own_up.start()
    own_down.start()

    def spread_copy(k, up):
        to = lax.rem(sp + k, nsp)
        src = up_hbm.at[:, cols(lax.rem(to, c_ff))] if up else down_hbm.at[cols(lax.rem(to, c_ff)), :]
        return pltpu.make_async_remote_copy(
            src_ref=src, dst_ref=(wup if up else wdn).at[tp, sp],
            send_sem=(s_u1 if up else s_d1).at[k - 1], recv_sem=(r_u1 if up else r_d1).at[k - 1],
            device_id=(to, tp), device_id_type=MESH)

    def across_copy(m, k, up):
        piece = (wup if up else wdn).at[tp, lax.rem(sp - k + nsp, nsp)]
        return pltpu.make_async_remote_copy(
            src_ref=piece, dst_ref=piece,
            send_sem=(s_u2 if up else s_d2).at[m - 1, k], recv_sem=(r_u2 if up else r_d2).at[m - 1, k],
            device_id=(sp, lax.rem(tp + 2 * m, ntp)), device_id_type=MESH)

    def pair_copy(m, up):
        piece = (wup if up else wdn).at[lax.rem(tp + 2 * m, ntp)]
        return pltpu.make_async_remote_copy(
            src_ref=piece, dst_ref=piece,
            send_sem=(s_u3 if up else s_d3).at[m], recv_sem=(r_u3 if up else r_d3).at[m],
            device_id=(sp, partner), device_id_type=MESH)

    def pass_on(first, last, up):
        for k in range(first, last):
            if k == 0:
                (own_up if up else own_down).wait()
            else:
                spread_copy(k, up).wait_recv()
            for m in range(1, M):
                across_copy(m, k, up).start()

    barrier = pltpu.get_barrier_semaphore()
    for k in range(1, nsp):
        pl.semaphore_signal(barrier, inc=1, device_id=(lax.rem(sp + k, nsp), tp), device_id_type=MESH)
    for k in range(1, ntp):
        pl.semaphore_signal(barrier, inc=1, device_id=(sp, lax.rem(tp + k, ntp)), device_id_type=MESH)
    pl.semaphore_wait(barrier, nsp + ntp - 2)

    def res_copy(k):
        to = lax.rem(tp + k, ntp)
        return pltpu.make_async_remote_copy(
            src_ref=resid_ref.at[pl.ds(to * q, q), :], dst_ref=resid_in.at[k - 1],
            send_sem=s_res.at[k - 1], recv_sem=r_res.at[k - 1],
            device_id=(sp, to), device_id_type=MESH)

    for k in range(1, nsp):
        spread_copy(k, True).start()
    for k in range(1, ntp):
        res_copy(k).start()

    lane = lax.broadcasted_iota(jnp.int32, (G, S), 1)
    group = jnp.where(lane < SL, 2 * (lane // PL), 2 * ((lane - SL) // PS) + 1)
    spread = (group == lax.broadcasted_iota(jnp.int32, (G, S), 0)).astype(F32)
    r = lax.broadcasted_iota(jnp.int32, (n, n), 0)
    t = lax.broadcasted_iota(jnp.int32, (n, n), 1)
    mix = (t == (r % SUB) * L + r // SUB).astype(F32)

    def per_state(ref):
        moved = lax.dot_general(ref[...], mix, (((1,), (1,)), ((), ())),
                                precision=lax.Precision.HIGHEST, preferred_element_type=F32)
        return lax.dot_general(moved, spread, (((0,), (0,)), ((), ())),
                               precision=lax.Precision.HIGHEST, preferred_element_type=F32)

    pace[...] = per_state(dt_ref)
    surge[...] = per_state(lf_ref)

    def flat_kind(ref, e):
        many, states = ref.shape[1:]
        width = half * states
        repeat = (lax.broadcasted_iota(jnp.int32, (states, width), 1) % states
                  == lax.broadcasted_iota(jnp.int32, (states, width), 0)).astype(F32)
        wide = jnp.dot(ref[e], repeat, precision=lax.Precision.HIGHEST, preferred_element_type=F32)
        owner = tp * half + lax.broadcasted_iota(jnp.int32, (many, width), 1) // states
        mine = owner == lax.broadcasted_iota(jnp.int32, (many, width), 0)
        return jnp.sum(jnp.where(mine, wide, 0.0), axis=0, keepdims=True)

    def flat(long_ref, short_ref, e):
        return jnp.concatenate([flat_kind(long_ref, e), flat_kind(short_ref, e)], axis=1)

    def widened(ref, index, states, sign):
        rows, width = half * CHAN, half * states
        repeat = (lax.broadcasted_iota(jnp.int32, (states, width), 1) % states
                  == lax.broadcasted_iota(jnp.int32, (states, width), 0)).astype(BF16)
        wide = jnp.dot(ref[index].reshape(rows, states).astype(BF16), repeat, preferred_element_type=F32)
        own_block = (lax.broadcasted_iota(jnp.int32, (rows, width), 0) // CHAN
                     == lax.broadcasted_iota(jnp.int32, (rows, width), 1) // states)
        return jnp.where(own_block, sign * wide, 0.0).astype(BF16)

    def block_map(index, sign=1.0):
        long_part = widened(lin_l, index, PL, sign)
        short_part = widened(lin_s, index, PS, sign)
        no_long, no_short = jnp.zeros((CHAN, SL), BF16), jnp.zeros((CHAN, S - SL), BF16)
        bands = []
        for g in range(half):
            band = slice(g * CHAN, (g + 1) * CHAN)
            bands.append(jnp.concatenate([long_part[band], no_short], axis=1))
            bands.append(jnp.concatenate([no_long, short_part[band]], axis=1))
        return jnp.concatenate(bands, axis=0)

    xv = jnp.dot(mix.astype(BF16), x_ref[...], preferred_element_type=F32).astype(BF16)
    for copy in lin_copies:
        copy.wait()
    for e in range(2):
        for c in range(2):
            st[:, pl.ds((2 * e + c) * S, S)] = jnp.dot(
                xv, block_map(4 * e + c), preferred_element_type=F32)

    for e in range(2):
        rate = flat(long_rate, short_rate, e)
        freq = flat(long_freq, short_freq, e)

        def step(i, carry):
            pr, pi, sr, si = carry
            at = i if e == 0 else L - 1 - i
            rows = pl.ds(pl.multiple_of(at * SUB, SUB), SUB)
            d = pace[rows, :]
            rd = rate * d
            m = jnp.exp(surge[rows, :] - rd)
            cos_v, sin_v = sincos(freq * d)
            w = jnp.sqrt(one_minus_exp_neg(2.0 * rd))
            ar, ai = m * cos_v, m * sin_v
            pr, pi = cmul(ar, ai, pr, pi)
            sr, si = cmul(ar, ai, sr, si)
            sr = sr + w * st[rows, pl.ds(2 * e * S, S)]
            si = si + w * st[rows, pl.ds((2 * e + 1) * S, S)]
            pre[rows, pl.ds(2 * e * S, S)] = pr
            pre[rows, pl.ds((2 * e + 1) * S, S)] = pi
            st[rows, pl.ds(2 * e * S, S)] = sr
            st[rows, pl.ds((2 * e + 1) * S, S)] = si
            return pr, pi, sr, si

        zero = jnp.zeros((SUB, S), F32)
        total = lax.fori_loop(0, L, step, (zero + 1.0, zero, zero, zero))
        for c in range(4):
            blk[4 * e + c] = total[c]
        order = range(SUB) if e == 0 else range(SUB - 1, -1, -1)
        run = None
        for b in order:
            now = tuple(blk[4 * e + c, b : b + 1, :] for c in range(4))
            if run is None:
                run = now
            else:
                p = cmul(now[0], now[1], run[0], run[1])
                s = cmul(now[0], now[1], run[2], run[3])
                run = (p[0], p[1], s[0] + now[2], s[1] + now[3])
        for c in range(4):
            ends[4 * e + c : 4 * e + c + 1, :] = run[c]

    def ends_copy(k):
        return pltpu.make_async_remote_copy(
            src_ref=ends, dst_ref=ends_all.at[k - 1],
            send_sem=s_ends.at[k - 1], recv_sem=r_ends.at[k - 1],
            device_id=(lax.rem(sp + k, nsp), tp), device_id_type=MESH)

    for k in range(1, nsp):
        ends_copy(k).start()
    for k in range(1, nsp):
        spread_copy(k, False).start()

    read = jnp.concatenate(
        [block_map(2), block_map(3, -1.0), block_map(6), block_map(7, -1.0)], axis=1)

    pass_on(0, nsp // 2, True)
    for k in range(1, nsp):
        ends_copy(k).wait_recv()
    blank = jnp.zeros((1, S), F32)

    def fold(j, carry, e):
        cr, ci = carry
        k = nsp - 1 - j if e == 0 else j + 1
        reached = k <= sp if e == 0 else nsp - k <= nsp - 1 - sp
        got = ends_all[k - 1]
        nr, ni = cmul(got[4 * e : 4 * e + 1], got[4 * e + 1 : 4 * e + 2], cr, ci)
        nr = nr + got[4 * e + 2 : 4 * e + 3]
        ni = ni + got[4 * e + 3 : 4 * e + 4]
        return jnp.where(reached, nr, cr), jnp.where(reached, ni, ci)

    for e in range(2):
        cr, ci = lax.fori_loop(0, nsp - 1, functools.partial(fold, e=e), (blank, blank))
        order = range(SUB) if e == 0 else range(SUB - 1, -1, -1)
        for b in order:
            cin[2 * e, b : b + 1, :] = cr
            cin[2 * e + 1, b : b + 1, :] = ci
            now = tuple(blk[4 * e + c, b : b + 1, :] for c in range(4))
            nr, ni = cmul(now[0], now[1], cr, ci)
            cr, ci = nr + now[2], ni + now[3]

        inr, ini = cin[2 * e], cin[2 * e + 1]

        def settle(i, _):
            rows = pl.ds(pl.multiple_of(i * SUB, SUB), SUB)
            re, im = pl.ds(2 * e * S, S), pl.ds((2 * e + 1) * S, S)
            ar, ai = cmul(pre[rows, re], pre[rows, im], inr, ini)
            st[rows, re] = st[rows, re] + ar
            st[rows, im] = st[rows, im] + ai
            return 0

        lax.fori_loop(0, L, settle, 0)

    y = lax.dot_general(st[...].astype(BF16), read, (((1,), (1,)), ((), ())),
                        preferred_element_type=F32)
    own = pl.ds(pl.multiple_of(tp * W, 128), W)
    skip_row, gain_row = skip_ref[:, own], gain_ref[:, own]
    y = y + skip_row * xv.astype(F32)
    y = 0.5 * y * (1.0 + jnp.tanh(0.7978845608028654 * (y + 0.044715 * y * y * y)))
    heads = []
    for h in range(W // NORM_W):
        head = y[:, h * NORM_W : (h + 1) * NORM_W]
        scale = lax.rsqrt(jnp.mean(head * head, axis=1, keepdims=True) + EPSILON)
        heads.append(head * scale * gain_row[:, h * NORM_W : (h + 1) * NORM_W])
    merged = jnp.concatenate(heads, axis=1).astype(BF16)
    t = lax.broadcasted_iota(jnp.int32, (n, n), 0)
    r = lax.broadcasted_iota(jnp.int32, (n, n), 1)
    unmix = (r == (t % L) * SUB + t // L).astype(BF16)
    mg[...] = jnp.dot(unmix, merged, preferred_element_type=F32).astype(BF16).reshape(ntp, q, W)

    def row_copy(k):
        to = lax.rem(tp + k, ntp)
        return pltpu.make_async_remote_copy(
            src_ref=mg.at[to], dst_ref=rows_in.at[k - 1],
            send_sem=s_rows.at[k - 1], recv_sem=r_rows.at[k - 1],
            device_id=(sp, to), device_id_type=MESH)

    for k in range(1, ntp):
        row_copy(k).start()
    pass_on(nsp // 2, nsp, True)
    emit_copy.wait()
    mrg[:, pl.ds(pl.multiple_of(tp * W, 128), W)] = mg[tp]
    mid_out[:, pl.ds(pl.multiple_of(tp * Dl, 128), Dl)] = resid_ref[pl.ds(pl.multiple_of(tp * q, q), q), :].astype(F32)
    for k in range(1, ntp):
        src = lax.rem(tp - k + ntp, ntp)
        res_copy(k).wait_recv()
        mid_out[:, pl.ds(pl.multiple_of(src * Dl, 128), Dl)] = resid_in[k - 1].astype(F32)
        row_copy(k).wait_recv()
        mrg[:, pl.ds(pl.multiple_of(src * W, 128), W)] = rows_in[k - 1]
    mid = mid_out[...] + jnp.dot(mrg[...], emit[...], preferred_element_type=F32)
    mid_out[...] = mid
    scale = lax.rsqrt(jnp.mean(mid * mid, axis=1, keepdims=True) + EPSILON)
    base, q_all = sp - chunk, c_ff * q
    nrm[chunk] = (mid * scale * lead_ref[...]).astype(BF16)

    def peer(k):
        return lax.rem(chunk + k, c_ff)

    H = c_ff // 2

    def nrm_across(m):
        return pltpu.make_async_remote_copy(
            src_ref=nrm.at[chunk], dst_ref=nrm.at[chunk],
            send_sem=s_nrm.at[0, m], recv_sem=r_nrm.at[0, m],
            device_id=(base + peer(2 * m), tp), device_id_type=MESH)

    def nrm_pair(m):
        return pltpu.make_async_remote_copy(
            src_ref=nrm.at[peer(2 * m)], dst_ref=nrm.at[peer(2 * m)],
            send_sem=s_nrm.at[1, m], recv_sem=r_nrm.at[1, m],
            device_id=(base + chunk + 1 - 2 * lax.rem(chunk, 2), tp), device_id_type=MESH)

    def rs_copy(k):
        return pltpu.make_async_remote_copy(
            src_ref=part.at[peer(k)], dst_ref=rs_in.at[k - 1],
            send_sem=s_rs.at[k - 1], recv_sem=r_rs.at[k - 1],
            device_id=(base + peer(k), tp), device_id_type=MESH)

    def fin_copy(k):
        to = lax.rem(tp + k, ntp)
        return pltpu.make_async_remote_copy(
            src_ref=fin.at[to], dst_ref=fin_in.at[k - 1],
            send_sem=s_fin.at[k - 1], recv_sem=r_fin.at[k - 1],
            device_id=(sp, to), device_id_type=MESH)

    for m in range(1, H):
        nrm_across(m).start()
    nrm_pair(0).start()
    pair_copy(0, True).start()
    pass_on(0, nsp, False)
    pair_copy(0, False).start()
    for m in range(1, H):
        nrm_across(m).wait_recv()
        nrm_pair(H - m).start()
    for up in (True, False):
        for m in range(1, M):
            for k in range(nsp):
                across_copy(m, k, up).wait_recv()
            pair_copy(M - m, up).start()
        if up:
            for m in range(M):
                pair_copy(m, True).wait_recv()
            for m in range(H):
                nrm_pair(m).wait_recv()
            rows = nrm[...].reshape(q_all, D)

            def raise_step(t, _):
                upward = jnp.dot(rows, wup[t].reshape(D, F), preferred_element_type=F32)
                hid[t] = jnp.square(jnp.maximum(upward, 0.0)).astype(BF16)
                return 0

            lax.fori_loop(0, ntp, raise_step, 0)
    for m in range(M):
        pair_copy(m, False).wait_recv()
    Dc = D // nsp
    for j in range(nsp):
        total = jnp.dot(hid[0], wdn[0, j], preferred_element_type=F32)
        for t in range(1, ntp):
            total = total + jnp.dot(hid[t], wdn[t, j], preferred_element_type=F32)
        part[:, :, j * Dc : (j + 1) * Dc] = total.astype(BF16).reshape(c_ff, q, Dc)
    for k in range(1, c_ff):
        rs_copy(k).start()
    result = mid_out[...] + part[chunk].astype(F32)
    for k in range(1, c_ff):
        rs_copy(k).wait_recv()
        result = result + rs_in[k - 1].astype(F32)
    result = result.astype(BF16)
    for t in range(ntp):
        fin[t] = result[:, t * Dl : (t + 1) * Dl]
    for k in range(1, ntp):
        fin_copy(k).start()
    out_ref[pl.ds(pl.multiple_of(tp * q, q), q), :] = fin[tp]
    for k in range(1, ntp):
        fin_copy(k).wait_recv()
        src = lax.rem(tp - k + ntp, ntp)
        out_ref[pl.ds(pl.multiple_of(src * q, q), q), :] = fin_in[k - 1]
    for k in range(1, c_ff):
        rs_copy(k).wait_send()
    for m in range(H):
        if m > 0:
            nrm_across(m).wait_send()
        nrm_pair(m).wait_send()
    for k in range(1, ntp):
        fin_copy(k).wait_send()
    for up in (True, False):
        for k in range(1, nsp):
            spread_copy(k, up).wait_send()
        for m in range(1, M):
            for k in range(nsp):
                across_copy(m, k, up).wait_send()
        for m in range(M):
            pair_copy(m, up).wait_send()
    for k in range(1, nsp):
        ends_copy(k).wait_send()
    for k in range(1, ntp):
        res_copy(k).wait_send()
        row_copy(k).wait_send()


def mesh_split(nsp, ntp):
    Y = ntp // 2
    X = Y if Y > 0 and nsp % Y == 0 else 1
    return nsp // X, X, Y


def paired_body(cfg, x_ref, dt_ref, lf_ref, long_rate, short_rate, long_freq, short_freq,
                skip_ref, gain_ref, resid_ref, lead_ref, long_hbm, short_hbm, emit_hbm, up_hbm, down_hbm,
                out_ref, lin_l, lin_s, lin_sem,
                pace, surge, pre, st, blk, ends, ends_all, cin, mg, rows_in, mrg, emit, resid_in,
                mid_out, wup, wdn, nrm, hid, loc, a_out, a_in, b_out, b_in, c_out, c_in, fin, fin_in,
                copy_sem, own_sem, s_ends, r_ends, s_rows, r_rows, s_res, r_res,
                s_z, r_z, s_x, r_x, s_d, r_d, s_t, r_t, s_y, r_y,
                s_a, r_a, s_b, r_b, s_c, r_c, s_fin, r_fin):
    nsp, ntp, n, S, W, G, PL, PS, D, Fz = cfg
    Z, X, Y = mesh_split(nsp, ntp)
    L = n // SUB
    half = G // 2
    SL = half * PL
    sp = lax.axis_index("sp")
    tp = lax.axis_index("tp")
    q = n // ntp
    Dl = D // ntp
    Dh = D // nsp // 2
    Rh = D // nsp // 2
    MESH = pl.DeviceIdType.MESH
    z, x, y, c = sp // X, lax.rem(sp, X), tp // 2, lax.rem(tp, 2)
    side = z // 2
    half_in, half_out = 1 + side, 3 * side
    far_in, far_out = 2 - side, 3 - 3 * side
    far0 = 2 - 2 * side
    mate = z + 1 - 2 * lax.rem(z, 2)
    inner, outer = z == half_in, z == half_out
    kinds = (z, mate, far_in, far_out)
    as_seen = 2 + jnp.where(outer, 1, 0)

    def dev(z_, x_, y_, c_):
        return (z_ * X + x_, y_ * 2 + c_)

    x_mate, y_mate, c_mate = dev(z, 1 - x, y, c), dev(z, x, 1 - y, c), dev(z, x, y, 1 - c)

    def remote(src, dst, ssem, rsem, to):
        return pltpu.make_async_remote_copy(src_ref=src, dst_ref=dst, send_sem=ssem, recv_sem=rsem,
                                            device_id=to, device_id_type=MESH)

    emit_copy = pltpu.make_async_copy(emit_hbm, emit, copy_sem.at[0])
    lin_copies = []
    for at in range(8):
        for kind, (src, dst) in enumerate(((long_hbm, lin_l), (short_hbm, lin_s))):
            lin_copies.append(pltpu.make_async_copy(
                src.at[at // 4, at // 2 % 2, at % 2, pl.ds(tp * half, half)], dst.at[at],
                lin_sem.at[kind, at]))

    def bank(up):
        return wup if up else wdn

    def shard(up, h, to):
        part = pl.ds(pl.multiple_of(to * Fz, 128), Fz)
        if up:
            return up_hbm.at[pl.ds(h * Rh, Rh), part]
        return down_hbm.at[part, pl.ds(h * Dh, Dh)]

    def own_copy(up, h):
        return pltpu.make_async_copy(shard(up, h, z), bank(up).at[c, sp, h], own_sem.at[1 - up, h])

    def z_copy(up, h, k):
        to = kinds[k]
        return remote(shard(up, h, to), bank(up).at[c, sp, h], s_z.at[1 - up, h, k],
                      r_z.at[1 - up, h, 1 if k == 1 else as_seen], dev(to, x, y, c))

    def z_wait(up, h, k):
        piece = bank(up).at[c, kinds[k] * X + x, h]
        remote(piece, piece, s_z.at[1 - up, h, k], r_z.at[1 - up, h, k], x_mate).wait_recv()

    def x_copy(up, h, k):
        piece = bank(up).at[c, kinds[k] * X + x, h]
        return remote(shard(up, h, z) if k == 0 else piece, piece,
                      s_x.at[1 - up, h, k], r_x.at[1 - up, h, k], x_mate)

    def d_copy(up, h, k, other):
        piece = bank(up).at[c, kinds[k] * X + (1 - x if other else x), h]
        return remote(shard(up, h, z) if k == 0 and not other else piece, piece,
                      s_d.at[1 - up, h, k, other], r_d.at[1 - up, h, k, other], c_mate)

    def hop1(up, h, k):
        z_wait(up, h, k)
        x_copy(up, h, k).start()
        d_copy(up, h, k, 0).start()

    def hop2(up, h, k):
        x_copy(up, h, k).wait_recv()
        d_copy(up, h, k, 1).start()

    def hop3(up, h, k):
        d_copy(up, h, k, 0).wait_recv()
        d_copy(up, h, k, 1).wait_recv()

    def res_copy(k):
        to = lax.rem(tp + k, ntp)
        return remote(resid_ref.at[pl.ds(to * q, q), :], resid_in.at[k - 1], s_res.at[k - 1], r_res.at[k - 1],
                      (sp, to))

    barrier = pltpu.get_barrier_semaphore()
    for k in range(1, nsp):
        pl.semaphore_signal(barrier, inc=1, device_id=(lax.rem(sp + k, nsp), tp), device_id_type=MESH)
    for k in range(1, ntp):
        pl.semaphore_signal(barrier, inc=1, device_id=(sp, lax.rem(tp + k, ntp)), device_id_type=MESH)
    for copy in lin_copies:
        copy.start()
    emit_copy.start()
    for up in (1, 0):
        for h in range(2):
            own_copy(up, h).start()

    lane = lax.broadcasted_iota(jnp.int32, (G, S), 1)
    group = jnp.where(lane < SL, 2 * (lane // PL), 2 * ((lane - SL) // PS) + 1)
    spread = (group == lax.broadcasted_iota(jnp.int32, (G, S), 0)).astype(F32)
    r = lax.broadcasted_iota(jnp.int32, (n, n), 0)
    t = lax.broadcasted_iota(jnp.int32, (n, n), 1)
    mix = (t == (r % SUB) * L + r // SUB).astype(F32)

    def per_state(ref):
        moved = lax.dot_general(ref[...], mix, (((1,), (1,)), ((), ())),
                                precision=lax.Precision.HIGHEST, preferred_element_type=F32)
        return lax.dot_general(moved, spread, (((0,), (0,)), ((), ())),
                               precision=lax.Precision.HIGHEST, preferred_element_type=F32)

    pace[...] = per_state(dt_ref)
    surge[...] = per_state(lf_ref)

    pl.semaphore_wait(barrier, nsp + ntp - 2)

    @pl.when(outer)
    def _():
        for k in (2, 3):
            z_copy(1, 0, k).start()

    @pl.when(inner)
    def _():
        z_copy(1, 0, 1).start()

    for h in range(2):
        x_copy(1, h, 0).start()
        d_copy(1, h, 0, 0).start()
    for k in range(1, ntp):
        res_copy(k).start()

    def flat_kind(ref, e):
        many, states = ref.shape[1:]
        width = half * states
        repeat = (lax.broadcasted_iota(jnp.int32, (states, width), 1) % states
                  == lax.broadcasted_iota(jnp.int32, (states, width), 0)).astype(F32)
        wide = jnp.dot(ref[e], repeat, precision=lax.Precision.HIGHEST, preferred_element_type=F32)
        owner = tp * half + lax.broadcasted_iota(jnp.int32, (many, width), 1) // states
        mine = owner == lax.broadcasted_iota(jnp.int32, (many, width), 0)
        return jnp.sum(jnp.where(mine, wide, 0.0), axis=0, keepdims=True)

    def flat(long_ref, short_ref, e):
        return jnp.concatenate([flat_kind(long_ref, e), flat_kind(short_ref, e)], axis=1)

    def widened(ref, index, states, sign):
        rows, width = half * CHAN, half * states
        repeat = (lax.broadcasted_iota(jnp.int32, (states, width), 1) % states
                  == lax.broadcasted_iota(jnp.int32, (states, width), 0)).astype(BF16)
        wide = jnp.dot(ref[index].reshape(rows, states).astype(BF16), repeat, preferred_element_type=F32)
        own_block = (lax.broadcasted_iota(jnp.int32, (rows, width), 0) // CHAN
                     == lax.broadcasted_iota(jnp.int32, (rows, width), 1) // states)
        return jnp.where(own_block, sign * wide, 0.0).astype(BF16)

    def block_map(index, sign=1.0):
        long_part = widened(lin_l, index, PL, sign)
        short_part = widened(lin_s, index, PS, sign)
        no_long, no_short = jnp.zeros((CHAN, SL), BF16), jnp.zeros((CHAN, S - SL), BF16)
        bands = []
        for g in range(half):
            band = slice(g * CHAN, (g + 1) * CHAN)
            bands.append(jnp.concatenate([long_part[band], no_short], axis=1))
            bands.append(jnp.concatenate([no_long, short_part[band]], axis=1))
        return jnp.concatenate(bands, axis=0)

    xv = jnp.dot(mix.astype(BF16), x_ref[...], preferred_element_type=F32).astype(BF16)
    for copy in lin_copies:
        copy.wait()
    for e in range(2):
        for part in range(2):
            st[:, pl.ds((2 * e + part) * S, S)] = jnp.dot(
                xv, block_map(4 * e + part), preferred_element_type=F32)

    for e in range(2):
        rate = flat(long_rate, short_rate, e)
        freq = flat(long_freq, short_freq, e)

        def step(i, carry):
            pr, pi, sr, si = carry
            at = i if e == 0 else L - 1 - i
            rows = pl.ds(pl.multiple_of(at * SUB, SUB), SUB)
            d = pace[rows, :]
            rd = rate * d
            m = jnp.exp(surge[rows, :] - rd)
            cos_v, sin_v = sincos(freq * d)
            w = jnp.sqrt(one_minus_exp_neg(2.0 * rd))
            ar, ai = m * cos_v, m * sin_v
            pr, pi = cmul(ar, ai, pr, pi)
            sr, si = cmul(ar, ai, sr, si)
            sr = sr + w * st[rows, pl.ds(2 * e * S, S)]
            si = si + w * st[rows, pl.ds((2 * e + 1) * S, S)]
            pre[rows, pl.ds(2 * e * S, S)] = pr
            pre[rows, pl.ds((2 * e + 1) * S, S)] = pi
            st[rows, pl.ds(2 * e * S, S)] = sr
            st[rows, pl.ds((2 * e + 1) * S, S)] = si
            return pr, pi, sr, si

        zero = jnp.zeros((SUB, S), F32)
        total = lax.fori_loop(0, L, step, (zero + 1.0, zero, zero, zero))
        for part in range(4):
            blk[4 * e + part] = total[part]
        order = range(SUB) if e == 0 else range(SUB - 1, -1, -1)
        run = None
        for b in order:
            now = tuple(blk[4 * e + part, b : b + 1, :] for part in range(4))
            if run is None:
                run = now
            else:
                p = cmul(now[0], now[1], run[0], run[1])
                s = cmul(now[0], now[1], run[2], run[3])
                run = (p[0], p[1], s[0] + now[2], s[1] + now[3])
        for part in range(4):
            ends[e, part : part + 1, :] = run[part]

    def ends_copy(e, k):
        return remote(ends.at[e], ends_all.at[e, k - 1], s_ends.at[e, k - 1], r_ends.at[e, k - 1],
                      (sp + k if e == 0 else sp - k, tp))

    def has_after(e, k):
        return sp + k < nsp if e == 0 else sp >= k

    def has_before(e, k):
        return has_after(1 - e, k)

    def ends_do(e, k, send, act):
        @pl.when(has_after(e, k) if send else has_before(e, k))
        def _():
            act(ends_copy(e, k))

    for k in range(1, nsp):
        for e in range(2):
            ends_do(e, k, True, lambda copy: copy.start())

    @pl.when(inner)
    def _():
        for k in (2, 3):
            z_copy(1, 0, k).start()
        z_copy(1, 1, 1).start()

    @pl.when(outer)
    def _():
        for h in range(2):
            z_copy(1, h, 1).start()
        for k in (2, 3):
            z_copy(1, 1, k).start()
        hop1(1, 0, 1)

    read = jnp.concatenate(
        [block_map(2), block_map(3, -1.0), block_map(6), block_map(7, -1.0)], axis=1)

    for k in range(nsp - 1, 0, -1):
        for e in range(2):
            ends_do(e, k, False, lambda copy: copy.wait_recv())
    blank = jnp.zeros((1, S), F32)

    def fold(j, carry, e):
        cr, ci = carry
        k = nsp - 1 - j
        got = ends_all[e, k - 1]
        nr, ni = cmul(got[0:1], got[1:2], cr, ci)
        reached = has_before(e, k)
        return jnp.where(reached, nr + got[2:3], cr), jnp.where(reached, ni + got[3:4], ci)

    for e in range(2):
        cr, ci = lax.fori_loop(0, nsp - 1, functools.partial(fold, e=e), (blank, blank))
        order = range(SUB) if e == 0 else range(SUB - 1, -1, -1)
        for b in order:
            cin[2 * e, b : b + 1, :] = cr
            cin[2 * e + 1, b : b + 1, :] = ci
            now = tuple(blk[4 * e + part, b : b + 1, :] for part in range(4))
            nr, ni = cmul(now[0], now[1], cr, ci)
            cr, ci = nr + now[2], ni + now[3]

        inr, ini = cin[2 * e], cin[2 * e + 1]

        def settle(i, _):
            rows = pl.ds(pl.multiple_of(i * SUB, SUB), SUB)
            re, im = pl.ds(2 * e * S, S), pl.ds((2 * e + 1) * S, S)
            ar, ai = cmul(pre[rows, re], pre[rows, im], inr, ini)
            st[rows, re] = st[rows, re] + ar
            st[rows, im] = st[rows, im] + ai
            return 0

        lax.fori_loop(0, L, settle, 0)

    v = lax.dot_general(st[...].astype(BF16), read, (((1,), (1,)), ((), ())),
                        preferred_element_type=F32)
    own = pl.ds(pl.multiple_of(tp * W, 128), W)
    skip_row, gain_row = skip_ref[:, own], gain_ref[:, own]
    v = v + skip_row * xv.astype(F32)
    v = 0.5 * v * (1.0 + jnp.tanh(0.7978845608028654 * (v + 0.044715 * v * v * v)))
    heads = []
    for h in range(W // NORM_W):
        head = v[:, h * NORM_W : (h + 1) * NORM_W]
        scale = lax.rsqrt(jnp.mean(head * head, axis=1, keepdims=True) + EPSILON)
        heads.append(head * scale * gain_row[:, h * NORM_W : (h + 1) * NORM_W])
    merged = jnp.concatenate(heads, axis=1).astype(BF16)
    t = lax.broadcasted_iota(jnp.int32, (n, n), 0)
    r = lax.broadcasted_iota(jnp.int32, (n, n), 1)
    unmix = (r == (t % L) * SUB + t // L).astype(BF16)
    mg[...] = jnp.dot(unmix, merged, preferred_element_type=F32).astype(BF16).reshape(ntp, q, W)

    def row_copy(k):
        to = lax.rem(tp + k, ntp)
        return remote(mg.at[to], rows_in.at[k - 1], s_rows.at[k - 1], r_rows.at[k - 1], (sp, to))

    for k in range(1, ntp):
        row_copy(k).start()

    @pl.when(inner)
    def _():
        for h in range(2):
            z_copy(0, h, 1).start()

    for h in range(2):
        hop2(1, h, 0)

    hop1(1, 0, 3)

    @pl.when(inner)
    def _():
        hop1(1, 0, 1)

    hop1(1, 1, 1)
    emit_copy.wait()
    mrg[:, pl.ds(pl.multiple_of(tp * W, 128), W)] = mg[tp]
    mid_out[:, pl.ds(pl.multiple_of(tp * Dl, 128), Dl)] = resid_ref[pl.ds(pl.multiple_of(tp * q, q), q), :].astype(F32)
    for k in range(1, ntp):
        src = lax.rem(tp - k + ntp, ntp)
        res_copy(k).wait_recv()
        mid_out[:, pl.ds(pl.multiple_of(src * Dl, 128), Dl)] = resid_in[k - 1].astype(F32)
        row_copy(k).wait_recv()
        mrg[:, pl.ds(pl.multiple_of(src * W, 128), W)] = rows_in[k - 1]
    mid = mid_out[...] + jnp.dot(mrg[...], emit[...], preferred_element_type=F32)
    mid_out[...] = mid
    scale = lax.rsqrt(jnp.mean(mid * mid, axis=1, keepdims=True) + EPSILON)
    nrm[0, z] = (mid * scale * lead_ref[...]).astype(BF16)

    def t_far():
        return remote(nrm.at[0, z], nrm.at[0, z], s_t.at[0], r_t.at[as_seen], dev(far_in, x, y, c))

    def t_mate(k):
        block = nrm.at[0, kinds[k]]
        return remote(block, block, s_t.at[max(k, 1)], r_t.at[max(k, 1)], dev(mate, x, y, c))

    def t_wait(k):
        t_mate(k).wait_recv()

    def y_copy(k):
        return remote(nrm.at[0, kinds[k]], nrm.at[1, kinds[k]], s_y.at[k], r_y.at[k], y_mate)

    t_far().start()
    t_mate(0).start()
    y_copy(0).start()

    @pl.when(inner)
    def _():
        for k in (2, 3):
            z_copy(1, 1, k).start()

    @pl.when(outer)
    def _():
        for h in range(2):
            z_copy(0, h, 1).start()

    for h in range(2):
        x_copy(0, h, 0).start()
        d_copy(0, h, 0, 0).start()

    hop2(1, 0, 3)
    hop1(1, 1, 3)
    hop2(1, 0, 1)
    hop1(1, 0, 2)
    t_wait(1)
    y_copy(1).start()

    @pl.when(inner)
    def _():
        for k in (3, 2):
            t_wait(k)
            t_mate(k).start()
            y_copy(k).start()

    hop2(1, 1, 1)
    hop2(1, 1, 3)
    hop2(1, 0, 2)

    @pl.when(outer)
    def _():
        t_wait(3)
        y_copy(3).start()
        for k in (2, 3):
            z_copy(0, 0, k).start()
        t_wait(2)
        y_copy(2).start()

    hop1(1, 1, 2)

    @pl.when(inner)
    def _():
        for k in (2, 3):
            z_copy(0, 0, k).start()

    @pl.when(outer)
    def _():
        for k in (2, 3):
            z_copy(0, 1, k).start()

    for h in range(2):
        hop1(0, h, 1)
    for h in range(2):
        hop2(0, h, 0)
    hop2(1, 1, 2)
    for k in range(4):
        y_copy(k).wait_recv()
    for h in range(2):
        own_copy(1, h).wait()
        for k in range(4):
            hop3(1, h, k)
    rows = nrm[...].reshape(2 * Z * q, D)
    for b in range(2):
        upward = jnp.dot(rows, wup[b].reshape(D, Fz), preferred_element_type=F32)
        hid[b] = jnp.square(jnp.maximum(upward, 0.0)).astype(BF16)

    def cols(zs, x_, h):
        return pl.ds(pl.multiple_of((zs * X + x_) * 2 * Dh + h * Dh, 128), Dh)

    def a_copy(zs, h):
        g = zs * 2 + h
        return remote(a_out.at[g], a_in.at[g], s_a.at[g], r_a.at[g], y_mate)

    def b_copy(zs, h):
        g = zs * 2 + h
        return remote(b_out.at[g, mate], b_in.at[g, mate], s_b.at[0, g], r_b.at[0, g], dev(mate, x, y, c))

    def b_far(zs, h):
        g = zs * 2 + h
        blocks = pl.ds(far0, 2)
        return remote(b_out.at[g, blocks], b_in.at[g, blocks], s_b.at[1, g], r_b.at[1, g], dev(mate, x, y, c))

    def c_copy(zs, h, i):
        g = zs * 2 + h
        return remote(c_out.at[g, i], c_in.at[g], s_c.at[i, g], r_c.at[g], dev(far0 + i, x, y, c))

    def stage_a(zs, h):
        g = zs * 2 + h
        for x_ in range(X):
            total = jnp.dot(hid[0], wdn[0, zs * X + x_, h], preferred_element_type=F32)
            total = total + jnp.dot(hid[1], wdn[1, zs * X + x_, h], preferred_element_type=F32)
            total = total.reshape(2, Z, q, Dh)
            a_out[g, :, x_] = total[1].astype(BF16)
            loc[g, :, x_] = total[0]
        a_copy(zs, h).start()

    def stage_b(zs, h):
        g = zs * 2 + h
        a_copy(zs, h).wait_recv()
        total = loc[g] + a_in[g].astype(F32)
        loc[g] = total
        b_out[g] = total.astype(BF16)

        @pl.when(outer)
        def _():
            b_far(zs, h).start()

        b_copy(zs, h).start()

    def stage_c(zs, h):
        g = zs * 2 + h

        @pl.when(inner)
        def _():
            b_far(zs, h).wait_recv()
            blocks = pl.ds(far0, 2)
            c_out[g] = (loc[g, blocks] + b_in[g, blocks].astype(F32)).astype(BF16)
            for i in range(2):
                c_copy(zs, h, i).start()

        b_copy(zs, h).wait_recv()
        own_sum = loc[g, z] + b_in[g, z].astype(F32)
        for x_ in range(X):
            mid_out[:, cols(zs, x_, h)] = mid_out[:, cols(zs, x_, h)] + own_sum[x_]

    def stage_d(zs, h):
        g = zs * 2 + h
        c_copy(zs, h, 0).wait_recv()
        for x_ in range(X):
            mid_out[:, cols(zs, x_, h)] = mid_out[:, cols(zs, x_, h)] + c_in[g, x_].astype(F32)

    def fin_copy(to, at):
        return remote(fin.at[to], fin_in.at[at], s_fin.at[to], r_fin.at[at], (sp, to))

    def stage_e(zs):
        fin[zs] = mid_out[:, pl.ds(pl.multiple_of(zs * Dl, 128), Dl)].astype(BF16)

        @pl.when(zs != tp)
        def _():
            fin_copy(zs, tp).start()

    turns = [(zs, h) for zs in (half_in, half_out, far_out, far_in) for h in range(2)]
    hop1(0, 0, 3)

    @pl.when(inner)
    def _():
        for k in (2, 3):
            z_copy(0, 1, k).start()

    for h in range(2):
        own_copy(0, h).wait()
        hop3(0, h, 0)
    for h in range(2):
        hop2(0, h, 1)
    hop1(0, 1, 3)
    for h in range(2):
        hop3(0, h, 1)
    stage_a(*turns[0])
    stage_a(*turns[1])
    stage_a(*turns[2])
    stage_a(*turns[3])
    stage_b(*turns[0])
    hop1(0, 0, 2)
    hop2(0, 0, 3)
    stage_b(*turns[1])
    hop3(0, 0, 3)
    stage_a(*turns[4])
    stage_b(*turns[2])
    hop2(0, 1, 3)
    stage_b(*turns[3])
    hop3(0, 1, 3)
    stage_a(*turns[5])
    stage_c(*turns[0])
    hop2(0, 0, 2)
    stage_c(*turns[1])
    hop1(0, 1, 2)
    hop3(0, 0, 2)
    stage_a(*turns[6])
    stage_c(*turns[2])
    stage_b(*turns[4])
    stage_c(*turns[3])
    stage_b(*turns[5])
    hop2(0, 1, 2)
    stage_c(*turns[4])
    hop3(0, 1, 2)
    stage_a(*turns[7])
    stage_b(*turns[6])
    stage_c(*turns[5])
    stage_c(*turns[6])
    stage_b(*turns[7])
    for zs in (half_out, far_out):
        for h in range(2):
            stage_d(zs, h)
        stage_e(zs)
    stage_c(*turns[7])
    for zs in (far_in, half_in):
        for h in range(2):
            stage_d(zs, h)
        stage_e(zs)
    out_ref[pl.ds(pl.multiple_of(tp * q, q), q), :] = fin[tp]
    for k in range(1, ntp):
        src = lax.rem(tp + k, ntp)
        fin_copy(src, src).wait_recv()
        out_ref[pl.ds(pl.multiple_of(src * q, q), q), :] = fin_in[src]

    for up in (1, 0):
        for h in range(2):
            for k in range(4):
                if k > 0:
                    z_copy(up, h, k).wait_send()
                x_copy(up, h, k).wait_send()
                for other in range(2):
                    d_copy(up, h, k, other).wait_send()
    for e in range(2):
        for k in range(1, nsp):
            ends_do(e, k, True, lambda copy: copy.wait_send())
    t_far().wait_send()
    t_mate(0).wait_send()

    @pl.when(inner)
    def _():
        for k in (2, 3):
            t_mate(k).wait_send()

    for k in range(4):
        y_copy(k).wait_send()
    for zs in range(Z):
        for h in range(2):
            a_copy(zs, h).wait_send()
            b_copy(zs, h).wait_send()

            @pl.when(outer)
            def _():
                b_far(zs, h).wait_send()

            @pl.when(inner)
            def _():
                for i in range(2):
                    c_copy(zs, h, i).wait_send()

        @pl.when(zs != tp)
        def _():
            fin_copy(zs, tp).wait_send()
    for k in range(1, ntp):
        res_copy(k).wait_send()
        row_copy(k).wait_send()


def paired_call(nsp, ntp, residual, lifted, dts, long_rate, short_rate, emitted, raising):
    n, W = lifted.shape
    G = dts.shape[0]
    half = G // 2
    PL, PS = long_rate.shape[2], short_rate.shape[2]
    S = half * (PL + PS)
    D = emitted.shape[1]
    Dl = residual.shape[1]
    q = n // ntp
    Z, X, Y = mesh_split(nsp, ntp)
    Fz = raising.shape[1] // Z
    Dh = D // nsp // 2
    groups = 2 * Z
    cfg = (nsp, ntp, n, S, W, G, PL, PS, D, Fz)
    vm = pl.BlockSpec(memory_space=pltpu.VMEM)
    dma = pltpu.SemaphoreType.DMA
    return pl.pallas_call(
        functools.partial(paired_body, cfg),
        out_shape=jax.ShapeDtypeStruct((n, Dl), BF16),
        in_specs=[vm] * 11 + [pl.BlockSpec(memory_space=pl.ANY)] * 5,
        out_specs=vm,
        scratch_shapes=[
            pltpu.VMEM((8, half, CHAN, PL), F32), pltpu.VMEM((8, half, CHAN, PS), F32), dma((2, 8)),
            pltpu.VMEM((n, S), F32), pltpu.VMEM((n, S), F32),
            pltpu.VMEM((n, 4 * S), F32), pltpu.VMEM((n, 4 * S), F32),
            pltpu.VMEM((8, SUB, S), F32), pltpu.VMEM((2, 4, S), F32), pltpu.VMEM((2, nsp - 1, 4, S), F32),
            pltpu.VMEM((4, SUB, S), F32),
            pltpu.VMEM((ntp, q, W), BF16), pltpu.VMEM((ntp - 1, q, W), BF16),
            pltpu.VMEM((q, ntp * W), BF16), pltpu.VMEM(emitted.shape, BF16),
            pltpu.VMEM((ntp - 1, q, Dl), BF16),
            pltpu.VMEM((q, D), F32),
            pltpu.VMEM((2, nsp, 2, D // nsp // 2, Fz), BF16), pltpu.VMEM((2, nsp, 2, Fz, Dh), BF16),
            pltpu.VMEM((2, Z, q, D), BF16), pltpu.VMEM((2, 2 * Z * q, Fz), BF16),
            pltpu.VMEM((groups, Z, X, q, Dh), F32),
            *[pltpu.VMEM((groups, Z, X, q, Dh), BF16)] * 4,
            pltpu.VMEM((groups, 2, X, q, Dh), BF16), pltpu.VMEM((groups, X, q, Dh), BF16),
            pltpu.VMEM((ntp, q, Dl), BF16), pltpu.VMEM((ntp, q, Dl), BF16),
            dma((1,)), dma((2, 2)), *[dma((2, nsp - 1))] * 2, *[dma((ntp - 1,))] * 4,
            *[dma((2, 2, 4))] * 4, *[dma((2, 2, 4, 2))] * 2, *[dma((4,))] * 4,
            *[dma((groups,))] * 2, *[dma((2, groups))] * 2, dma((2, groups)), dma((groups,)),
            *[dma((ntp,))] * 2,
        ],
        compiler_params=pltpu.CompilerParams(collective_id=0, has_side_effects=True),
        cost_estimate=pl.CostEstimate(flops=10**9, bytes_accessed=3 * 10**7, transcendentals=10**6),
    )


def on_device(residual, lifted, dts, fades, long_rate, short_rate, long_freq, short_freq,
              long_lin, short_lin, skip, closing, emitted, leading, raising, lowering):
    nsp, ntp = lax.axis_size("sp"), lax.axis_size("tp")
    operands = (lifted, dts, fades, long_rate, short_rate, long_freq, short_freq, skip[None], closing[None],
                residual, leading[None], long_lin.swapaxes(4, 5), short_lin.swapaxes(4, 5), emitted, raising, lowering)
    Z, X, Y = mesh_split(nsp, ntp)
    if X == 2 and Y == 2 and Z == ntp:
        return paired_call(nsp, ntp, residual, lifted, dts, long_rate, short_rate, emitted, raising)(*operands)
    n, W = lifted.shape
    G = dts.shape[0]
    half = G // 2
    PL, PS = long_rate.shape[2], short_rate.shape[2]
    S = half * (PL + PS)
    D = emitted.shape[1]
    Dl = residual.shape[1]
    q = n // ntp
    c_ff = min(nsp, raising.shape[1] // 128)
    F = raising.shape[1] // c_ff
    q_all, M = c_ff * q, ntp // 2
    cfg = (nsp, ntp, n, S, W, G, PL, PS, D, c_ff, F)
    vm = pl.BlockSpec(memory_space=pltpu.VMEM)
    dma = pltpu.SemaphoreType.DMA
    return pl.pallas_call(
        functools.partial(mixer_body, cfg),
        out_shape=jax.ShapeDtypeStruct((n, Dl), BF16),
        in_specs=[vm] * 11 + [pl.BlockSpec(memory_space=pl.ANY)] * 5,
        out_specs=vm,
        scratch_shapes=[
            pltpu.VMEM((8, half, CHAN, PL), F32), pltpu.VMEM((8, half, CHAN, PS), F32), dma((2, 8)),
            pltpu.VMEM((n, S), F32), pltpu.VMEM((n, S), F32),
            pltpu.VMEM((n, 4 * S), F32), pltpu.VMEM((n, 4 * S), F32),
            pltpu.VMEM((8, SUB, S), F32), pltpu.VMEM((8, S), F32), pltpu.VMEM((nsp - 1, 8, S), F32),
            pltpu.VMEM((4, SUB, S), F32),
            pltpu.VMEM((ntp, q, W), BF16), pltpu.VMEM((ntp - 1, q, W), BF16),
            pltpu.VMEM((q, ntp * W), BF16), pltpu.VMEM(emitted.shape, BF16),
            pltpu.VMEM((ntp - 1, q, Dl), BF16),
            pltpu.VMEM((q, D), F32),
            pltpu.VMEM((ntp, nsp, D // nsp, F), BF16), pltpu.VMEM((ntp, nsp, F, D // nsp), BF16),
            pltpu.VMEM((c_ff, q, D), BF16), pltpu.VMEM((ntp, q_all, F), BF16),
            pltpu.VMEM((c_ff, q, D), BF16), pltpu.VMEM((c_ff - 1, q, D), BF16),
            pltpu.VMEM((ntp, q, Dl), BF16), pltpu.VMEM((ntp - 1, q, Dl), BF16),
            dma((3,)), dma((nsp - 1,)), dma((nsp - 1,)), dma((ntp - 1,)), dma((ntp - 1,)),
            dma((ntp - 1,)), dma((ntp - 1,)),
            *[dma((nsp - 1,))] * 4, *[dma((M - 1, nsp))] * 4, *[dma((M,))] * 4,
            *[dma((2, c_ff // 2))] * 2, *[dma((c_ff - 1,))] * 2, *[dma((ntp - 1,))] * 2,
        ],
        compiler_params=pltpu.CompilerParams(collective_id=0, has_side_effects=True),
        cost_estimate=pl.CostEstimate(flops=10**9, bytes_accessed=3 * 10**7, transcendentals=10**6),
    )(*operands)


def solution(mesh):
    both, swapped = P("sp", "tp"), P("tp", "sp")
    in_specs = (both, both, swapped, swapped) + (P(),) * 10 + (both, swapped)
    return jax.shard_map(on_device, mesh=mesh, in_specs=in_specs, out_specs=both, check_vma=False)
```

```python
import functools

import jax
import jax.numpy as jnp
from jax import lax
from jax.experimental import pallas as pl
from jax.experimental.pallas import tpu as pltpu
from jax.sharding import PartitionSpec as P

CHAN = 16
NORM_W = 128
EPSILON = 1e-06
SUB = 8
F32, BF16 = jnp.float32, jnp.bfloat16


def sincos(a):
    k = jnp.floor(a * 0.6366197723675814 + 0.5)
    r = a - k * 1.5703125
    r = r - k * 4.8351287841796875e-4
    r = r - k * 3.138556210e-7
    z = r * r
    s = r + r * z * (-1.6666654611e-1 + z * (8.3321608736e-3 + z * -1.9515295891e-4))
    c = 1.0 - 0.5 * z + z * z * (
        4.166664568298827e-2 + z * (-1.388731625493765e-3 + z * 2.443315711809948e-5)
    )
    half = jnp.floor(k * 0.5)
    odd = (k - 2.0 * half) > 0.5
    half_odd = (half - 2.0 * jnp.floor(half * 0.5)) > 0.5
    cos_v = jnp.where(odd, -s, c)
    sin_v = jnp.where(odd, c, s)
    return jnp.where(half_odd, -cos_v, cos_v), jnp.where(half_odd, -sin_v, sin_v)


def one_minus_exp_neg(u):
    t = jnp.full_like(u, 1.0)
    for m in range(10, 1, -1):
        t = 1.0 - u * (1.0 / m) * t
    return u * t


def cmul(ar, ai, br, bi):
    return ar * br - ai * bi, ar * bi + ai * br


def mixer_body(cfg, x_ref, dt_ref, lf_ref, long_rate, short_rate, long_freq, short_freq,
               skip_ref, gain_ref, resid_ref, lead_ref, long_hbm, short_hbm, emit_hbm, up_hbm, down_hbm,
               out_ref, lin_l, lin_s, lin_sem,
               pace, surge, pre, st, blk, ends, ends_all, cin, mg, rows_in, mrg, emit, resid_in,
               mid_out, wup, wdn, nrm, hid, part, rs_in, fin, fin_in,
               copy_sem, s_ends, r_ends, s_rows, r_rows, s_res, r_res,
               s_u1, r_u1, s_d1, r_d1, s_u2, r_u2, s_d2, r_d2, s_u3, r_u3, s_d3, r_d3,
               s_nrm, r_nrm, s_rs, r_rs, s_fin, r_fin):
    nsp, ntp, n, S, W, G, PL, PS, D, c_ff, F = cfg
    M = ntp // 2
    L = n // SUB
    half = G // 2
    SL = half * PL
    sp = lax.axis_index("sp")
    tp = lax.axis_index("tp")
    q = n // ntp
    Dl = D // ntp
    MESH = pl.DeviceIdType.MESH

    emit_copy = pltpu.make_async_copy(emit_hbm, emit, copy_sem.at[0])
    lin_copies = []
    for at in range(8):
        for kind, (src, dst) in enumerate(((long_hbm, lin_l), (short_hbm, lin_s))):
            lin_copies.append(pltpu.make_async_copy(
                src.at[at // 4, at // 2 % 2, at % 2, pl.ds(tp * half, half)], dst.at[at],
                lin_sem.at[kind, at]))
    for copy in lin_copies:
        copy.start()
    emit_copy.start()
    chunk = lax.rem(sp, c_ff)
    partner = tp + 1 - 2 * lax.rem(tp, 2)

    def cols(of):
        return pl.ds(pl.multiple_of(of * F, 128), F)

    own_up = pltpu.make_async_copy(up_hbm.at[:, cols(chunk)], wup.at[tp, sp], copy_sem.at[1])
    own_down = pltpu.make_async_copy(down_hbm.at[cols(chunk), :], wdn.at[tp, sp], copy_sem.at[2])
    own_up.start()
    own_down.start()

    def spread_copy(k, up):
        to = lax.rem(sp + k, nsp)
        src = up_hbm.at[:, cols(lax.rem(to, c_ff))] if up else down_hbm.at[cols(lax.rem(to, c_ff)), :]
        return pltpu.make_async_remote_copy(
            src_ref=src, dst_ref=(wup if up else wdn).at[tp, sp],
            send_sem=(s_u1 if up else s_d1).at[k - 1], recv_sem=(r_u1 if up else r_d1).at[k - 1],
            device_id=(to, tp), device_id_type=MESH)

    def across_copy(m, k, up):
        piece = (wup if up else wdn).at[tp, lax.rem(sp - k + nsp, nsp)]
        return pltpu.make_async_remote_copy(
            src_ref=piece, dst_ref=piece,
            send_sem=(s_u2 if up else s_d2).at[m - 1, k], recv_sem=(r_u2 if up else r_d2).at[m - 1, k],
            device_id=(sp, lax.rem(tp + 2 * m, ntp)), device_id_type=MESH)

    def pair_copy(m, up):
        piece = (wup if up else wdn).at[lax.rem(tp + 2 * m, ntp)]
        return pltpu.make_async_remote_copy(
            src_ref=piece, dst_ref=piece,
            send_sem=(s_u3 if up else s_d3).at[m], recv_sem=(r_u3 if up else r_d3).at[m],
            device_id=(sp, partner), device_id_type=MESH)

    def pass_on(first, last, up):
        for k in range(first, last):
            if k == 0:
                (own_up if up else own_down).wait()
            else:
                spread_copy(k, up).wait_recv()
            for m in range(1, M):
                across_copy(m, k, up).start()

    barrier = pltpu.get_barrier_semaphore()
    for k in range(1, nsp):
        pl.semaphore_signal(barrier, inc=1, device_id=(lax.rem(sp + k, nsp), tp), device_id_type=MESH)
    for k in range(1, ntp):
        pl.semaphore_signal(barrier, inc=1, device_id=(sp, lax.rem(tp + k, ntp)), device_id_type=MESH)
    pl.semaphore_wait(barrier, nsp + ntp - 2)

    def res_copy(k):
        to = lax.rem(tp + k, ntp)
        return pltpu.make_async_remote_copy(
            src_ref=resid_ref.at[pl.ds(to * q, q), :], dst_ref=resid_in.at[k - 1],
            send_sem=s_res.at[k - 1], recv_sem=r_res.at[k - 1],
            device_id=(sp, to), device_id_type=MESH)

    for k in range(1, nsp):
        spread_copy(k, True).start()
    for k in range(1, ntp):
        res_copy(k).start()

    lane = lax.broadcasted_iota(jnp.int32, (G, S), 1)
    group = jnp.where(lane < SL, 2 * (lane // PL), 2 * ((lane - SL) // PS) + 1)
    spread = (group == lax.broadcasted_iota(jnp.int32, (G, S), 0)).astype(F32)
    r = lax.broadcasted_iota(jnp.int32, (n, n), 0)
    t = lax.broadcasted_iota(jnp.int32, (n, n), 1)
    mix = (t == (r % SUB) * L + r // SUB).astype(F32)

    def per_state(ref):
        moved = lax.dot_general(ref[...], mix, (((1,), (1,)), ((), ())),
                                precision=lax.Precision.HIGHEST, preferred_element_type=F32)
        return lax.dot_general(moved, spread, (((0,), (0,)), ((), ())),
                               precision=lax.Precision.HIGHEST, preferred_element_type=F32)

    pace[...] = per_state(dt_ref)
    surge[...] = per_state(lf_ref)

    def flat_kind(ref, e):
        many, states = ref.shape[1:]
        width = half * states
        repeat = (lax.broadcasted_iota(jnp.int32, (states, width), 1) % states
                  == lax.broadcasted_iota(jnp.int32, (states, width), 0)).astype(F32)
        wide = jnp.dot(ref[e], repeat, precision=lax.Precision.HIGHEST, preferred_element_type=F32)
        owner = tp * half + lax.broadcasted_iota(jnp.int32, (many, width), 1) // states
        mine = owner == lax.broadcasted_iota(jnp.int32, (many, width), 0)
        return jnp.sum(jnp.where(mine, wide, 0.0), axis=0, keepdims=True)

    def flat(long_ref, short_ref, e):
        return jnp.concatenate([flat_kind(long_ref, e), flat_kind(short_ref, e)], axis=1)

    def widened(ref, index, states, sign):
        rows, width = half * CHAN, half * states
        repeat = (lax.broadcasted_iota(jnp.int32, (states, width), 1) % states
                  == lax.broadcasted_iota(jnp.int32, (states, width), 0)).astype(BF16)
        wide = jnp.dot(ref[index].reshape(rows, states).astype(BF16), repeat, preferred_element_type=F32)
        own_block = (lax.broadcasted_iota(jnp.int32, (rows, width), 0) // CHAN
                     == lax.broadcasted_iota(jnp.int32, (rows, width), 1) // states)
        return jnp.where(own_block, sign * wide, 0.0).astype(BF16)

    def block_map(index, sign=1.0):
        long_part = widened(lin_l, index, PL, sign)
        short_part = widened(lin_s, index, PS, sign)
        no_long, no_short = jnp.zeros((CHAN, SL), BF16), jnp.zeros((CHAN, S - SL), BF16)
        bands = []
        for g in range(half):
            band = slice(g * CHAN, (g + 1) * CHAN)
            bands.append(jnp.concatenate([long_part[band], no_short], axis=1))
            bands.append(jnp.concatenate([no_long, short_part[band]], axis=1))
        return jnp.concatenate(bands, axis=0)

    xv = jnp.dot(mix.astype(BF16), x_ref[...], preferred_element_type=F32).astype(BF16)
    for copy in lin_copies:
        copy.wait()
    for e in range(2):
        for c in range(2):
            st[:, pl.ds((2 * e + c) * S, S)] = jnp.dot(
                xv, block_map(4 * e + c), preferred_element_type=F32)

    for e in range(2):
        rate = flat(long_rate, short_rate, e)
        freq = flat(long_freq, short_freq, e)

        def step(i, carry):
            pr, pi, sr, si = carry
            at = i if e == 0 else L - 1 - i
            rows = pl.ds(pl.multiple_of(at * SUB, SUB), SUB)
            d = pace[rows, :]
            rd = rate * d
            m = jnp.exp(surge[rows, :] - rd)
            cos_v, sin_v = sincos(freq * d)
            w = jnp.sqrt(one_minus_exp_neg(2.0 * rd))
            ar, ai = m * cos_v, m * sin_v
            pr, pi = cmul(ar, ai, pr, pi)
            sr, si = cmul(ar, ai, sr, si)
            sr = sr + w * st[rows, pl.ds(2 * e * S, S)]
            si = si + w * st[rows, pl.ds((2 * e + 1) * S, S)]
            pre[rows, pl.ds(2 * e * S, S)] = pr
            pre[rows, pl.ds((2 * e + 1) * S, S)] = pi
            st[rows, pl.ds(2 * e * S, S)] = sr
            st[rows, pl.ds((2 * e + 1) * S, S)] = si
            return pr, pi, sr, si

        zero = jnp.zeros((SUB, S), F32)
        total = lax.fori_loop(0, L, step, (zero + 1.0, zero, zero, zero))
        for c in range(4):
            blk[4 * e + c] = total[c]
        order = range(SUB) if e == 0 else range(SUB - 1, -1, -1)
        run = None
        for b in order:
            now = tuple(blk[4 * e + c, b : b + 1, :] for c in range(4))
            if run is None:
                run = now
            else:
                p = cmul(now[0], now[1], run[0], run[1])
                s = cmul(now[0], now[1], run[2], run[3])
                run = (p[0], p[1], s[0] + now[2], s[1] + now[3])
        for c in range(4):
            ends[4 * e + c : 4 * e + c + 1, :] = run[c]

    def ends_copy(k):
        return pltpu.make_async_remote_copy(
            src_ref=ends, dst_ref=ends_all.at[k - 1],
            send_sem=s_ends.at[k - 1], recv_sem=r_ends.at[k - 1],
            device_id=(lax.rem(sp + k, nsp), tp), device_id_type=MESH)

    for k in range(1, nsp):
        ends_copy(k).start()
    for k in range(1, nsp):
        spread_copy(k, False).start()

    read = jnp.concatenate(
        [block_map(2), block_map(3, -1.0), block_map(6), block_map(7, -1.0)], axis=1)

    pass_on(0, nsp // 2, True)
    for k in range(1, nsp):
        ends_copy(k).wait_recv()
    blank = jnp.zeros((1, S), F32)

    def fold(j, carry, e):
        cr, ci = carry
        k = nsp - 1 - j if e == 0 else j + 1
        reached = k <= sp if e == 0 else nsp - k <= nsp - 1 - sp
        got = ends_all[k - 1]
        nr, ni = cmul(got[4 * e : 4 * e + 1], got[4 * e + 1 : 4 * e + 2], cr, ci)
        nr = nr + got[4 * e + 2 : 4 * e + 3]
        ni = ni + got[4 * e + 3 : 4 * e + 4]
        return jnp.where(reached, nr, cr), jnp.where(reached, ni, ci)

    for e in range(2):
        cr, ci = lax.fori_loop(0, nsp - 1, functools.partial(fold, e=e), (blank, blank))
        order = range(SUB) if e == 0 else range(SUB - 1, -1, -1)
        for b in order:
            cin[2 * e, b : b + 1, :] = cr
            cin[2 * e + 1, b : b + 1, :] = ci
            now = tuple(blk[4 * e + c, b : b + 1, :] for c in range(4))
            nr, ni = cmul(now[0], now[1], cr, ci)
            cr, ci = nr + now[2], ni + now[3]

        inr, ini = cin[2 * e], cin[2 * e + 1]

        def settle(i, _):
            rows = pl.ds(pl.multiple_of(i * SUB, SUB), SUB)
            re, im = pl.ds(2 * e * S, S), pl.ds((2 * e + 1) * S, S)
            ar, ai = cmul(pre[rows, re], pre[rows, im], inr, ini)
            st[rows, re] = st[rows, re] + ar
            st[rows, im] = st[rows, im] + ai
            return 0

        lax.fori_loop(0, L, settle, 0)

    y = lax.dot_general(st[...].astype(BF16), read, (((1,), (1,)), ((), ())),
                        preferred_element_type=F32)
    own = pl.ds(pl.multiple_of(tp * W, 128), W)
    skip_row, gain_row = skip_ref[:, own], gain_ref[:, own]
    y = y + skip_row * xv.astype(F32)
    y = 0.5 * y * (1.0 + jnp.tanh(0.7978845608028654 * (y + 0.044715 * y * y * y)))
    heads = []
    for h in range(W // NORM_W):
        head = y[:, h * NORM_W : (h + 1) * NORM_W]
        scale = lax.rsqrt(jnp.mean(head * head, axis=1, keepdims=True) + EPSILON)
        heads.append(head * scale * gain_row[:, h * NORM_W : (h + 1) * NORM_W])
    merged = jnp.concatenate(heads, axis=1).astype(BF16)
    t = lax.broadcasted_iota(jnp.int32, (n, n), 0)
    r = lax.broadcasted_iota(jnp.int32, (n, n), 1)
    unmix = (r == (t % L) * SUB + t // L).astype(BF16)
    mg[...] = jnp.dot(unmix, merged, preferred_element_type=F32).astype(BF16).reshape(ntp, q, W)

    def row_copy(k):
        to = lax.rem(tp + k, ntp)
        return pltpu.make_async_remote_copy(
            src_ref=mg.at[to], dst_ref=rows_in.at[k - 1],
            send_sem=s_rows.at[k - 1], recv_sem=r_rows.at[k - 1],
            device_id=(sp, to), device_id_type=MESH)

    for k in range(1, ntp):
        row_copy(k).start()
    pass_on(nsp // 2, nsp, True)
    emit_copy.wait()
    mrg[:, pl.ds(pl.multiple_of(tp * W, 128), W)] = mg[tp]
    mid_out[:, pl.ds(pl.multiple_of(tp * Dl, 128), Dl)] = resid_ref[pl.ds(pl.multiple_of(tp * q, q), q), :].astype(F32)
    for k in range(1, ntp):
        src = lax.rem(tp - k + ntp, ntp)
        res_copy(k).wait_recv()
        mid_out[:, pl.ds(pl.multiple_of(src * Dl, 128), Dl)] = resid_in[k - 1].astype(F32)
        row_copy(k).wait_recv()
        mrg[:, pl.ds(pl.multiple_of(src * W, 128), W)] = rows_in[k - 1]
    mid = mid_out[...] + jnp.dot(mrg[...], emit[...], preferred_element_type=F32)
    mid_out[...] = mid
    scale = lax.rsqrt(jnp.mean(mid * mid, axis=1, keepdims=True) + EPSILON)
    base, q_all = sp - chunk, c_ff * q
    nrm[chunk] = (mid * scale * lead_ref[...]).astype(BF16)

    def peer(k):
        return lax.rem(chunk + k, c_ff)

    H = c_ff // 2

    def nrm_across(m):
        return pltpu.make_async_remote_copy(
            src_ref=nrm.at[chunk], dst_ref=nrm.at[chunk],
            send_sem=s_nrm.at[0, m], recv_sem=r_nrm.at[0, m],
            device_id=(base + peer(2 * m), tp), device_id_type=MESH)

    def nrm_pair(m):
        return pltpu.make_async_remote_copy(
            src_ref=nrm.at[peer(2 * m)], dst_ref=nrm.at[peer(2 * m)],
            send_sem=s_nrm.at[1, m], recv_sem=r_nrm.at[1, m],
            device_id=(base + chunk + 1 - 2 * lax.rem(chunk, 2), tp), device_id_type=MESH)

    def rs_copy(k):
        return pltpu.make_async_remote_copy(
            src_ref=part.at[peer(k)], dst_ref=rs_in.at[k - 1],
            send_sem=s_rs.at[k - 1], recv_sem=r_rs.at[k - 1],
            device_id=(base + peer(k), tp), device_id_type=MESH)

    def fin_copy(k):
        to = lax.rem(tp + k, ntp)
        return pltpu.make_async_remote_copy(
            src_ref=fin.at[to], dst_ref=fin_in.at[k - 1],
            send_sem=s_fin.at[k - 1], recv_sem=r_fin.at[k - 1],
            device_id=(sp, to), device_id_type=MESH)

    for m in range(1, H):
        nrm_across(m).start()
    nrm_pair(0).start()
    pair_copy(0, True).start()
    pass_on(0, nsp, False)
    pair_copy(0, False).start()
    for m in range(1, H):
        nrm_across(m).wait_recv()
        nrm_pair(H - m).start()
    for up in (True, False):
        for m in range(1, M):
            for k in range(nsp):
                across_copy(m, k, up).wait_recv()
            pair_copy(M - m, up).start()
        if up:
            for m in range(M):
                pair_copy(m, True).wait_recv()
            for m in range(H):
                nrm_pair(m).wait_recv()
            rows = nrm[...].reshape(q_all, D)

            def raise_step(t, _):
                upward = jnp.dot(rows, wup[t].reshape(D, F), preferred_element_type=F32)
                hid[t] = jnp.square(jnp.maximum(upward, 0.0)).astype(BF16)
                return 0

            lax.fori_loop(0, ntp, raise_step, 0)
    for m in range(M):
        pair_copy(m, False).wait_recv()
    Dc = D // nsp
    for j in range(nsp):
        total = jnp.dot(hid[0], wdn[0, j], preferred_element_type=F32)
        for t in range(1, ntp):
            total = total + jnp.dot(hid[t], wdn[t, j], preferred_element_type=F32)
        part[:, :, j * Dc : (j + 1) * Dc] = total.astype(BF16).reshape(c_ff, q, Dc)
    for k in range(1, c_ff):
        rs_copy(k).start()
    result = mid_out[...] + part[chunk].astype(F32)
    for k in range(1, c_ff):
        rs_copy(k).wait_recv()
        result = result + rs_in[k - 1].astype(F32)
    result = result.astype(BF16)
    for t in range(ntp):
        fin[t] = result[:, t * Dl : (t + 1) * Dl]
    for k in range(1, ntp):
        fin_copy(k).start()
    out_ref[pl.ds(pl.multiple_of(tp * q, q), q), :] = fin[tp]
    for k in range(1, ntp):
        fin_copy(k).wait_recv()
        src = lax.rem(tp - k + ntp, ntp)
        out_ref[pl.ds(pl.multiple_of(src * q, q), q), :] = fin_in[k - 1]
    for k in range(1, c_ff):
        rs_copy(k).wait_send()
    for m in range(H):
        if m > 0:
            nrm_across(m).wait_send()
        nrm_pair(m).wait_send()
    for k in range(1, ntp):
        fin_copy(k).wait_send()
    for up in (True, False):
        for k in range(1, nsp):
            spread_copy(k, up).wait_send()
        for m in range(1, M):
            for k in range(nsp):
                across_copy(m, k, up).wait_send()
        for m in range(M):
            pair_copy(m, up).wait_send()
    for k in range(1, nsp):
        ends_copy(k).wait_send()
    for k in range(1, ntp):
        res_copy(k).wait_send()
        row_copy(k).wait_send()


def mesh_split(nsp, ntp):
    Y = ntp // 2
    X = Y if Y > 0 and nsp % Y == 0 else 1
    return nsp // X, X, Y


def paired_body(cfg, x_hbm, dt_hbm, lf_hbm, long_rate_hbm, short_rate_hbm, long_freq_hbm, short_freq_hbm,
                skip_hbm, gain_hbm, resid_hbm, lead_hbm, long_hbm, short_hbm, emit_hbm, up_hbm, down_hbm,
                out_ref, x_ref, dt_ref, lf_ref, long_rate, short_rate, long_freq, short_freq,
                skip_ref, gain_ref, resid_ref, lead_ref, in_sem, lin_l, lin_s, lin_sem,
                pace, surge, pre, st, blk, ends, ends_all, cin, mg, rows_in, mrg, emit, resid_in,
                mid_out, wup, wdn, nrm, hid, loc, a_out, a_in, b_out, b_in, c_out, c_in, home_in,
                copy_sem, own_sem, s_ends, r_ends, s_rows, r_rows, s_res, r_res,
                s_z, r_z, s_x, r_x, s_d, r_d_up, r_d_down, s_t, r_t, s_y, r_y,
                s_a, r_a, s_b, r_b, s_c, r_c, s_last, s_home, r_home):
    nsp, ntp, n, S, W, G, PL, PS, D, Fz = cfg
    Z, X, Y = mesh_split(nsp, ntp)
    L = n // SUB
    half = G // 2
    SL = half * PL
    sp = lax.axis_index("sp")
    tp = lax.axis_index("tp")
    q = n // ntp
    Dl = D // ntp
    Dh = D // nsp // 2
    Rh = D // nsp // 2
    MESH = pl.DeviceIdType.MESH
    z, x, y, c = sp // X, lax.rem(sp, X), tp // 2, lax.rem(tp, 2)
    side = z // 2
    half_in, half_out = 1 + side, 3 * side
    far_in, far_out = 2 - side, 3 - 3 * side
    far0 = 2 - 2 * side
    mate = z + 1 - 2 * lax.rem(z, 2)
    inner, outer = z == half_in, z == half_out
    kinds = (z, mate, far_in, far_out)
    as_seen = 2 + jnp.where(outer, 1, 0)

    def dev(z_, x_, y_, c_):
        return (z_ * X + x_, y_ * 2 + c_)

    x_mate, y_mate, c_mate = dev(z, 1 - x, y, c), dev(z, x, 1 - y, c), dev(z, x, y, 1 - c)

    def remote(src, dst, ssem, rsem, to):
        return pltpu.make_async_remote_copy(src_ref=src, dst_ref=dst, send_sem=ssem, recv_sem=rsem,
                                            device_id=to, device_id_type=MESH)

    in_copies = [pltpu.make_async_copy(src, dst, in_sem.at[at]) for at, (src, dst) in enumerate((
        (dt_hbm, dt_ref), (lf_hbm, lf_ref), (x_hbm, x_ref), (long_rate_hbm, long_rate), (short_rate_hbm, short_rate),
        (long_freq_hbm, long_freq), (short_freq_hbm, short_freq), (skip_hbm, skip_ref), (gain_hbm, gain_ref),
        (lead_hbm, lead_ref), (resid_hbm.at[pl.ds(pl.multiple_of(tp * q, q), q), :], resid_ref)))]
    emit_copy = pltpu.make_async_copy(emit_hbm, emit, copy_sem.at[0])
    lin_copies = []
    for at in range(8):
        for kind, (src, dst) in enumerate(((long_hbm, lin_l), (short_hbm, lin_s))):
            lin_copies.append(pltpu.make_async_copy(
                src.at[at // 4, at // 2 % 2, at % 2, pl.ds(tp * half, half)], dst.at[at], lin_sem.at[kind]))

    def sent(ref, sem):
        remote(ref, ref, sem, sem, c_mate).wait_send()

    def came(ref, sem):
        remote(ref, ref, sem, sem, c_mate).wait_recv()

    def bank(up):
        return wup if up else wdn

    def shard(up, h, to):
        part = pl.ds(pl.multiple_of(to * Fz, 128), Fz)
        if up:
            return up_hbm.at[pl.ds(h * Rh, Rh), part]
        return down_hbm.at[part, pl.ds(h * Dh, Dh)]

    def own_copy(up, h):
        return pltpu.make_async_copy(shard(up, h, z), bank(up).at[c, sp, h], own_sem.at[1 - up])

    def own_wait(up):
        pltpu.make_async_copy(bank(up).at[c, sp], bank(up).at[c, sp], own_sem.at[1 - up]).wait()

    def z_copy(up, h, k):
        to = kinds[k]
        return remote(shard(up, h, to), bank(up).at[c, sp, h], s_z.at[0],
                      r_z.at[1 - up, h, 0 if k == 1 else as_seen - 1], dev(to, x, y, c))

    def x_copy(up, h, k):
        piece = bank(up).at[c, kinds[k] * X + x, h]
        return remote(shard(up, h, z) if k == 0 else piece, piece, s_x.at[0], r_x.at[1 - up, h, k], x_mate)

    def d_copy(up, h, k, other):
        piece = bank(up).at[c, kinds[k] * X + (1 - x if other else x), h]
        return remote(shard(up, h, z) if k == 0 and not other else piece, piece, s_d.at[0],
                      r_d_up.at[0] if up else r_d_down.at[0 if k < 2 else 1 + (k - 2) * 2 + h], c_mate)

    def hop1(up, h, k):
        came(bank(up).at[c, kinds[k] * X + x, h], r_z.at[1 - up, h, k - 1])
        x_copy(up, h, k).start()
        d_copy(up, h, k, 0).start()

    def hop2(up, h, k):
        x_copy(up, h, k).wait_recv()
        d_copy(up, h, k, 1).start()

    def hop3_up():
        came(wup.at[1 - c], r_d_up.at[0])

    def hop3_near():
        came(wdn.at[1 - c, pl.ds(side * 2 * X, 2 * X)], r_d_down.at[0])

    def hop3_far(h, k):
        came(wdn.at[1 - c, kinds[k] * X], r_d_down.at[1 + (k - 2) * 2 + h])

    def res_copy(k):
        to = lax.rem(tp + k, ntp)
        return remote(resid_hbm.at[pl.ds(pl.multiple_of(to * q, q), q), :], resid_in.at[k - 1], s_res.at[0],
                      r_res.at[0], (sp, to))

    barrier = pltpu.get_barrier_semaphore()
    for k in range(1, nsp):
        pl.semaphore_signal(barrier, inc=1, device_id=(lax.rem(sp + k, nsp), tp), device_id_type=MESH)
    for k in range(1, ntp):
        pl.semaphore_signal(barrier, inc=1, device_id=(sp, lax.rem(tp + k, ntp)), device_id_type=MESH)
    for copy in in_copies + lin_copies:
        copy.start()

    pl.semaphore_wait(barrier, nsp + ntp - 2)

    @pl.when(outer)
    def _():
        for k in (2, 3):
            z_copy(1, 0, k).start()

    @pl.when(inner)
    def _():
        z_copy(1, 0, 1).start()

    for h in range(2):
        x_copy(1, h, 0).start()
        d_copy(1, h, 0, 0).start()
    for k in range(1, ntp):
        res_copy(k).start()
    emit_copy.start()
    for up in (1, 0):
        for h in range(2):
            own_copy(up, h).start()

    lane = lax.broadcasted_iota(jnp.int32, (G, S), 1)
    group = jnp.where(lane < SL, 2 * (lane // PL), 2 * ((lane - SL) // PS) + 1)
    spread = (group == lax.broadcasted_iota(jnp.int32, (G, S), 0)).astype(F32)
    r = lax.broadcasted_iota(jnp.int32, (n, n), 0)
    t = lax.broadcasted_iota(jnp.int32, (n, n), 1)
    mix = (t == (r % SUB) * L + r // SUB).astype(F32)

    def per_state(ref):
        moved = lax.dot_general(ref[...], mix, (((1,), (1,)), ((), ())),
                                precision=lax.Precision.HIGHEST, preferred_element_type=F32)
        return lax.dot_general(moved, spread, (((0,), (0,)), ((), ())),
                               precision=lax.Precision.HIGHEST, preferred_element_type=F32)

    for copy in in_copies[:2]:
        copy.wait()
    pace[...] = per_state(dt_ref)
    surge[...] = per_state(lf_ref)

    def flat_kind(ref, e):
        many, states = ref.shape[1:]
        width = half * states
        repeat = (lax.broadcasted_iota(jnp.int32, (states, width), 1) % states
                  == lax.broadcasted_iota(jnp.int32, (states, width), 0)).astype(F32)
        wide = jnp.dot(ref[e], repeat, precision=lax.Precision.HIGHEST, preferred_element_type=F32)
        owner = tp * half + lax.broadcasted_iota(jnp.int32, (many, width), 1) // states
        mine = owner == lax.broadcasted_iota(jnp.int32, (many, width), 0)
        return jnp.sum(jnp.where(mine, wide, 0.0), axis=0, keepdims=True)

    def flat(long_ref, short_ref, e):
        return jnp.concatenate([flat_kind(long_ref, e), flat_kind(short_ref, e)], axis=1)

    def widened(ref, index, states, sign):
        rows, width = half * CHAN, half * states
        repeat = (lax.broadcasted_iota(jnp.int32, (states, width), 1) % states
                  == lax.broadcasted_iota(jnp.int32, (states, width), 0)).astype(BF16)
        wide = jnp.dot(ref[index].reshape(rows, states).astype(BF16), repeat, preferred_element_type=F32)
        own_block = (lax.broadcasted_iota(jnp.int32, (rows, width), 0) // CHAN
                     == lax.broadcasted_iota(jnp.int32, (rows, width), 1) // states)
        return jnp.where(own_block, sign * wide, 0.0).astype(BF16)

    def block_map(index, sign=1.0):
        long_part = widened(lin_l, index, PL, sign)
        short_part = widened(lin_s, index, PS, sign)
        no_long, no_short = jnp.zeros((CHAN, SL), BF16), jnp.zeros((CHAN, S - SL), BF16)
        bands = []
        for g in range(half):
            band = slice(g * CHAN, (g + 1) * CHAN)
            bands.append(jnp.concatenate([long_part[band], no_short], axis=1))
            bands.append(jnp.concatenate([no_long, short_part[band]], axis=1))
        return jnp.concatenate(bands, axis=0)

    for copy in in_copies[2:]:
        copy.wait()
    xv = jnp.dot(mix.astype(BF16), x_ref[...], preferred_element_type=F32).astype(BF16)
    for kind, ref in enumerate((lin_l, lin_s)):
        pltpu.make_async_copy(ref, ref, lin_sem.at[kind]).wait()
    for e in range(2):
        for part in range(2):
            st[:, pl.ds((2 * e + part) * S, S)] = jnp.dot(
                xv, block_map(4 * e + part), preferred_element_type=F32)

    for e in range(2):
        rate = flat(long_rate, short_rate, e)
        freq = flat(long_freq, short_freq, e)

        def step(i, carry):
            pr, pi, sr, si = carry
            at = i if e == 0 else L - 1 - i
            rows = pl.ds(pl.multiple_of(at * SUB, SUB), SUB)
            d = pace[rows, :]
            rd = rate * d
            m = jnp.exp(surge[rows, :] - rd)
            cos_v, sin_v = sincos(freq * d)
            w = jnp.sqrt(one_minus_exp_neg(2.0 * rd))
            ar, ai = m * cos_v, m * sin_v
            pr, pi = cmul(ar, ai, pr, pi)
            sr, si = cmul(ar, ai, sr, si)
            sr = sr + w * st[rows, pl.ds(2 * e * S, S)]
            si = si + w * st[rows, pl.ds((2 * e + 1) * S, S)]
            pre[rows, pl.ds(2 * e * S, S)] = pr
            pre[rows, pl.ds((2 * e + 1) * S, S)] = pi
            st[rows, pl.ds(2 * e * S, S)] = sr
            st[rows, pl.ds((2 * e + 1) * S, S)] = si
            return pr, pi, sr, si

        zero = jnp.zeros((SUB, S), F32)
        total = lax.fori_loop(0, L, step, (zero + 1.0, zero, zero, zero))
        for part in range(4):
            blk[4 * e + part] = total[part]
        order = range(SUB) if e == 0 else range(SUB - 1, -1, -1)
        run = None
        for b in order:
            now = tuple(blk[4 * e + part, b : b + 1, :] for part in range(4))
            if run is None:
                run = now
            else:
                p = cmul(now[0], now[1], run[0], run[1])
                s = cmul(now[0], now[1], run[2], run[3])
                run = (p[0], p[1], s[0] + now[2], s[1] + now[3])
        for part in range(4):
            ends[e, part : part + 1, :] = run[part]

    def ends_copy(e, k):
        return remote(ends.at[e], ends_all.at[e, k - 1], s_ends.at[0], r_ends.at[0],
                      (sp + k if e == 0 else sp - k, tp))

    def has_after(e, k):
        return sp + k < nsp if e == 0 else sp >= k

    def has_before(e, k):
        return has_after(1 - e, k)

    for k in range(1, nsp):
        for e in range(2):
            @pl.when(has_after(e, k))
            def _():
                ends_copy(e, k).start()

    @pl.when(inner)
    def _():
        for k in (2, 3):
            z_copy(1, 0, k).start()
        z_copy(1, 1, 1).start()

    @pl.when(outer)
    def _():
        for h in range(2):
            z_copy(1, h, 1).start()
        for k in (2, 3):
            z_copy(1, 1, k).start()
        hop1(1, 0, 1)

    read = jnp.concatenate(
        [block_map(2), block_map(3, -1.0), block_map(6), block_map(7, -1.0)], axis=1)

    came(ends_all.at[0], r_ends.at[0])
    blank = jnp.zeros((1, S), F32)

    def fold(j, carry, e):
        cr, ci = carry
        k = nsp - 1 - j
        got = ends_all[e, k - 1]
        nr, ni = cmul(got[0:1], got[1:2], cr, ci)
        reached = has_before(e, k)
        return jnp.where(reached, nr + got[2:3], cr), jnp.where(reached, ni + got[3:4], ci)

    for e in range(2):
        cr, ci = lax.fori_loop(0, nsp - 1, functools.partial(fold, e=e), (blank, blank))
        order = range(SUB) if e == 0 else range(SUB - 1, -1, -1)
        for b in order:
            cin[2 * e, b : b + 1, :] = cr
            cin[2 * e + 1, b : b + 1, :] = ci
            now = tuple(blk[4 * e + part, b : b + 1, :] for part in range(4))
            nr, ni = cmul(now[0], now[1], cr, ci)
            cr, ci = nr + now[2], ni + now[3]

        inr, ini = cin[2 * e], cin[2 * e + 1]

        def settle(i, _):
            rows = pl.ds(pl.multiple_of(i * SUB, SUB), SUB)
            re, im = pl.ds(2 * e * S, S), pl.ds((2 * e + 1) * S, S)
            ar, ai = cmul(pre[rows, re], pre[rows, im], inr, ini)
            st[rows, re] = st[rows, re] + ar
            st[rows, im] = st[rows, im] + ai
            return 0

        lax.fori_loop(0, L, settle, 0)

    v = lax.dot_general(st[...].astype(BF16), read, (((1,), (1,)), ((), ())),
                        preferred_element_type=F32)
    own = pl.ds(pl.multiple_of(tp * W, 128), W)
    skip_row, gain_row = skip_ref[:, own], gain_ref[:, own]
    v = v + skip_row * xv.astype(F32)
    v = 0.5 * v * (1.0 + jnp.tanh(0.7978845608028654 * (v + 0.044715 * v * v * v)))
    heads = []
    for h in range(W // NORM_W):
        head = v[:, h * NORM_W : (h + 1) * NORM_W]
        scale = lax.rsqrt(jnp.mean(head * head, axis=1, keepdims=True) + EPSILON)
        heads.append(head * scale * gain_row[:, h * NORM_W : (h + 1) * NORM_W])
    merged = jnp.concatenate(heads, axis=1).astype(BF16)
    t = lax.broadcasted_iota(jnp.int32, (n, n), 0)
    r = lax.broadcasted_iota(jnp.int32, (n, n), 1)
    unmix = (r == (t % L) * SUB + t // L).astype(BF16)
    mg[...] = jnp.dot(unmix, merged, preferred_element_type=F32).astype(BF16).reshape(ntp, q, W)

    def row_copy(k):
        to = lax.rem(tp + k, ntp)
        return remote(mg.at[to], rows_in.at[k - 1], s_rows.at[0], r_rows.at[0], (sp, to))

    for k in range(1, ntp):
        row_copy(k).start()

    @pl.when(inner)
    def _():
        for h in range(2):
            z_copy(0, h, 1).start()

    for h in range(2):
        hop2(1, h, 0)

    hop1(1, 0, 3)

    @pl.when(inner)
    def _():
        hop1(1, 0, 1)

    hop1(1, 1, 1)
    emit_copy.wait()
    mrg[:, pl.ds(pl.multiple_of(tp * W, 128), W)] = mg[tp]
    mid_out[:, pl.ds(pl.multiple_of(tp * Dl, 128), Dl)] = resid_ref[...].astype(F32)
    came(resid_in, r_res.at[0])
    came(rows_in, r_rows.at[0])
    for k in range(1, ntp):
        src = lax.rem(tp - k + ntp, ntp)
        mid_out[:, pl.ds(pl.multiple_of(src * Dl, 128), Dl)] = resid_in[k - 1].astype(F32)
        mrg[:, pl.ds(pl.multiple_of(src * W, 128), W)] = rows_in[k - 1]
    mid = mid_out[...] + jnp.dot(mrg[...], emit[...], preferred_element_type=F32)
    mid_out[...] = mid
    scale = lax.rsqrt(jnp.mean(mid * mid, axis=1, keepdims=True) + EPSILON)
    nrm[0, z] = (mid * scale * lead_ref[...]).astype(BF16)

    def t_far():
        return remote(nrm.at[0, z], nrm.at[0, z], s_t.at[0], r_t.at[as_seen - 1], dev(far_in, x, y, c))

    def t_mate(k):
        block = nrm.at[0, kinds[k]]
        return remote(block, block, s_t.at[0 if k == 0 else 1], r_t.at[max(k, 1) - 1], dev(mate, x, y, c))

    def t_wait(k):
        t_mate(k).wait_recv()

    def y_copy(k):
        return remote(nrm.at[0, kinds[k]], nrm.at[1, kinds[k]], s_y.at[0], r_y.at[0], y_mate)

    t_far().start()
    t_mate(0).start()
    y_copy(0).start()

    @pl.when(inner)
    def _():
        for k in (2, 3):
            z_copy(1, 1, k).start()

    @pl.when(outer)
    def _():
        for h in range(2):
            z_copy(0, h, 1).start()

    for h in range(2):
        x_copy(0, h, 0).start()
        d_copy(0, h, 0, 0).start()

    hop2(1, 0, 3)
    hop1(1, 1, 3)
    hop2(1, 0, 1)
    hop1(1, 0, 2)
    t_wait(1)
    y_copy(1).start()

    @pl.when(inner)
    def _():
        for k in (3, 2):
            t_wait(k)
            t_mate(k).start()
            y_copy(k).start()

    hop2(1, 1, 1)
    hop2(1, 1, 3)
    hop2(1, 0, 2)

    hop1(1, 1, 2)

    @pl.when(inner)
    def _():
        for k in (2, 3):
            z_copy(0, 0, k).start()

    @pl.when(outer)
    def _():
        z_copy(0, 0, 2).start()
        for k in (3, 2):
            t_wait(k)
            y_copy(k).start()
        z_copy(0, 0, 3).start()
        for k in (2, 3):
            z_copy(0, 1, k).start()

    for h in range(2):
        hop1(0, h, 1)
    for h in range(2):
        hop2(0, h, 0)
    hop2(1, 1, 2)
    came(nrm.at[1], r_y.at[0])
    own_wait(1)
    hop3_up()
    rows = nrm[...].reshape(2 * Z * q, D)
    for b in range(2):
        upward = jnp.dot(rows, wup[b].reshape(D, Fz), preferred_element_type=F32)
        hid[b] = jnp.square(jnp.maximum(upward, 0.0)).astype(BF16)

    def cols(zs, x_, h):
        return pl.ds(pl.multiple_of((zs * X + x_) * 2 * Dh + h * Dh, 128), Dh)

    def a_copy(zs, h):
        g = zs * 2 + h
        return remote(a_out.at[g], a_in.at[g], s_a.at[0], r_a.at[g], y_mate)

    def b_copy(zs, h):
        g = zs * 2 + h
        return remote(b_out.at[g, mate], b_in.at[g, mate], s_b.at[0], r_b.at[0, g], dev(mate, x, y, c))

    def b_far(zs, h):
        g = zs * 2 + h
        blocks = pl.ds(far0, 2)
        return remote(b_out.at[g, blocks], b_in.at[g, blocks], s_b.at[1], r_b.at[1, g], dev(mate, x, y, c))

    def c_copy(zs, h, i):
        g = zs * 2 + h
        return remote(c_out.at[g, i], c_in.at[tp, h], s_c.at[0], r_c.at[0], ((far0 + i) * X + x, zs))

    def stage_a(zs, h):
        g = zs * 2 + h
        for x_ in range(X):
            total = jnp.dot(hid[0], wdn[0, zs * X + x_, h], preferred_element_type=F32)
            total = total + jnp.dot(hid[1], wdn[1, zs * X + x_, h], preferred_element_type=F32)
            total = total.reshape(2, Z, q, Dh)
            a_out[g, :, x_] = total[1].astype(BF16)
            loc[g, :, x_] = total[0]
        a_copy(zs, h).start()

    def stage_b(zs, h):
        g = zs * 2 + h
        a_copy(zs, h).wait_recv()
        total = loc[g] + a_in[g].astype(F32)
        loc[g] = total
        b_out[g] = total.astype(BF16)

        @pl.when(outer)
        def _():
            b_far(zs, h).start()

        b_copy(zs, h).start()

    def stage_c(zs, h):
        g = zs * 2 + h

        @pl.when(inner)
        def _():
            b_far(zs, h).wait_recv()
            blocks = pl.ds(far0, 2)
            c_out[g] = (loc[g, blocks] + b_in[g, blocks].astype(F32)).astype(BF16)
            for i in range(2):
                c_copy(zs, h, i).start()

        b_copy(zs, h).wait_recv()
        own_sum = loc[g, z] + b_in[g, z].astype(F32)
        for x_ in range(X):
            mid_out[:, cols(zs, x_, h)] = mid_out[:, cols(zs, x_, h)] + own_sum[x_]

    def last_copy(zs, to, slot):
        return remote(b_out.at[zs * 2 + 1, to], c_in.at[tp, slot], s_last.at[0], r_c.at[slot - 1], (to * X + x, zs))

    def last_sums(zs):
        g = zs * 2 + 1
        a_copy(zs, 1).wait_recv()
        loc[g] = loc[g] + a_in[g].astype(F32)
        b_out[g] = loc[g].astype(BF16)
        for i in range(2):
            last_copy(zs, far0 + i, as_seen - 1).start()
        last_copy(zs, mate, 2).start()
        for x_ in range(X):
            mid_out[:, cols(zs, x_, 1)] = mid_out[:, cols(zs, x_, 1)] + loc[g, z, x_]

    def home_copy(zs):
        return remote(mid_out.at[:, pl.ds(pl.multiple_of(zs * Dl, 128), Dl)], home_in.at[tp], s_home.at[0],
                      r_home.at[0], (sp, zs))

    def stage_d(zs):
        @pl.when(zs == tp)
        def _():
            home_in[tp] = mid_out[:, pl.ds(pl.multiple_of(zs * Dl, 128), Dl)]

        @pl.when(zs != tp)
        def _():
            home_copy(zs).start()

    turns = [(zs, h) for zs in (half_in, half_out, far_out, far_in) for h in range(2)]
    hop1(0, 0, 3)

    @pl.when(inner)
    def _():
        for k in (2, 3):
            z_copy(0, 1, k).start()

    own_wait(0)
    for h in range(2):
        hop2(0, h, 1)
    hop3_near()
    stage_a(*turns[0])
    stage_a(*turns[1])
    stage_a(*turns[2])
    stage_a(*turns[3])
    hop1(0, 1, 3)
    stage_b(*turns[0])
    hop1(0, 0, 2)
    hop2(0, 0, 3)
    stage_b(*turns[1])
    hop3_far(0, 3)
    stage_a(*turns[4])
    stage_b(*turns[2])
    hop2(0, 1, 3)
    stage_b(*turns[3])
    hop3_far(1, 3)
    stage_a(*turns[5])
    stage_c(*turns[0])
    hop2(0, 0, 2)
    stage_c(*turns[1])
    stage_d(half_in)
    hop1(0, 1, 2)
    hop3_far(0, 2)
    stage_a(*turns[6])
    stage_c(*turns[2])
    stage_b(*turns[4])
    stage_c(*turns[3])
    stage_d(half_out)
    stage_b(*turns[5])
    hop2(0, 1, 2)
    stage_b(*turns[6])
    hop3_far(1, 2)
    stage_a(*turns[7])
    stage_c(*turns[4])
    stage_c(*turns[5])
    stage_d(far_out)
    last_sums(far_in)
    stage_c(*turns[6])
    stage_d(far_in)
    came(home_in.at[pl.ds(0, ntp - 1)], r_home.at[0])
    came(c_in.at[:, pl.ds(0, 2)], r_c.at[0])

    @pl.when((tp == half_in) | (tp == far_in))
    def _():
        came(c_in.at[:, 2], r_c.at[1])
        for x_ in range(X):
            at = pl.ds((2 * x_ + 1) * Dh, Dh)
            home_in[:, :, at] = home_in[:, :, at] + c_in[:, 2, x_].astype(F32)

    for src in range(ntp):
        for x_ in range(X):
            for h in range(2):
                at = pl.ds((2 * x_ + h) * Dh, Dh)
                out_ref[pl.ds(src * q, q), at] = (home_in[src, :, at] + c_in[src, h, x_].astype(F32)).astype(BF16)

    sent(wup.at[0, pl.ds(0, 6)], s_z.at[0])
    sent(wup.at[0], s_x.at[0])
    sent(wup, s_d.at[0])
    sent(ends_all.at[0], s_ends.at[0])
    sent(nrm.at[0, pl.ds(0, 2)], s_t.at[0])
    sent(nrm.at[0], s_y.at[0])
    sent(a_out, s_a.at[0])
    sent(b_out.at[pl.ds(0, 2 * Z - 1), 0], s_b.at[0])
    sent(b_out.at[0, pl.ds(0, 3)], s_last.at[0])
    sent(home_in.at[pl.ds(0, ntp - 1)], s_home.at[0])
    sent(resid_in, s_res.at[0])
    sent(rows_in, s_rows.at[0])

    @pl.when(inner)
    def _():
        sent(nrm.at[0, pl.ds(0, 2)], s_t.at[1])
        sent(c_out.at[pl.ds(0, 2 * Z - 1)], s_c.at[0])

    @pl.when(outer)
    def _():
        sent(b_out.at[pl.ds(0, 2 * Z - 1), pl.ds(0, 2)], s_b.at[1])


def paired_call(nsp, ntp, residual, lifted, dts, long_rate, short_rate, emitted, raising):
    n, W = lifted.shape
    G = dts.shape[0]
    half = G // 2
    PL, PS = long_rate.shape[2], short_rate.shape[2]
    S = half * (PL + PS)
    D = emitted.shape[1]
    Dl = residual.shape[1]
    q = n // ntp
    Z, X, Y = mesh_split(nsp, ntp)
    Fz = raising.shape[1] // Z
    Dh = D // nsp // 2
    groups = 2 * Z
    cfg = (nsp, ntp, n, S, W, G, PL, PS, D, Fz)
    vm = pl.BlockSpec(memory_space=pltpu.VMEM)
    dma = pltpu.SemaphoreType.DMA
    return pl.pallas_call(
        functools.partial(paired_body, cfg),
        out_shape=jax.ShapeDtypeStruct((n, Dl), BF16),
        in_specs=[pl.BlockSpec(memory_space=pl.ANY)] * 16,
        out_specs=vm,
        scratch_shapes=[
            pltpu.VMEM(lifted.shape, BF16), pltpu.VMEM(dts.shape, F32), pltpu.VMEM(dts.shape, F32),
            *[pltpu.VMEM(long_rate.shape, F32), pltpu.VMEM(short_rate.shape, F32)] * 2,
            pltpu.VMEM((1, ntp * W), F32), pltpu.VMEM((1, ntp * W), F32), pltpu.VMEM((q, Dl), BF16),
            pltpu.VMEM((1, D), F32), dma((11,)),
            pltpu.VMEM((8, half, CHAN, PL), F32), pltpu.VMEM((8, half, CHAN, PS), F32), dma((2,)),
            pltpu.VMEM((n, S), F32), pltpu.VMEM((n, S), F32),
            pltpu.VMEM((n, 4 * S), F32), pltpu.VMEM((n, 4 * S), F32),
            pltpu.VMEM((8, SUB, S), F32), pltpu.VMEM((2, 4, S), F32), pltpu.VMEM((2, nsp - 1, 4, S), F32),
            pltpu.VMEM((4, SUB, S), F32),
            pltpu.VMEM((ntp, q, W), BF16), pltpu.VMEM((ntp - 1, q, W), BF16),
            pltpu.VMEM((q, ntp * W), BF16), pltpu.VMEM(emitted.shape, BF16),
            pltpu.VMEM((ntp - 1, q, Dl), BF16),
            pltpu.VMEM((q, D), F32),
            pltpu.VMEM((2, nsp, 2, D // nsp // 2, Fz), BF16), pltpu.VMEM((2, nsp, 2, Fz, Dh), BF16),
            pltpu.VMEM((2, Z, q, D), BF16), pltpu.VMEM((2, 2 * Z * q, Fz), BF16),
            pltpu.VMEM((groups, Z, X, q, Dh), F32),
            *[pltpu.VMEM((groups, Z, X, q, Dh), BF16)] * 4,
            pltpu.VMEM((groups, 2, X, q, Dh), BF16), pltpu.VMEM((ntp, 3, X, q, Dh), BF16),
            pltpu.VMEM((ntp, q, Dl), F32),
            dma((1,)), dma((2,)), *[dma((1,))] * 6,
            dma((1,)), dma((2, 2, 3)), dma((1,)), dma((2, 2, 4)), dma((1,)), dma((1,)), dma((5,)),
            dma((2,)), dma((3,)), dma((1,)), dma((1,)),
            dma((1,)), dma((groups,)), dma((2,)), dma((2, groups)), dma((1,)), dma((2,)), *[dma((1,))] * 3,
        ],
        compiler_params=pltpu.CompilerParams(collective_id=0, has_side_effects=True),
        cost_estimate=pl.CostEstimate(flops=10**9, bytes_accessed=3 * 10**7, transcendentals=10**6),
    )


def on_device(residual, lifted, dts, fades, long_rate, short_rate, long_freq, short_freq,
              long_lin, short_lin, skip, closing, emitted, leading, raising, lowering):
    nsp, ntp = lax.axis_size("sp"), lax.axis_size("tp")
    operands = (lifted, dts, fades, long_rate, short_rate, long_freq, short_freq, skip[None], closing[None],
                residual, leading[None], long_lin.swapaxes(4, 5), short_lin.swapaxes(4, 5), emitted, raising, lowering)
    Z, X, Y = mesh_split(nsp, ntp)
    if X == 2 and Y == 2 and Z == ntp:
        return paired_call(nsp, ntp, residual, lifted, dts, long_rate, short_rate, emitted, raising)(*operands)
    n, W = lifted.shape
    G = dts.shape[0]
    half = G // 2
    PL, PS = long_rate.shape[2], short_rate.shape[2]
    S = half * (PL + PS)
    D = emitted.shape[1]
    Dl = residual.shape[1]
    q = n // ntp
    c_ff = min(nsp, raising.shape[1] // 128)
    F = raising.shape[1] // c_ff
    q_all, M = c_ff * q, ntp // 2
    cfg = (nsp, ntp, n, S, W, G, PL, PS, D, c_ff, F)
    vm = pl.BlockSpec(memory_space=pltpu.VMEM)
    dma = pltpu.SemaphoreType.DMA
    return pl.pallas_call(
        functools.partial(mixer_body, cfg),
        out_shape=jax.ShapeDtypeStruct((n, Dl), BF16),
        in_specs=[vm] * 11 + [pl.BlockSpec(memory_space=pl.ANY)] * 5,
        out_specs=vm,
        scratch_shapes=[
            pltpu.VMEM((8, half, CHAN, PL), F32), pltpu.VMEM((8, half, CHAN, PS), F32), dma((2, 8)),
            pltpu.VMEM((n, S), F32), pltpu.VMEM((n, S), F32),
            pltpu.VMEM((n, 4 * S), F32), pltpu.VMEM((n, 4 * S), F32),
            pltpu.VMEM((8, SUB, S), F32), pltpu.VMEM((8, S), F32), pltpu.VMEM((nsp - 1, 8, S), F32),
            pltpu.VMEM((4, SUB, S), F32),
            pltpu.VMEM((ntp, q, W), BF16), pltpu.VMEM((ntp - 1, q, W), BF16),
            pltpu.VMEM((q, ntp * W), BF16), pltpu.VMEM(emitted.shape, BF16),
            pltpu.VMEM((ntp - 1, q, Dl), BF16),
            pltpu.VMEM((q, D), F32),
            pltpu.VMEM((ntp, nsp, D // nsp, F), BF16), pltpu.VMEM((ntp, nsp, F, D // nsp), BF16),
            pltpu.VMEM((c_ff, q, D), BF16), pltpu.VMEM((ntp, q_all, F), BF16),
            pltpu.VMEM((c_ff, q, D), BF16), pltpu.VMEM((c_ff - 1, q, D), BF16),
            pltpu.VMEM((ntp, q, Dl), BF16), pltpu.VMEM((ntp - 1, q, Dl), BF16),
            dma((3,)), dma((nsp - 1,)), dma((nsp - 1,)), dma((ntp - 1,)), dma((ntp - 1,)),
            dma((ntp - 1,)), dma((ntp - 1,)),
            *[dma((nsp - 1,))] * 4, *[dma((M - 1, nsp))] * 4, *[dma((M,))] * 4,
            *[dma((2, c_ff // 2))] * 2, *[dma((c_ff - 1,))] * 2, *[dma((ntp - 1,))] * 2,
        ],
        compiler_params=pltpu.CompilerParams(collective_id=0, has_side_effects=True),
        cost_estimate=pl.CostEstimate(flops=10**9, bytes_accessed=3 * 10**7, transcendentals=10**6),
    )(*operands)


def solution(mesh):
    both, swapped = P("sp", "tp"), P("tp", "sp")
    in_specs = (both, both, swapped, swapped) + (P(),) * 10 + (both, swapped)
    return jax.shard_map(on_device, mesh=mesh, in_specs=in_specs, out_specs=both, check_vma=False)
```

```python
import functools

import jax
import jax.numpy as jnp
from jax import lax
from jax.experimental import pallas as pl
from jax.experimental.pallas import tpu as pltpu
from jax.sharding import PartitionSpec as P

CHAN = 16
NORM_W = 128
EPSILON = 1e-06
SUB = 8
PARTS = 4
F32, BF16 = jnp.float32, jnp.bfloat16


def sincos(a):
    k = jnp.floor(a * 0.6366197723675814 + 0.5)
    r = a - k * 1.5703125
    r = r - k * 4.8351287841796875e-4
    r = r - k * 3.138556210e-7
    z = r * r
    s = r + r * z * (-1.6666654611e-1 + z * (8.3321608736e-3 + z * -1.9515295891e-4))
    c = 1.0 - 0.5 * z + z * z * (
        4.166664568298827e-2 + z * (-1.388731625493765e-3 + z * 2.443315711809948e-5)
    )
    half = jnp.floor(k * 0.5)
    odd = (k - 2.0 * half) > 0.5
    half_odd = (half - 2.0 * jnp.floor(half * 0.5)) > 0.5
    cos_v = jnp.where(odd, -s, c)
    sin_v = jnp.where(odd, c, s)
    return jnp.where(half_odd, -cos_v, cos_v), jnp.where(half_odd, -sin_v, sin_v)


def one_minus_exp_neg(u):
    t = jnp.full_like(u, 1.0)
    for m in range(10, 1, -1):
        t = 1.0 - u * (1.0 / m) * t
    return u * t


def cmul(ar, ai, br, bi):
    return ar * br - ai * bi, ar * bi + ai * br


def mixer_body(cfg, x_ref, dt_ref, lf_ref, long_rate, short_rate, long_freq, short_freq,
               skip_ref, gain_ref, resid_ref, lead_ref, long_hbm, short_hbm, emit_hbm, up_hbm, down_hbm,
               out_ref, lin_l, lin_s, lin_sem,
               pace, surge, pre, st, blk, ends, ends_all, cin, mg, rows_in, mrg, emit, resid_in,
               mid_out, wup, wdn, nrm, hid, part, rs_in, fin, fin_in,
               copy_sem, s_ends, r_ends, s_rows, r_rows, s_res, r_res,
               s_u1, r_u1, s_d1, r_d1, s_u2, r_u2, s_d2, r_d2, s_u3, r_u3, s_d3, r_d3,
               s_nrm, r_nrm, s_rs, r_rs, s_fin, r_fin):
    nsp, ntp, n, S, W, G, PL, PS, D, c_ff, F = cfg
    M = ntp // 2
    L = n // SUB
    half = G // 2
    SL = half * PL
    sp = lax.axis_index("sp")
    tp = lax.axis_index("tp")
    q = n // ntp
    Dl = D // ntp
    MESH = pl.DeviceIdType.MESH

    emit_copy = pltpu.make_async_copy(emit_hbm, emit, copy_sem.at[0])
    lin_copies = []
    for at in range(8):
        for kind, (src, dst) in enumerate(((long_hbm, lin_l), (short_hbm, lin_s))):
            lin_copies.append(pltpu.make_async_copy(
                src.at[at // 4, at // 2 % 2, at % 2, pl.ds(tp * half, half)], dst.at[at],
                lin_sem.at[kind, at]))
    for copy in lin_copies:
        copy.start()
    emit_copy.start()
    chunk = lax.rem(sp, c_ff)
    partner = tp + 1 - 2 * lax.rem(tp, 2)

    def cols(of):
        return pl.ds(pl.multiple_of(of * F, 128), F)

    own_up = pltpu.make_async_copy(up_hbm.at[:, cols(chunk)], wup.at[tp, sp], copy_sem.at[1])
    own_down = pltpu.make_async_copy(down_hbm.at[cols(chunk), :], wdn.at[tp, sp], copy_sem.at[2])
    own_up.start()
    own_down.start()

    def spread_copy(k, up):
        to = lax.rem(sp + k, nsp)
        src = up_hbm.at[:, cols(lax.rem(to, c_ff))] if up else down_hbm.at[cols(lax.rem(to, c_ff)), :]
        return pltpu.make_async_remote_copy(
            src_ref=src, dst_ref=(wup if up else wdn).at[tp, sp],
            send_sem=(s_u1 if up else s_d1).at[k - 1], recv_sem=(r_u1 if up else r_d1).at[k - 1],
            device_id=(to, tp), device_id_type=MESH)

    def across_copy(m, k, up):
        piece = (wup if up else wdn).at[tp, lax.rem(sp - k + nsp, nsp)]
        return pltpu.make_async_remote_copy(
            src_ref=piece, dst_ref=piece,
            send_sem=(s_u2 if up else s_d2).at[m - 1, k], recv_sem=(r_u2 if up else r_d2).at[m - 1, k],
            device_id=(sp, lax.rem(tp + 2 * m, ntp)), device_id_type=MESH)

    def pair_copy(m, up):
        piece = (wup if up else wdn).at[lax.rem(tp + 2 * m, ntp)]
        return pltpu.make_async_remote_copy(
            src_ref=piece, dst_ref=piece,
            send_sem=(s_u3 if up else s_d3).at[m], recv_sem=(r_u3 if up else r_d3).at[m],
            device_id=(sp, partner), device_id_type=MESH)

    def pass_on(first, last, up):
        for k in range(first, last):
            if k == 0:
                (own_up if up else own_down).wait()
            else:
                spread_copy(k, up).wait_recv()
            for m in range(1, M):
                across_copy(m, k, up).start()

    barrier = pltpu.get_barrier_semaphore()
    for k in range(1, nsp):
        pl.semaphore_signal(barrier, inc=1, device_id=(lax.rem(sp + k, nsp), tp), device_id_type=MESH)
    for k in range(1, ntp):
        pl.semaphore_signal(barrier, inc=1, device_id=(sp, lax.rem(tp + k, ntp)), device_id_type=MESH)
    pl.semaphore_wait(barrier, nsp + ntp - 2)

    def res_copy(k):
        to = lax.rem(tp + k, ntp)
        return pltpu.make_async_remote_copy(
            src_ref=resid_ref.at[pl.ds(to * q, q), :], dst_ref=resid_in.at[k - 1],
            send_sem=s_res.at[k - 1], recv_sem=r_res.at[k - 1],
            device_id=(sp, to), device_id_type=MESH)

    for k in range(1, nsp):
        spread_copy(k, True).start()
    for k in range(1, ntp):
        res_copy(k).start()

    lane = lax.broadcasted_iota(jnp.int32, (G, S), 1)
    group = jnp.where(lane < SL, 2 * (lane // PL), 2 * ((lane - SL) // PS) + 1)
    spread = (group == lax.broadcasted_iota(jnp.int32, (G, S), 0)).astype(F32)
    r = lax.broadcasted_iota(jnp.int32, (n, n), 0)
    t = lax.broadcasted_iota(jnp.int32, (n, n), 1)
    mix = (t == (r % SUB) * L + r // SUB).astype(F32)

    def per_state(ref):
        moved = lax.dot_general(ref[...], mix, (((1,), (1,)), ((), ())),
                                precision=lax.Precision.HIGHEST, preferred_element_type=F32)
        return lax.dot_general(moved, spread, (((0,), (0,)), ((), ())),
                               precision=lax.Precision.HIGHEST, preferred_element_type=F32)

    pace[...] = per_state(dt_ref)
    surge[...] = per_state(lf_ref)

    def flat_kind(ref, e):
        many, states = ref.shape[1:]
        width = half * states
        repeat = (lax.broadcasted_iota(jnp.int32, (states, width), 1) % states
                  == lax.broadcasted_iota(jnp.int32, (states, width), 0)).astype(F32)
        wide = jnp.dot(ref[e], repeat, precision=lax.Precision.HIGHEST, preferred_element_type=F32)
        owner = tp * half + lax.broadcasted_iota(jnp.int32, (many, width), 1) // states
        mine = owner == lax.broadcasted_iota(jnp.int32, (many, width), 0)
        return jnp.sum(jnp.where(mine, wide, 0.0), axis=0, keepdims=True)

    def flat(long_ref, short_ref, e):
        return jnp.concatenate([flat_kind(long_ref, e), flat_kind(short_ref, e)], axis=1)

    def widened(ref, index, states, sign):
        rows, width = half * CHAN, half * states
        repeat = (lax.broadcasted_iota(jnp.int32, (states, width), 1) % states
                  == lax.broadcasted_iota(jnp.int32, (states, width), 0)).astype(BF16)
        wide = jnp.dot(ref[index].reshape(rows, states).astype(BF16), repeat, preferred_element_type=F32)
        own_block = (lax.broadcasted_iota(jnp.int32, (rows, width), 0) // CHAN
                     == lax.broadcasted_iota(jnp.int32, (rows, width), 1) // states)
        return jnp.where(own_block, sign * wide, 0.0).astype(BF16)

    def block_map(index, sign=1.0):
        long_part = widened(lin_l, index, PL, sign)
        short_part = widened(lin_s, index, PS, sign)
        no_long, no_short = jnp.zeros((CHAN, SL), BF16), jnp.zeros((CHAN, S - SL), BF16)
        bands = []
        for g in range(half):
            band = slice(g * CHAN, (g + 1) * CHAN)
            bands.append(jnp.concatenate([long_part[band], no_short], axis=1))
            bands.append(jnp.concatenate([no_long, short_part[band]], axis=1))
        return jnp.concatenate(bands, axis=0)

    xv = jnp.dot(mix.astype(BF16), x_ref[...], preferred_element_type=F32).astype(BF16)
    for copy in lin_copies:
        copy.wait()
    for e in range(2):
        for c in range(2):
            st[:, pl.ds((2 * e + c) * S, S)] = jnp.dot(
                xv, block_map(4 * e + c), preferred_element_type=F32)

    for e in range(2):
        rate = flat(long_rate, short_rate, e)
        freq = flat(long_freq, short_freq, e)

        def step(i, carry):
            pr, pi, sr, si = carry
            at = i if e == 0 else L - 1 - i
            rows = pl.ds(pl.multiple_of(at * SUB, SUB), SUB)
            d = pace[rows, :]
            rd = rate * d
            m = jnp.exp(surge[rows, :] - rd)
            cos_v, sin_v = sincos(freq * d)
            w = jnp.sqrt(one_minus_exp_neg(2.0 * rd))
            ar, ai = m * cos_v, m * sin_v
            pr, pi = cmul(ar, ai, pr, pi)
            sr, si = cmul(ar, ai, sr, si)
            sr = sr + w * st[rows, pl.ds(2 * e * S, S)]
            si = si + w * st[rows, pl.ds((2 * e + 1) * S, S)]
            pre[rows, pl.ds(2 * e * S, S)] = pr
            pre[rows, pl.ds((2 * e + 1) * S, S)] = pi
            st[rows, pl.ds(2 * e * S, S)] = sr
            st[rows, pl.ds((2 * e + 1) * S, S)] = si
            return pr, pi, sr, si

        zero = jnp.zeros((SUB, S), F32)
        total = lax.fori_loop(0, L, step, (zero + 1.0, zero, zero, zero))
        for c in range(4):
            blk[4 * e + c] = total[c]
        order = range(SUB) if e == 0 else range(SUB - 1, -1, -1)
        run = None
        for b in order:
            now = tuple(blk[4 * e + c, b : b + 1, :] for c in range(4))
            if run is None:
                run = now
            else:
                p = cmul(now[0], now[1], run[0], run[1])
                s = cmul(now[0], now[1], run[2], run[3])
                run = (p[0], p[1], s[0] + now[2], s[1] + now[3])
        for c in range(4):
            ends[4 * e + c : 4 * e + c + 1, :] = run[c]

    def ends_copy(k):
        return pltpu.make_async_remote_copy(
            src_ref=ends, dst_ref=ends_all.at[k - 1],
            send_sem=s_ends.at[k - 1], recv_sem=r_ends.at[k - 1],
            device_id=(lax.rem(sp + k, nsp), tp), device_id_type=MESH)

    for k in range(1, nsp):
        ends_copy(k).start()
    for k in range(1, nsp):
        spread_copy(k, False).start()

    read = jnp.concatenate(
        [block_map(2), block_map(3, -1.0), block_map(6), block_map(7, -1.0)], axis=1)

    pass_on(0, nsp // 2, True)
    for k in range(1, nsp):
        ends_copy(k).wait_recv()
    blank = jnp.zeros((1, S), F32)

    def fold(j, carry, e):
        cr, ci = carry
        k = nsp - 1 - j if e == 0 else j + 1
        reached = k <= sp if e == 0 else nsp - k <= nsp - 1 - sp
        got = ends_all[k - 1]
        nr, ni = cmul(got[4 * e : 4 * e + 1], got[4 * e + 1 : 4 * e + 2], cr, ci)
        nr = nr + got[4 * e + 2 : 4 * e + 3]
        ni = ni + got[4 * e + 3 : 4 * e + 4]
        return jnp.where(reached, nr, cr), jnp.where(reached, ni, ci)

    for e in range(2):
        cr, ci = lax.fori_loop(0, nsp - 1, functools.partial(fold, e=e), (blank, blank))
        order = range(SUB) if e == 0 else range(SUB - 1, -1, -1)
        for b in order:
            cin[2 * e, b : b + 1, :] = cr
            cin[2 * e + 1, b : b + 1, :] = ci
            now = tuple(blk[4 * e + c, b : b + 1, :] for c in range(4))
            nr, ni = cmul(now[0], now[1], cr, ci)
            cr, ci = nr + now[2], ni + now[3]

        inr, ini = cin[2 * e], cin[2 * e + 1]

        def settle(i, _):
            rows = pl.ds(pl.multiple_of(i * SUB, SUB), SUB)
            re, im = pl.ds(2 * e * S, S), pl.ds((2 * e + 1) * S, S)
            ar, ai = cmul(pre[rows, re], pre[rows, im], inr, ini)
            st[rows, re] = st[rows, re] + ar
            st[rows, im] = st[rows, im] + ai
            return 0

        lax.fori_loop(0, L, settle, 0)

    y = lax.dot_general(st[...].astype(BF16), read, (((1,), (1,)), ((), ())),
                        preferred_element_type=F32)
    own = pl.ds(pl.multiple_of(tp * W, 128), W)
    skip_row, gain_row = skip_ref[:, own], gain_ref[:, own]
    y = y + skip_row * xv.astype(F32)
    y = 0.5 * y * (1.0 + jnp.tanh(0.7978845608028654 * (y + 0.044715 * y * y * y)))
    heads = []
    for h in range(W // NORM_W):
        head = y[:, h * NORM_W : (h + 1) * NORM_W]
        scale = lax.rsqrt(jnp.mean(head * head, axis=1, keepdims=True) + EPSILON)
        heads.append(head * scale * gain_row[:, h * NORM_W : (h + 1) * NORM_W])
    merged = jnp.concatenate(heads, axis=1).astype(BF16)
    t = lax.broadcasted_iota(jnp.int32, (n, n), 0)
    r = lax.broadcasted_iota(jnp.int32, (n, n), 1)
    unmix = (r == (t % L) * SUB + t // L).astype(BF16)
    mg[...] = jnp.dot(unmix, merged, preferred_element_type=F32).astype(BF16).reshape(ntp, q, W)

    def row_copy(k):
        to = lax.rem(tp + k, ntp)
        return pltpu.make_async_remote_copy(
            src_ref=mg.at[to], dst_ref=rows_in.at[k - 1],
            send_sem=s_rows.at[k - 1], recv_sem=r_rows.at[k - 1],
            device_id=(sp, to), device_id_type=MESH)

    for k in range(1, ntp):
        row_copy(k).start()
    pass_on(nsp // 2, nsp, True)
    emit_copy.wait()
    mrg[:, pl.ds(pl.multiple_of(tp * W, 128), W)] = mg[tp]
    mid_out[:, pl.ds(pl.multiple_of(tp * Dl, 128), Dl)] = resid_ref[pl.ds(pl.multiple_of(tp * q, q), q), :].astype(F32)
    for k in range(1, ntp):
        src = lax.rem(tp - k + ntp, ntp)
        res_copy(k).wait_recv()
        mid_out[:, pl.ds(pl.multiple_of(src * Dl, 128), Dl)] = resid_in[k - 1].astype(F32)
        row_copy(k).wait_recv()
        mrg[:, pl.ds(pl.multiple_of(src * W, 128), W)] = rows_in[k - 1]
    mid = mid_out[...] + jnp.dot(mrg[...], emit[...], preferred_element_type=F32)
    mid_out[...] = mid
    scale = lax.rsqrt(jnp.mean(mid * mid, axis=1, keepdims=True) + EPSILON)
    base, q_all = sp - chunk, c_ff * q
    nrm[chunk] = (mid * scale * lead_ref[...]).astype(BF16)

    def peer(k):
        return lax.rem(chunk + k, c_ff)

    H = c_ff // 2

    def nrm_across(m):
        return pltpu.make_async_remote_copy(
            src_ref=nrm.at[chunk], dst_ref=nrm.at[chunk],
            send_sem=s_nrm.at[0, m], recv_sem=r_nrm.at[0, m],
            device_id=(base + peer(2 * m), tp), device_id_type=MESH)

    def nrm_pair(m):
        return pltpu.make_async_remote_copy(
            src_ref=nrm.at[peer(2 * m)], dst_ref=nrm.at[peer(2 * m)],
            send_sem=s_nrm.at[1, m], recv_sem=r_nrm.at[1, m],
            device_id=(base + chunk + 1 - 2 * lax.rem(chunk, 2), tp), device_id_type=MESH)

    def rs_copy(k):
        return pltpu.make_async_remote_copy(
            src_ref=part.at[peer(k)], dst_ref=rs_in.at[k - 1],
            send_sem=s_rs.at[k - 1], recv_sem=r_rs.at[k - 1],
            device_id=(base + peer(k), tp), device_id_type=MESH)

    def fin_copy(k):
        to = lax.rem(tp + k, ntp)
        return pltpu.make_async_remote_copy(
            src_ref=fin.at[to], dst_ref=fin_in.at[k - 1],
            send_sem=s_fin.at[k - 1], recv_sem=r_fin.at[k - 1],
            device_id=(sp, to), device_id_type=MESH)

    for m in range(1, H):
        nrm_across(m).start()
    nrm_pair(0).start()
    pair_copy(0, True).start()
    pass_on(0, nsp, False)
    pair_copy(0, False).start()
    for m in range(1, H):
        nrm_across(m).wait_recv()
        nrm_pair(H - m).start()
    for up in (True, False):
        for m in range(1, M):
            for k in range(nsp):
                across_copy(m, k, up).wait_recv()
            pair_copy(M - m, up).start()
        if up:
            for m in range(M):
                pair_copy(m, True).wait_recv()
            for m in range(H):
                nrm_pair(m).wait_recv()
            rows = nrm[...].reshape(q_all, D)

            def raise_step(t, _):
                upward = jnp.dot(rows, wup[t].reshape(D, F), preferred_element_type=F32)
                hid[t] = jnp.square(jnp.maximum(upward, 0.0)).astype(BF16)
                return 0

            lax.fori_loop(0, ntp, raise_step, 0)
    for m in range(M):
        pair_copy(m, False).wait_recv()
    Dc = D // nsp
    for j in range(nsp):
        total = jnp.dot(hid[0], wdn[0, j], preferred_element_type=F32)
        for t in range(1, ntp):
            total = total + jnp.dot(hid[t], wdn[t, j], preferred_element_type=F32)
        part[:, :, j * Dc : (j + 1) * Dc] = total.astype(BF16).reshape(c_ff, q, Dc)
    for k in range(1, c_ff):
        rs_copy(k).start()
    result = mid_out[...] + part[chunk].astype(F32)
    for k in range(1, c_ff):
        rs_copy(k).wait_recv()
        result = result + rs_in[k - 1].astype(F32)
    result = result.astype(BF16)
    for t in range(ntp):
        fin[t] = result[:, t * Dl : (t + 1) * Dl]
    for k in range(1, ntp):
        fin_copy(k).start()
    out_ref[pl.ds(pl.multiple_of(tp * q, q), q), :] = fin[tp]
    for k in range(1, ntp):
        fin_copy(k).wait_recv()
        src = lax.rem(tp - k + ntp, ntp)
        out_ref[pl.ds(pl.multiple_of(src * q, q), q), :] = fin_in[k - 1]
    for k in range(1, c_ff):
        rs_copy(k).wait_send()
    for m in range(H):
        if m > 0:
            nrm_across(m).wait_send()
        nrm_pair(m).wait_send()
    for k in range(1, ntp):
        fin_copy(k).wait_send()
    for up in (True, False):
        for k in range(1, nsp):
            spread_copy(k, up).wait_send()
        for m in range(1, M):
            for k in range(nsp):
                across_copy(m, k, up).wait_send()
        for m in range(M):
            pair_copy(m, up).wait_send()
    for k in range(1, nsp):
        ends_copy(k).wait_send()
    for k in range(1, ntp):
        res_copy(k).wait_send()
        row_copy(k).wait_send()


def mesh_split(nsp, ntp):
    Y = ntp // 2
    X = Y if Y > 0 and nsp % Y == 0 else 1
    return nsp // X, X, Y


def paired_body(cfg, x_hbm, dt_hbm, lf_hbm, long_rate_hbm, short_rate_hbm, long_freq_hbm, short_freq_hbm,
                skip_hbm, gain_hbm, resid_hbm, lead_hbm, long_hbm, short_hbm, emit_hbm, up_hbm, down_hbm,
                out_ref, x_ref, dt_ref, lf_ref, long_rate, short_rate, long_freq, short_freq,
                skip_ref, gain_ref, resid_ref, lead_ref, in_sem, lin_l, lin_s, lin_sem,
                pace, surge, pre, st, blk, ends, ends_all, cin, mg, rows_in, mrg, emit, resid_in,
                mid_out, wup, wdn, nrm, hid, loc, a_out, a_in, b_out, b_in, c_out, c_in, home_in,
                copy_sem, own_sem, s_ends, r_ends, s_rows, r_rows, s_res, r_res,
                s_z, r_z, s_x, r_x, s_d, r_d_up, r_d_down, s_t, r_t, s_y, r_y,
                s_a, r_a, s_b, r_b, s_c, r_c, s_last, s_home, r_home,
                o_out, s_own, r_own, r_tz, r_tx, r_td, r_ta):
    nsp, ntp, n, S, W, G, PL, PS, D, Fz = cfg
    Z, X, Y = mesh_split(nsp, ntp)
    L = n // SUB
    half = G // 2
    SL = half * PL
    sp = lax.axis_index("sp")
    tp = lax.axis_index("tp")
    q = n // ntp
    Dl = D // ntp
    Dh = D // nsp // 2
    Rh = D // nsp // 2
    MESH = pl.DeviceIdType.MESH
    z, x, y, c = sp // X, lax.rem(sp, X), tp // 2, lax.rem(tp, 2)
    side = z // 2
    half_in, half_out = 1 + side, 3 * side
    far_in, far_out = 2 - side, 3 - 3 * side
    far0 = 2 - 2 * side
    mate = z + 1 - 2 * lax.rem(z, 2)
    inner, outer = z == half_in, z == half_out
    kinds = (z, mate, far_in, far_out)
    as_seen = 2 + jnp.where(outer, 1, 0)

    def dev(z_, x_, y_, c_):
        return (z_ * X + x_, y_ * 2 + c_)

    x_mate, y_mate, c_mate = dev(z, 1 - x, y, c), dev(z, x, 1 - y, c), dev(z, x, y, 1 - c)

    def remote(src, dst, ssem, rsem, to):
        return pltpu.make_async_remote_copy(src_ref=src, dst_ref=dst, send_sem=ssem, recv_sem=rsem,
                                            device_id=to, device_id_type=MESH)

    in_copies = [pltpu.make_async_copy(src, dst, in_sem.at[at]) for at, (src, dst) in enumerate((
        (dt_hbm, dt_ref), (lf_hbm, lf_ref), (x_hbm, x_ref), (long_rate_hbm, long_rate), (short_rate_hbm, short_rate),
        (long_freq_hbm, long_freq), (short_freq_hbm, short_freq), (skip_hbm, skip_ref), (gain_hbm, gain_ref),
        (lead_hbm, lead_ref), (resid_hbm.at[pl.ds(pl.multiple_of(tp * q, q), q), :], resid_ref)))]
    emit_copy = pltpu.make_async_copy(emit_hbm, emit, copy_sem.at[0])
    lin_copies = []
    for at in range(8):
        for kind, (src, dst) in enumerate(((long_hbm, lin_l), (short_hbm, lin_s))):
            lin_copies.append(pltpu.make_async_copy(
                src.at[at // 4, at // 2 % 2, at % 2, pl.ds(tp * half, half)], dst.at[at], lin_sem.at[kind]))

    def sent(ref, sem):
        remote(ref, ref, sem, sem, c_mate).wait_send()

    def came(ref, sem):
        remote(ref, ref, sem, sem, c_mate).wait_recv()

    def bank(up):
        return wup if up else wdn

    def shard(up, h, to):
        part = pl.ds(pl.multiple_of(to * Fz, 128), Fz)
        if up:
            return up_hbm.at[pl.ds(h * Rh, Rh), part]
        return down_hbm.at[part, pl.ds(h * Dh, Dh)]

    def own_copy(up, h):
        return pltpu.make_async_copy(shard(up, h, z), bank(up).at[c, sp, h], own_sem.at[1 - up])

    def own_wait(up):
        pltpu.make_async_copy(bank(up).at[c, sp], bank(up).at[c, sp], own_sem.at[1 - up]).wait()

    def z_copy(up, h, k):
        to = kinds[k]
        return remote(shard(up, h, to), bank(up).at[c, sp, h], s_z.at[0],
                      r_z.at[1 - up, h, 0 if k == 1 else as_seen - 1], dev(to, x, y, c))

    def x_copy(up, h, k):
        piece = bank(up).at[c, kinds[k] * X + x, h]
        return remote(shard(up, h, z) if k == 0 else piece, piece, s_x.at[0], r_x.at[1 - up, h, k], x_mate)

    def d_copy(up, h, k, other):
        piece = bank(up).at[c, kinds[k] * X + (1 - x if other else x), h]
        return remote(shard(up, h, z) if k == 0 and not other else piece, piece, s_d.at[0],
                      r_d_up.at[0] if up else r_d_down.at[0 if k < 2 else 1 + (k - 2) * 2 + h], c_mate)

    def hop1(up, h, k):
        came(bank(up).at[c, kinds[k] * X + x, h], r_z.at[1 - up, h, k - 1])
        x_copy(up, h, k).start()
        d_copy(up, h, k, 0).start()

    def tail_rows(part):
        return pl.ds(part * (Fz // PARTS), Fz // PARTS)

    def tail_send(part, k):
        to = kinds[k]
        src = down_hbm.at[pl.ds(pl.multiple_of(to * Fz + part * (Fz // PARTS), 16), Fz // PARTS), pl.ds(Dh, Dh)]
        return remote(src, wdn.at[c, sp, 1, tail_rows(part)], s_z.at[0], r_tz.at[part], dev(to, x, y, c))

    def tail_x(part):
        piece = wdn.at[c, far_in * X + x, 1, tail_rows(part)]
        return remote(piece, piece, s_x.at[0], r_tx.at[part], x_mate)

    def tail_d(part, other):
        piece = wdn.at[c, far_in * X + (1 - x if other else x), 1, tail_rows(part)]
        return remote(piece, piece, s_d.at[0], r_td.at[other], c_mate)

    def tail1(part):
        came(wdn.at[c, far_in * X + x, 1, tail_rows(part)], r_tz.at[part])
        tail_x(part).start()
        tail_d(part, 0).start()

    def tail2(part):
        tail_x(part).wait_recv()
        tail_d(part, 1).start()

    def tail3(other):
        came(wdn.at[1 - c, far_in * X + (1 - x if other else x), 1], r_td.at[other])

    def hop2(up, h, k):
        x_copy(up, h, k).wait_recv()
        d_copy(up, h, k, 1).start()

    def hop3_up():
        came(wup.at[1 - c], r_d_up.at[0])

    def hop3_near():
        came(wdn.at[1 - c, pl.ds(side * 2 * X, 2 * X)], r_d_down.at[0])

    def hop3_far(h, k):
        came(wdn.at[1 - c, kinds[k] * X], r_d_down.at[1 + (k - 2) * 2 + h])

    def res_copy(k):
        to = lax.rem(tp + k, ntp)
        return remote(resid_hbm.at[pl.ds(pl.multiple_of(to * q, q), q), :], resid_in.at[k - 1], s_res.at[0],
                      r_res.at[0], (sp, to))

    barrier = pltpu.get_barrier_semaphore()
    for k in range(1, nsp):
        pl.semaphore_signal(barrier, inc=1, device_id=(lax.rem(sp + k, nsp), tp), device_id_type=MESH)
    for k in range(1, ntp):
        pl.semaphore_signal(barrier, inc=1, device_id=(sp, lax.rem(tp + k, ntp)), device_id_type=MESH)
    for copy in in_copies + lin_copies:
        copy.start()

    pl.semaphore_wait(barrier, nsp + ntp - 2)

    @pl.when(outer)
    def _():
        for k in (2, 3):
            z_copy(1, 0, k).start()

    @pl.when(inner)
    def _():
        z_copy(1, 0, 1).start()

    for h in range(2):
        x_copy(1, h, 0).start()
        d_copy(1, h, 0, 0).start()
    for k in range(1, ntp):
        res_copy(k).start()
    emit_copy.start()
    for up in (1, 0):
        for h in range(2):
            own_copy(up, h).start()

    lane = lax.broadcasted_iota(jnp.int32, (G, S), 1)
    group = jnp.where(lane < SL, 2 * (lane // PL), 2 * ((lane - SL) // PS) + 1)
    spread = (group == lax.broadcasted_iota(jnp.int32, (G, S), 0)).astype(F32)
    r = lax.broadcasted_iota(jnp.int32, (n, n), 0)
    t = lax.broadcasted_iota(jnp.int32, (n, n), 1)
    mix = (t == (r % SUB) * L + r // SUB).astype(F32)

    def per_state(ref):
        moved = lax.dot_general(ref[...], mix, (((1,), (1,)), ((), ())),
                                precision=lax.Precision.HIGHEST, preferred_element_type=F32)
        return lax.dot_general(moved, spread, (((0,), (0,)), ((), ())),
                               precision=lax.Precision.HIGHEST, preferred_element_type=F32)

    for copy in in_copies[:2]:
        copy.wait()
    pace[...] = per_state(dt_ref)
    surge[...] = per_state(lf_ref)

    def flat_kind(ref, e):
        many, states = ref.shape[1:]
        width = half * states
        repeat = (lax.broadcasted_iota(jnp.int32, (states, width), 1) % states
                  == lax.broadcasted_iota(jnp.int32, (states, width), 0)).astype(F32)
        wide = jnp.dot(ref[e], repeat, precision=lax.Precision.HIGHEST, preferred_element_type=F32)
        owner = tp * half + lax.broadcasted_iota(jnp.int32, (many, width), 1) // states
        mine = owner == lax.broadcasted_iota(jnp.int32, (many, width), 0)
        return jnp.sum(jnp.where(mine, wide, 0.0), axis=0, keepdims=True)

    def flat(long_ref, short_ref, e):
        return jnp.concatenate([flat_kind(long_ref, e), flat_kind(short_ref, e)], axis=1)

    def widened(ref, index, states, sign):
        rows, width = half * CHAN, half * states
        repeat = (lax.broadcasted_iota(jnp.int32, (states, width), 1) % states
                  == lax.broadcasted_iota(jnp.int32, (states, width), 0)).astype(BF16)
        wide = jnp.dot(ref[index].reshape(rows, states).astype(BF16), repeat, preferred_element_type=F32)
        own_block = (lax.broadcasted_iota(jnp.int32, (rows, width), 0) // CHAN
                     == lax.broadcasted_iota(jnp.int32, (rows, width), 1) // states)
        return jnp.where(own_block, sign * wide, 0.0).astype(BF16)

    def block_map(index, sign=1.0):
        long_part = widened(lin_l, index, PL, sign)
        short_part = widened(lin_s, index, PS, sign)
        no_long, no_short = jnp.zeros((CHAN, SL), BF16), jnp.zeros((CHAN, S - SL), BF16)
        bands = []
        for g in range(half):
            band = slice(g * CHAN, (g + 1) * CHAN)
            bands.append(jnp.concatenate([long_part[band], no_short], axis=1))
            bands.append(jnp.concatenate([no_long, short_part[band]], axis=1))
        return jnp.concatenate(bands, axis=0)

    for copy in in_copies[2:]:
        copy.wait()
    xv = jnp.dot(mix.astype(BF16), x_ref[...], preferred_element_type=F32).astype(BF16)
    for kind, ref in enumerate((lin_l, lin_s)):
        pltpu.make_async_copy(ref, ref, lin_sem.at[kind]).wait()
    for e in range(2):
        for part in range(2):
            st[:, pl.ds((2 * e + part) * S, S)] = jnp.dot(
                xv, block_map(4 * e + part), preferred_element_type=F32)

    for e in range(2):
        rate = flat(long_rate, short_rate, e)
        freq = flat(long_freq, short_freq, e)

        def step(i, carry):
            pr, pi, sr, si = carry
            at = i if e == 0 else L - 1 - i
            rows = pl.ds(pl.multiple_of(at * SUB, SUB), SUB)
            d = pace[rows, :]
            rd = rate * d
            m = jnp.exp(surge[rows, :] - rd)
            cos_v, sin_v = sincos(freq * d)
            w = jnp.sqrt(one_minus_exp_neg(2.0 * rd))
            ar, ai = m * cos_v, m * sin_v
            pr, pi = cmul(ar, ai, pr, pi)
            sr, si = cmul(ar, ai, sr, si)
            sr = sr + w * st[rows, pl.ds(2 * e * S, S)]
            si = si + w * st[rows, pl.ds((2 * e + 1) * S, S)]
            pre[rows, pl.ds(2 * e * S, S)] = pr
            pre[rows, pl.ds((2 * e + 1) * S, S)] = pi
            st[rows, pl.ds(2 * e * S, S)] = sr
            st[rows, pl.ds((2 * e + 1) * S, S)] = si
            return pr, pi, sr, si

        zero = jnp.zeros((SUB, S), F32)
        total = lax.fori_loop(0, L, step, (zero + 1.0, zero, zero, zero))
        for part in range(4):
            blk[4 * e + part] = total[part]
        order = range(SUB) if e == 0 else range(SUB - 1, -1, -1)
        run = None
        for b in order:
            now = tuple(blk[4 * e + part, b : b + 1, :] for part in range(4))
            if run is None:
                run = now
            else:
                p = cmul(now[0], now[1], run[0], run[1])
                s = cmul(now[0], now[1], run[2], run[3])
                run = (p[0], p[1], s[0] + now[2], s[1] + now[3])
        for part in range(4):
            ends[e, part : part + 1, :] = run[part]

    def ends_copy(e, k):
        return remote(ends.at[e], ends_all.at[e, k - 1], s_ends.at[0], r_ends.at[0],
                      (sp + k if e == 0 else sp - k, tp))

    def has_after(e, k):
        return sp + k < nsp if e == 0 else sp >= k

    def has_before(e, k):
        return has_after(1 - e, k)

    for k in range(1, nsp):
        for e in range(2):
            @pl.when(has_after(e, k))
            def _():
                ends_copy(e, k).start()

    @pl.when(inner)
    def _():
        for k in (2, 3):
            z_copy(1, 0, k).start()
        z_copy(1, 1, 1).start()

    @pl.when(outer)
    def _():
        for h in range(2):
            z_copy(1, h, 1).start()
        for k in (2, 3):
            z_copy(1, 1, k).start()
        hop1(1, 0, 1)

    read = jnp.concatenate(
        [block_map(2), block_map(3, -1.0), block_map(6), block_map(7, -1.0)], axis=1)

    came(ends_all.at[0], r_ends.at[0])
    blank = jnp.zeros((1, S), F32)

    def fold(j, carry, e):
        cr, ci = carry
        k = nsp - 1 - j
        got = ends_all[e, k - 1]
        nr, ni = cmul(got[0:1], got[1:2], cr, ci)
        reached = has_before(e, k)
        return jnp.where(reached, nr + got[2:3], cr), jnp.where(reached, ni + got[3:4], ci)

    for e in range(2):
        cr, ci = lax.fori_loop(0, nsp - 1, functools.partial(fold, e=e), (blank, blank))
        order = range(SUB) if e == 0 else range(SUB - 1, -1, -1)
        for b in order:
            cin[2 * e, b : b + 1, :] = cr
            cin[2 * e + 1, b : b + 1, :] = ci
            now = tuple(blk[4 * e + part, b : b + 1, :] for part in range(4))
            nr, ni = cmul(now[0], now[1], cr, ci)
            cr, ci = nr + now[2], ni + now[3]

        inr, ini = cin[2 * e], cin[2 * e + 1]

        def settle(i, _):
            rows = pl.ds(pl.multiple_of(i * SUB, SUB), SUB)
            re, im = pl.ds(2 * e * S, S), pl.ds((2 * e + 1) * S, S)
            ar, ai = cmul(pre[rows, re], pre[rows, im], inr, ini)
            st[rows, re] = st[rows, re] + ar
            st[rows, im] = st[rows, im] + ai
            return 0

        lax.fori_loop(0, L, settle, 0)

    v = lax.dot_general(st[...].astype(BF16), read, (((1,), (1,)), ((), ())),
                        preferred_element_type=F32)
    own = pl.ds(pl.multiple_of(tp * W, 128), W)
    skip_row, gain_row = skip_ref[:, own], gain_ref[:, own]
    v = v + skip_row * xv.astype(F32)
    v = 0.5 * v * (1.0 + jnp.tanh(0.7978845608028654 * (v + 0.044715 * v * v * v)))
    heads = []
    for h in range(W // NORM_W):
        head = v[:, h * NORM_W : (h + 1) * NORM_W]
        scale = lax.rsqrt(jnp.mean(head * head, axis=1, keepdims=True) + EPSILON)
        heads.append(head * scale * gain_row[:, h * NORM_W : (h + 1) * NORM_W])
    merged = jnp.concatenate(heads, axis=1).astype(BF16)
    t = lax.broadcasted_iota(jnp.int32, (n, n), 0)
    r = lax.broadcasted_iota(jnp.int32, (n, n), 1)
    unmix = (r == (t % L) * SUB + t // L).astype(BF16)
    mg[...] = jnp.dot(unmix, merged, preferred_element_type=F32).astype(BF16).reshape(ntp, q, W)

    def row_copy(k):
        to = lax.rem(tp + k, ntp)
        return remote(mg.at[to], rows_in.at[k - 1], s_rows.at[0], r_rows.at[0], (sp, to))

    for k in range(1, ntp):
        row_copy(k).start()

    @pl.when(inner)
    def _():
        for h in range(2):
            z_copy(0, h, 1).start()

    for h in range(2):
        hop2(1, h, 0)

    hop1(1, 0, 3)

    @pl.when(inner)
    def _():
        hop1(1, 0, 1)

    hop1(1, 1, 1)
    emit_copy.wait()
    mrg[:, pl.ds(pl.multiple_of(tp * W, 128), W)] = mg[tp]
    mid_out[:, pl.ds(pl.multiple_of(tp * Dl, 128), Dl)] = resid_ref[...].astype(F32)
    came(resid_in, r_res.at[0])
    came(rows_in, r_rows.at[0])
    for k in range(1, ntp):
        src = lax.rem(tp - k + ntp, ntp)
        mid_out[:, pl.ds(pl.multiple_of(src * Dl, 128), Dl)] = resid_in[k - 1].astype(F32)
        mrg[:, pl.ds(pl.multiple_of(src * W, 128), W)] = rows_in[k - 1]
    mid = mid_out[...] + jnp.dot(mrg[...], emit[...], preferred_element_type=F32)
    mid_out[...] = mid
    scale = lax.rsqrt(jnp.mean(mid * mid, axis=1, keepdims=True) + EPSILON)
    nrm[0, z] = (mid * scale * lead_ref[...]).astype(BF16)

    def t_far():
        return remote(nrm.at[0, z], nrm.at[0, z], s_t.at[0], r_t.at[as_seen - 1], dev(far_in, x, y, c))

    def t_mate(k):
        block = nrm.at[0, kinds[k]]
        return remote(block, block, s_t.at[0 if k == 0 else 1], r_t.at[max(k, 1) - 1], dev(mate, x, y, c))

    def t_wait(k):
        t_mate(k).wait_recv()

    def y_copy(k):
        return remote(nrm.at[0, kinds[k]], nrm.at[1, kinds[k]], s_y.at[0], r_y.at[0], y_mate)

    t_far().start()
    t_mate(0).start()
    y_copy(0).start()

    @pl.when(inner)
    def _():
        for k in (2, 3):
            z_copy(1, 1, k).start()

    @pl.when(outer)
    def _():
        for h in range(2):
            z_copy(0, h, 1).start()

    for h in range(2):
        x_copy(0, h, 0).start()
        d_copy(0, h, 0, 0).start()

    hop2(1, 0, 3)
    hop1(1, 1, 3)
    hop2(1, 0, 1)
    hop1(1, 0, 2)
    t_wait(1)
    y_copy(1).start()

    @pl.when(inner)
    def _():
        for k in (3, 2):
            t_wait(k)
            t_mate(k).start()
            y_copy(k).start()

    hop2(1, 1, 1)
    hop2(1, 1, 3)
    hop2(1, 0, 2)

    hop1(1, 1, 2)

    @pl.when(inner)
    def _():
        for k in (2, 3):
            z_copy(0, 0, k).start()

    @pl.when(outer)
    def _():
        z_copy(0, 0, 2).start()
        for k in (3, 2):
            t_wait(k)
            y_copy(k).start()
        z_copy(0, 0, 3).start()
        for k in (2, 3):
            z_copy(0, 1, k).start()

    for h in range(2):
        hop1(0, h, 1)
    for h in range(2):
        hop2(0, h, 0)
    hop2(1, 1, 2)
    came(nrm.at[1], r_y.at[0])
    own_wait(1)
    hop3_up()
    rows = nrm[...].reshape(2 * Z * q, D)
    for b in range(2):
        upward = jnp.dot(rows, wup[b].reshape(D, Fz), preferred_element_type=F32)
        hid[b] = jnp.square(jnp.maximum(upward, 0.0)).astype(BF16)

    def cols(zs, x_, h):
        return pl.ds(pl.multiple_of((zs * X + x_) * 2 * Dh + h * Dh, 128), Dh)

    def a_copy(zs, h):
        g = zs * 2 + h
        return remote(a_out.at[g], a_in.at[g], s_a.at[0], r_a.at[g], y_mate)

    def b_copy(zs, h):
        g = zs * 2 + h
        return remote(b_out.at[g, mate], b_in.at[g, mate], s_b.at[0], r_b.at[0, g], dev(mate, x, y, c))

    def b_far(zs, h):
        g = zs * 2 + h
        blocks = pl.ds(far0, 2)
        return remote(b_out.at[g, blocks], b_in.at[g, blocks], s_b.at[1], r_b.at[1, g], dev(mate, x, y, c))

    def c_copy(zs, h, i):
        g = zs * 2 + h
        return remote(c_out.at[g, i], c_in.at[tp, h], s_c.at[0], r_c.at[0], ((far0 + i) * X + x, zs))

    def stage_a(zs, h):
        g = zs * 2 + h
        for x_ in range(X):
            total = jnp.dot(hid[0], wdn[0, zs * X + x_, h], preferred_element_type=F32)
            total = total + jnp.dot(hid[1], wdn[1, zs * X + x_, h], preferred_element_type=F32)
            total = total.reshape(2, Z, q, Dh)
            a_out[g, :, x_] = total[1].astype(BF16)
            loc[g, :, x_] = total[0]
        a_copy(zs, h).start()

    def stage_b(zs, h):
        g = zs * 2 + h
        a_copy(zs, h).wait_recv()
        total = loc[g] + a_in[g].astype(F32)
        loc[g] = total
        b_out[g] = total.astype(BF16)

        @pl.when(outer)
        def _():
            b_far(zs, h).start()

        b_copy(zs, h).start()

    def keep(zs, src, dst):
        @pl.when(zs == tp)
        def _():
            dst[...] = src[...]

        @pl.when(zs != tp)
        def _():
            remote(src, dst, s_own.at[0], r_own.at[0], (sp, zs)).start()

    def stage_c(zs, h):
        g = zs * 2 + h

        @pl.when(inner)
        def _():
            b_far(zs, h).wait_recv()
            blocks = pl.ds(far0, 2)
            c_out[g] = (loc[g, blocks] + b_in[g, blocks].astype(F32)).astype(BF16)
            for i in range(2):
                c_copy(zs, h, i).start()

        b_copy(zs, h).wait_recv()
        o_out[g] = (loc[g, z] + b_in[g, z].astype(F32)).astype(BF16)
        keep(zs, o_out.at[g], c_in.at[tp, 3 + h])

    last = far_in * 2 + 1

    def tail_copy(xd, other):
        return remote(a_out.at[last, :, xd], a_in.at[last, :, xd], s_a.at[0], r_ta.at[other], y_mate)

    def tail_a(other):
        xd = 1 - x if other else x
        total = jnp.dot(hid[0], wdn[0, far_in * X + xd, 1], preferred_element_type=F32)
        total = total + jnp.dot(hid[1], wdn[1, far_in * X + xd, 1], preferred_element_type=F32)
        total = total.reshape(2, Z, q, Dh)
        a_out[last, :, xd] = total[1].astype(BF16)
        loc[last, :, xd] = total[0]
        tail_copy(xd, other).start()

    def tail_sums(other):
        xd = 1 - x if other else x
        tail_copy(xd, other).wait_recv()
        b_out[last, :, xd] = (loc[last, :, xd] + a_in[last, :, xd].astype(F32)).astype(BF16)
        for i in range(2):
            to = far0 + i
            remote(b_out.at[last, to, xd], c_in.at[tp, as_seen - 1, xd], s_last.at[0], r_c.at[as_seen - 2],
                   (to * X + x, far_in)).start()
        remote(b_out.at[last, mate, xd], c_in.at[tp, 2, xd], s_last.at[0], r_c.at[1], (mate * X + x, far_in)).start()
        keep(far_in, b_out.at[last, z, xd], c_in.at[tp, 4, xd])

    def home_copy(zs):
        return remote(mid_out.at[:, pl.ds(pl.multiple_of(zs * Dl, 128), Dl)], home_in.at[tp], s_home.at[0],
                      r_home.at[0], (sp, zs))

    turns = [(zs, h) for zs in (half_in, half_out, far_out, far_in) for h in range(2)]
    hop1(0, 0, 3)

    @pl.when(inner)
    def _():
        for part in range(PARTS):
            for k in (2, 3):
                tail_send(part, k).start()

    for zs in range(Z):
        @pl.when(zs == tp)
        def _():
            home_in[tp] = mid_out[:, zs * Dl : (zs + 1) * Dl]

        @pl.when(zs != tp)
        def _():
            home_copy(zs).start()

    own_wait(0)
    for h in range(2):
        hop2(0, h, 1)
    hop3_near()
    stage_a(*turns[0])
    stage_a(*turns[1])
    stage_a(*turns[2])
    stage_a(*turns[3])
    hop1(0, 1, 3)
    stage_b(*turns[0])
    hop2(0, 0, 3)
    stage_b(*turns[1])
    hop1(0, 0, 2)
    hop3_far(0, 3)
    stage_a(*turns[4])
    stage_b(*turns[2])
    hop2(0, 1, 3)
    tail1(0)
    stage_b(*turns[3])
    tail1(1)
    hop3_far(1, 3)
    stage_a(*turns[5])
    stage_b(*turns[4])
    hop2(0, 0, 2)
    tail1(2)
    stage_c(*turns[0])
    tail1(3)
    hop3_far(0, 2)
    stage_a(*turns[6])
    tail2(0)
    stage_c(*turns[1])
    stage_c(*turns[2])
    tail2(1)
    tail3(0)
    tail_a(0)
    stage_c(*turns[3])
    tail2(2)
    stage_b(*turns[5])
    tail2(3)
    tail3(1)
    tail_a(1)
    stage_b(*turns[6])
    tail_sums(0)
    stage_c(*turns[4])
    stage_c(*turns[5])
    tail_sums(1)
    stage_c(*turns[6])
    came(home_in.at[pl.ds(0, ntp - 1)], r_home.at[0])
    came(c_in.at[pl.ds(0, ntp - 1), pl.ds(3, 2)], r_own.at[0])
    came(c_in.at[:, pl.ds(0, 2)], r_c.at[0])

    @pl.when((tp == half_in) | (tp == far_in))
    def _():
        came(c_in.at[:, 2], r_c.at[1])
        for x_ in range(X):
            at = pl.ds((2 * x_ + 1) * Dh, Dh)
            home_in[:, :, at] = home_in[:, :, at] + c_in[:, 2, x_].astype(F32)

    for src in range(ntp):
        for x_ in range(X):
            for h in range(2):
                at = pl.ds((2 * x_ + h) * Dh, Dh)
                total = home_in[src, :, at] + c_in[src, h, x_].astype(F32) + c_in[src, 3 + h, x_].astype(F32)
                out_ref[pl.ds(src * q, q), at] = total.astype(BF16)

    sent(wup.at[0, pl.ds(0, 6)], s_z.at[0])
    sent(wup.at[0], s_x.at[0])
    sent(wup, s_d.at[0])
    sent(ends_all.at[0], s_ends.at[0])
    sent(nrm.at[0, pl.ds(0, 2)], s_t.at[0])
    sent(nrm.at[0], s_y.at[0])
    sent(a_out, s_a.at[0])
    sent(b_out.at[pl.ds(0, 2 * Z - 1), 0], s_b.at[0])
    sent(b_out.at[0, pl.ds(0, 3)], s_last.at[0])
    sent(c_in.at[pl.ds(0, ntp - 1), pl.ds(3, 2)], s_own.at[0])
    sent(home_in.at[pl.ds(0, ntp - 1)], s_home.at[0])
    sent(resid_in, s_res.at[0])
    sent(rows_in, s_rows.at[0])

    @pl.when(inner)
    def _():
        sent(nrm.at[0, pl.ds(0, 2)], s_t.at[1])
        sent(c_out.at[pl.ds(0, 2 * Z - 1)], s_c.at[0])

    @pl.when(outer)
    def _():
        sent(b_out.at[pl.ds(0, 2 * Z - 1), pl.ds(0, 2)], s_b.at[1])


def paired_call(nsp, ntp, residual, lifted, dts, long_rate, short_rate, emitted, raising):
    n, W = lifted.shape
    G = dts.shape[0]
    half = G // 2
    PL, PS = long_rate.shape[2], short_rate.shape[2]
    S = half * (PL + PS)
    D = emitted.shape[1]
    Dl = residual.shape[1]
    q = n // ntp
    Z, X, Y = mesh_split(nsp, ntp)
    Fz = raising.shape[1] // Z
    Dh = D // nsp // 2
    groups = 2 * Z
    cfg = (nsp, ntp, n, S, W, G, PL, PS, D, Fz)
    vm = pl.BlockSpec(memory_space=pltpu.VMEM)
    dma = pltpu.SemaphoreType.DMA
    return pl.pallas_call(
        functools.partial(paired_body, cfg),
        out_shape=jax.ShapeDtypeStruct((n, Dl), BF16),
        in_specs=[pl.BlockSpec(memory_space=pl.ANY)] * 16,
        out_specs=vm,
        scratch_shapes=[
            pltpu.VMEM(lifted.shape, BF16), pltpu.VMEM(dts.shape, F32), pltpu.VMEM(dts.shape, F32),
            *[pltpu.VMEM(long_rate.shape, F32), pltpu.VMEM(short_rate.shape, F32)] * 2,
            pltpu.VMEM((1, ntp * W), F32), pltpu.VMEM((1, ntp * W), F32), pltpu.VMEM((q, Dl), BF16),
            pltpu.VMEM((1, D), F32), dma((11,)),
            pltpu.VMEM((8, half, CHAN, PL), F32), pltpu.VMEM((8, half, CHAN, PS), F32), dma((2,)),
            pltpu.VMEM((n, S), F32), pltpu.VMEM((n, S), F32),
            pltpu.VMEM((n, 4 * S), F32), pltpu.VMEM((n, 4 * S), F32),
            pltpu.VMEM((8, SUB, S), F32), pltpu.VMEM((2, 4, S), F32), pltpu.VMEM((2, nsp - 1, 4, S), F32),
            pltpu.VMEM((4, SUB, S), F32),
            pltpu.VMEM((ntp, q, W), BF16), pltpu.VMEM((ntp - 1, q, W), BF16),
            pltpu.VMEM((q, ntp * W), BF16), pltpu.VMEM(emitted.shape, BF16),
            pltpu.VMEM((ntp - 1, q, Dl), BF16),
            pltpu.VMEM((q, D), F32),
            pltpu.VMEM((2, nsp, 2, D // nsp // 2, Fz), BF16), pltpu.VMEM((2, nsp, 2, Fz, Dh), BF16),
            pltpu.VMEM((2, Z, q, D), BF16), pltpu.VMEM((2, 2 * Z * q, Fz), BF16),
            pltpu.VMEM((groups, Z, X, q, Dh), F32),
            *[pltpu.VMEM((groups, Z, X, q, Dh), BF16)] * 4,
            pltpu.VMEM((groups, 2, X, q, Dh), BF16), pltpu.VMEM((ntp, 5, X, q, Dh), BF16),
            pltpu.VMEM((ntp, q, Dl), F32),
            dma((1,)), dma((2,)), *[dma((1,))] * 6,
            dma((1,)), dma((2, 2, 3)), dma((1,)), dma((2, 2, 4)), dma((1,)), dma((1,)), dma((5,)),
            dma((2,)), dma((3,)), dma((1,)), dma((1,)),
            dma((1,)), dma((groups,)), dma((2,)), dma((2, groups)), dma((1,)), dma((2,)), *[dma((1,))] * 3,
            pltpu.VMEM((groups, X, q, Dh), BF16), dma((1,)), dma((1,)), dma((PARTS,)), dma((PARTS,)), dma((2,)), dma((2,)),
        ],
        compiler_params=pltpu.CompilerParams(collective_id=0, has_side_effects=True),
        cost_estimate=pl.CostEstimate(flops=10**9, bytes_accessed=3 * 10**7, transcendentals=10**6),
    )


def on_device(residual, lifted, dts, fades, long_rate, short_rate, long_freq, short_freq,
              long_lin, short_lin, skip, closing, emitted, leading, raising, lowering):
    nsp, ntp = lax.axis_size("sp"), lax.axis_size("tp")
    operands = (lifted, dts, fades, long_rate, short_rate, long_freq, short_freq, skip[None], closing[None],
                residual, leading[None], long_lin.swapaxes(4, 5), short_lin.swapaxes(4, 5), emitted, raising, lowering)
    Z, X, Y = mesh_split(nsp, ntp)
    if X == 2 and Y == 2 and Z == ntp:
        return paired_call(nsp, ntp, residual, lifted, dts, long_rate, short_rate, emitted, raising)(*operands)
    n, W = lifted.shape
    G = dts.shape[0]
    half = G // 2
    PL, PS = long_rate.shape[2], short_rate.shape[2]
    S = half * (PL + PS)
    D = emitted.shape[1]
    Dl = residual.shape[1]
    q = n // ntp
    c_ff = min(nsp, raising.shape[1] // 128)
    F = raising.shape[1] // c_ff
    q_all, M = c_ff * q, ntp // 2
    cfg = (nsp, ntp, n, S, W, G, PL, PS, D, c_ff, F)
    vm = pl.BlockSpec(memory_space=pltpu.VMEM)
    dma = pltpu.SemaphoreType.DMA
    return pl.pallas_call(
        functools.partial(mixer_body, cfg),
        out_shape=jax.ShapeDtypeStruct((n, Dl), BF16),
        in_specs=[vm] * 11 + [pl.BlockSpec(memory_space=pl.ANY)] * 5,
        out_specs=vm,
        scratch_shapes=[
            pltpu.VMEM((8, half, CHAN, PL), F32), pltpu.VMEM((8, half, CHAN, PS), F32), dma((2, 8)),
            pltpu.VMEM((n, S), F32), pltpu.VMEM((n, S), F32),
            pltpu.VMEM((n, 4 * S), F32), pltpu.VMEM((n, 4 * S), F32),
            pltpu.VMEM((8, SUB, S), F32), pltpu.VMEM((8, S), F32), pltpu.VMEM((nsp - 1, 8, S), F32),
            pltpu.VMEM((4, SUB, S), F32),
            pltpu.VMEM((ntp, q, W), BF16), pltpu.VMEM((ntp - 1, q, W), BF16),
            pltpu.VMEM((q, ntp * W), BF16), pltpu.VMEM(emitted.shape, BF16),
            pltpu.VMEM((ntp - 1, q, Dl), BF16),
            pltpu.VMEM((q, D), F32),
            pltpu.VMEM((ntp, nsp, D // nsp, F), BF16), pltpu.VMEM((ntp, nsp, F, D // nsp), BF16),
            pltpu.VMEM((c_ff, q, D), BF16), pltpu.VMEM((ntp, q_all, F), BF16),
            pltpu.VMEM((c_ff, q, D), BF16), pltpu.VMEM((c_ff - 1, q, D), BF16),
            pltpu.VMEM((ntp, q, Dl), BF16), pltpu.VMEM((ntp - 1, q, Dl), BF16),
            dma((3,)), dma((nsp - 1,)), dma((nsp - 1,)), dma((ntp - 1,)), dma((ntp - 1,)),
            dma((ntp - 1,)), dma((ntp - 1,)),
            *[dma((nsp - 1,))] * 4, *[dma((M - 1, nsp))] * 4, *[dma((M,))] * 4,
            *[dma((2, c_ff // 2))] * 2, *[dma((c_ff - 1,))] * 2, *[dma((ntp - 1,))] * 2,
        ],
        compiler_params=pltpu.CompilerParams(collective_id=0, has_side_effects=True),
        cost_estimate=pl.CostEstimate(flops=10**9, bytes_accessed=3 * 10**7, transcendentals=10**6),
    )(*operands)


def solution(mesh):
    both, swapped = P("sp", "tp"), P("tp", "sp")
    in_specs = (both, both, swapped, swapped) + (P(),) * 10 + (both, swapped)
    return jax.shard_map(on_device, mesh=mesh, in_specs=in_specs, out_specs=both, check_vma=False)
```

```python
import functools

import jax
import jax.numpy as jnp
from jax import lax
from jax.experimental import pallas as pl
from jax.experimental.pallas import tpu as pltpu
from jax.sharding import PartitionSpec as P

CHAN = 16
NORM_W = 128
EPSILON = 1e-06
SUB = 8
PARTS = 4
F32, BF16 = jnp.float32, jnp.bfloat16


def sincos(a):
    k = jnp.floor(a * 0.6366197723675814 + 0.5)
    r = a - k * 1.5703125
    r = r - k * 4.8351287841796875e-4
    r = r - k * 3.138556210e-7
    z = r * r
    s = r + r * z * (-1.6666654611e-1 + z * (8.3321608736e-3 + z * -1.9515295891e-4))
    c = 1.0 - 0.5 * z + z * z * (
        4.166664568298827e-2 + z * (-1.388731625493765e-3 + z * 2.443315711809948e-5)
    )
    half = jnp.floor(k * 0.5)
    odd = (k - 2.0 * half) > 0.5
    half_odd = (half - 2.0 * jnp.floor(half * 0.5)) > 0.5
    cos_v = jnp.where(odd, -s, c)
    sin_v = jnp.where(odd, c, s)
    return jnp.where(half_odd, -cos_v, cos_v), jnp.where(half_odd, -sin_v, sin_v)


def one_minus_exp_neg(u):
    t = jnp.full_like(u, 1.0)
    for m in range(10, 1, -1):
        t = 1.0 - u * (1.0 / m) * t
    return u * t


def cmul(ar, ai, br, bi):
    return ar * br - ai * bi, ar * bi + ai * br


def mixer_body(cfg, x_ref, dt_ref, lf_ref, long_rate, short_rate, long_freq, short_freq,
               skip_ref, gain_ref, resid_ref, lead_ref, long_hbm, short_hbm, emit_hbm, up_hbm, down_hbm,
               out_ref, lin_l, lin_s, lin_sem,
               pace, surge, pre, st, blk, ends, ends_all, cin, mg, rows_in, mrg, emit, resid_in,
               mid_out, wup, wdn, nrm, hid, part, rs_in, fin, fin_in,
               copy_sem, s_ends, r_ends, s_rows, r_rows, s_res, r_res,
               s_u1, r_u1, s_d1, r_d1, s_u2, r_u2, s_d2, r_d2, s_u3, r_u3, s_d3, r_d3,
               s_nrm, r_nrm, s_rs, r_rs, s_fin, r_fin):
    nsp, ntp, n, S, W, G, PL, PS, D, c_ff, F = cfg
    M = ntp // 2
    L = n // SUB
    half = G // 2
    SL = half * PL
    sp = lax.axis_index("sp")
    tp = lax.axis_index("tp")
    q = n // ntp
    Dl = D // ntp
    MESH = pl.DeviceIdType.MESH

    emit_copy = pltpu.make_async_copy(emit_hbm, emit, copy_sem.at[0])
    lin_copies = []
    for at in range(8):
        for kind, (src, dst) in enumerate(((long_hbm, lin_l), (short_hbm, lin_s))):
            lin_copies.append(pltpu.make_async_copy(
                src.at[at // 4, at // 2 % 2, at % 2, pl.ds(tp * half, half)], dst.at[at],
                lin_sem.at[kind, at]))
    for copy in lin_copies:
        copy.start()
    emit_copy.start()
    chunk = lax.rem(sp, c_ff)
    partner = tp + 1 - 2 * lax.rem(tp, 2)

    def cols(of):
        return pl.ds(pl.multiple_of(of * F, 128), F)

    own_up = pltpu.make_async_copy(up_hbm.at[:, cols(chunk)], wup.at[tp, sp], copy_sem.at[1])
    own_down = pltpu.make_async_copy(down_hbm.at[cols(chunk), :], wdn.at[tp, sp], copy_sem.at[2])
    own_up.start()
    own_down.start()

    def spread_copy(k, up):
        to = lax.rem(sp + k, nsp)
        src = up_hbm.at[:, cols(lax.rem(to, c_ff))] if up else down_hbm.at[cols(lax.rem(to, c_ff)), :]
        return pltpu.make_async_remote_copy(
            src_ref=src, dst_ref=(wup if up else wdn).at[tp, sp],
            send_sem=(s_u1 if up else s_d1).at[k - 1], recv_sem=(r_u1 if up else r_d1).at[k - 1],
            device_id=(to, tp), device_id_type=MESH)

    def across_copy(m, k, up):
        piece = (wup if up else wdn).at[tp, lax.rem(sp - k + nsp, nsp)]
        return pltpu.make_async_remote_copy(
            src_ref=piece, dst_ref=piece,
            send_sem=(s_u2 if up else s_d2).at[m - 1, k], recv_sem=(r_u2 if up else r_d2).at[m - 1, k],
            device_id=(sp, lax.rem(tp + 2 * m, ntp)), device_id_type=MESH)

    def pair_copy(m, up):
        piece = (wup if up else wdn).at[lax.rem(tp + 2 * m, ntp)]
        return pltpu.make_async_remote_copy(
            src_ref=piece, dst_ref=piece,
            send_sem=(s_u3 if up else s_d3).at[m], recv_sem=(r_u3 if up else r_d3).at[m],
            device_id=(sp, partner), device_id_type=MESH)

    def pass_on(first, last, up):
        for k in range(first, last):
            if k == 0:
                (own_up if up else own_down).wait()
            else:
                spread_copy(k, up).wait_recv()
            for m in range(1, M):
                across_copy(m, k, up).start()

    barrier = pltpu.get_barrier_semaphore()
    for k in range(1, nsp):
        pl.semaphore_signal(barrier, inc=1, device_id=(lax.rem(sp + k, nsp), tp), device_id_type=MESH)
    for k in range(1, ntp):
        pl.semaphore_signal(barrier, inc=1, device_id=(sp, lax.rem(tp + k, ntp)), device_id_type=MESH)
    pl.semaphore_wait(barrier, nsp + ntp - 2)

    def res_copy(k):
        to = lax.rem(tp + k, ntp)
        return pltpu.make_async_remote_copy(
            src_ref=resid_ref.at[pl.ds(to * q, q), :], dst_ref=resid_in.at[k - 1],
            send_sem=s_res.at[k - 1], recv_sem=r_res.at[k - 1],
            device_id=(sp, to), device_id_type=MESH)

    for k in range(1, nsp):
        spread_copy(k, True).start()
    for k in range(1, ntp):
        res_copy(k).start()

    lane = lax.broadcasted_iota(jnp.int32, (G, S), 1)
    group = jnp.where(lane < SL, 2 * (lane // PL), 2 * ((lane - SL) // PS) + 1)
    spread = (group == lax.broadcasted_iota(jnp.int32, (G, S), 0)).astype(F32)
    r = lax.broadcasted_iota(jnp.int32, (n, n), 0)
    t = lax.broadcasted_iota(jnp.int32, (n, n), 1)
    mix = (t == (r % SUB) * L + r // SUB).astype(F32)

    def per_state(ref):
        moved = lax.dot_general(ref[...], mix, (((1,), (1,)), ((), ())),
                                precision=lax.Precision.HIGHEST, preferred_element_type=F32)
        return lax.dot_general(moved, spread, (((0,), (0,)), ((), ())),
                               precision=lax.Precision.HIGHEST, preferred_element_type=F32)

    pace[...] = per_state(dt_ref)
    surge[...] = per_state(lf_ref)

    def flat_kind(ref, e):
        many, states = ref.shape[1:]
        width = half * states
        repeat = (lax.broadcasted_iota(jnp.int32, (states, width), 1) % states
                  == lax.broadcasted_iota(jnp.int32, (states, width), 0)).astype(F32)
        wide = jnp.dot(ref[e], repeat, precision=lax.Precision.HIGHEST, preferred_element_type=F32)
        owner = tp * half + lax.broadcasted_iota(jnp.int32, (many, width), 1) // states
        mine = owner == lax.broadcasted_iota(jnp.int32, (many, width), 0)
        return jnp.sum(jnp.where(mine, wide, 0.0), axis=0, keepdims=True)

    def flat(long_ref, short_ref, e):
        return jnp.concatenate([flat_kind(long_ref, e), flat_kind(short_ref, e)], axis=1)

    def widened(ref, index, states, sign):
        rows, width = half * CHAN, half * states
        repeat = (lax.broadcasted_iota(jnp.int32, (states, width), 1) % states
                  == lax.broadcasted_iota(jnp.int32, (states, width), 0)).astype(BF16)
        wide = jnp.dot(ref[index].reshape(rows, states).astype(BF16), repeat, preferred_element_type=F32)
        own_block = (lax.broadcasted_iota(jnp.int32, (rows, width), 0) // CHAN
                     == lax.broadcasted_iota(jnp.int32, (rows, width), 1) // states)
        return jnp.where(own_block, sign * wide, 0.0).astype(BF16)

    def block_map(index, sign=1.0):
        long_part = widened(lin_l, index, PL, sign)
        short_part = widened(lin_s, index, PS, sign)
        no_long, no_short = jnp.zeros((CHAN, SL), BF16), jnp.zeros((CHAN, S - SL), BF16)
        bands = []
        for g in range(half):
            band = slice(g * CHAN, (g + 1) * CHAN)
            bands.append(jnp.concatenate([long_part[band], no_short], axis=1))
            bands.append(jnp.concatenate([no_long, short_part[band]], axis=1))
        return jnp.concatenate(bands, axis=0)

    xv = jnp.dot(mix.astype(BF16), x_ref[...], preferred_element_type=F32).astype(BF16)
    for copy in lin_copies:
        copy.wait()
    for e in range(2):
        for c in range(2):
            st[:, pl.ds((2 * e + c) * S, S)] = jnp.dot(
                xv, block_map(4 * e + c), preferred_element_type=F32)

    for e in range(2):
        rate = flat(long_rate, short_rate, e)
        freq = flat(long_freq, short_freq, e)

        def step(i, carry):
            pr, pi, sr, si = carry
            at = i if e == 0 else L - 1 - i
            rows = pl.ds(pl.multiple_of(at * SUB, SUB), SUB)
            d = pace[rows, :]
            rd = rate * d
            m = jnp.exp(surge[rows, :] - rd)
            cos_v, sin_v = sincos(freq * d)
            w = jnp.sqrt(one_minus_exp_neg(2.0 * rd))
            ar, ai = m * cos_v, m * sin_v
            pr, pi = cmul(ar, ai, pr, pi)
            sr, si = cmul(ar, ai, sr, si)
            sr = sr + w * st[rows, pl.ds(2 * e * S, S)]
            si = si + w * st[rows, pl.ds((2 * e + 1) * S, S)]
            pre[rows, pl.ds(2 * e * S, S)] = pr
            pre[rows, pl.ds((2 * e + 1) * S, S)] = pi
            st[rows, pl.ds(2 * e * S, S)] = sr
            st[rows, pl.ds((2 * e + 1) * S, S)] = si
            return pr, pi, sr, si

        zero = jnp.zeros((SUB, S), F32)
        total = lax.fori_loop(0, L, step, (zero + 1.0, zero, zero, zero))
        for c in range(4):
            blk[4 * e + c] = total[c]
        order = range(SUB) if e == 0 else range(SUB - 1, -1, -1)
        run = None
        for b in order:
            now = tuple(blk[4 * e + c, b : b + 1, :] for c in range(4))
            if run is None:
                run = now
            else:
                p = cmul(now[0], now[1], run[0], run[1])
                s = cmul(now[0], now[1], run[2], run[3])
                run = (p[0], p[1], s[0] + now[2], s[1] + now[3])
        for c in range(4):
            ends[4 * e + c : 4 * e + c + 1, :] = run[c]

    def ends_copy(k):
        return pltpu.make_async_remote_copy(
            src_ref=ends, dst_ref=ends_all.at[k - 1],
            send_sem=s_ends.at[k - 1], recv_sem=r_ends.at[k - 1],
            device_id=(lax.rem(sp + k, nsp), tp), device_id_type=MESH)

    for k in range(1, nsp):
        ends_copy(k).start()
    for k in range(1, nsp):
        spread_copy(k, False).start()

    read = jnp.concatenate(
        [block_map(2), block_map(3, -1.0), block_map(6), block_map(7, -1.0)], axis=1)

    pass_on(0, nsp // 2, True)
    for k in range(1, nsp):
        ends_copy(k).wait_recv()
    blank = jnp.zeros((1, S), F32)

    def fold(j, carry, e):
        cr, ci = carry
        k = nsp - 1 - j if e == 0 else j + 1
        reached = k <= sp if e == 0 else nsp - k <= nsp - 1 - sp
        got = ends_all[k - 1]
        nr, ni = cmul(got[4 * e : 4 * e + 1], got[4 * e + 1 : 4 * e + 2], cr, ci)
        nr = nr + got[4 * e + 2 : 4 * e + 3]
        ni = ni + got[4 * e + 3 : 4 * e + 4]
        return jnp.where(reached, nr, cr), jnp.where(reached, ni, ci)

    for e in range(2):
        cr, ci = lax.fori_loop(0, nsp - 1, functools.partial(fold, e=e), (blank, blank))
        order = range(SUB) if e == 0 else range(SUB - 1, -1, -1)
        for b in order:
            cin[2 * e, b : b + 1, :] = cr
            cin[2 * e + 1, b : b + 1, :] = ci
            now = tuple(blk[4 * e + c, b : b + 1, :] for c in range(4))
            nr, ni = cmul(now[0], now[1], cr, ci)
            cr, ci = nr + now[2], ni + now[3]

        inr, ini = cin[2 * e], cin[2 * e + 1]

        def settle(i, _):
            rows = pl.ds(pl.multiple_of(i * SUB, SUB), SUB)
            re, im = pl.ds(2 * e * S, S), pl.ds((2 * e + 1) * S, S)
            ar, ai = cmul(pre[rows, re], pre[rows, im], inr, ini)
            st[rows, re] = st[rows, re] + ar
            st[rows, im] = st[rows, im] + ai
            return 0

        lax.fori_loop(0, L, settle, 0)

    y = lax.dot_general(st[...].astype(BF16), read, (((1,), (1,)), ((), ())),
                        preferred_element_type=F32)
    own = pl.ds(pl.multiple_of(tp * W, 128), W)
    skip_row, gain_row = skip_ref[:, own], gain_ref[:, own]
    y = y + skip_row * xv.astype(F32)
    y = 0.5 * y * (1.0 + jnp.tanh(0.7978845608028654 * (y + 0.044715 * y * y * y)))
    heads = []
    for h in range(W // NORM_W):
        head = y[:, h * NORM_W : (h + 1) * NORM_W]
        scale = lax.rsqrt(jnp.mean(head * head, axis=1, keepdims=True) + EPSILON)
        heads.append(head * scale * gain_row[:, h * NORM_W : (h + 1) * NORM_W])
    merged = jnp.concatenate(heads, axis=1).astype(BF16)
    t = lax.broadcasted_iota(jnp.int32, (n, n), 0)
    r = lax.broadcasted_iota(jnp.int32, (n, n), 1)
    unmix = (r == (t % L) * SUB + t // L).astype(BF16)
    mg[...] = jnp.dot(unmix, merged, preferred_element_type=F32).astype(BF16).reshape(ntp, q, W)

    def row_copy(k):
        to = lax.rem(tp + k, ntp)
        return pltpu.make_async_remote_copy(
            src_ref=mg.at[to], dst_ref=rows_in.at[k - 1],
            send_sem=s_rows.at[k - 1], recv_sem=r_rows.at[k - 1],
            device_id=(sp, to), device_id_type=MESH)

    for k in range(1, ntp):
        row_copy(k).start()
    pass_on(nsp // 2, nsp, True)
    emit_copy.wait()
    mrg[:, pl.ds(pl.multiple_of(tp * W, 128), W)] = mg[tp]
    mid_out[:, pl.ds(pl.multiple_of(tp * Dl, 128), Dl)] = resid_ref[pl.ds(pl.multiple_of(tp * q, q), q), :].astype(F32)
    for k in range(1, ntp):
        src = lax.rem(tp - k + ntp, ntp)
        res_copy(k).wait_recv()
        mid_out[:, pl.ds(pl.multiple_of(src * Dl, 128), Dl)] = resid_in[k - 1].astype(F32)
        row_copy(k).wait_recv()
        mrg[:, pl.ds(pl.multiple_of(src * W, 128), W)] = rows_in[k - 1]
    mid = mid_out[...] + jnp.dot(mrg[...], emit[...], preferred_element_type=F32)
    mid_out[...] = mid
    scale = lax.rsqrt(jnp.mean(mid * mid, axis=1, keepdims=True) + EPSILON)
    base, q_all = sp - chunk, c_ff * q
    nrm[chunk] = (mid * scale * lead_ref[...]).astype(BF16)

    def peer(k):
        return lax.rem(chunk + k, c_ff)

    H = c_ff // 2

    def nrm_across(m):
        return pltpu.make_async_remote_copy(
            src_ref=nrm.at[chunk], dst_ref=nrm.at[chunk],
            send_sem=s_nrm.at[0, m], recv_sem=r_nrm.at[0, m],
            device_id=(base + peer(2 * m), tp), device_id_type=MESH)

    def nrm_pair(m):
        return pltpu.make_async_remote_copy(
            src_ref=nrm.at[peer(2 * m)], dst_ref=nrm.at[peer(2 * m)],
            send_sem=s_nrm.at[1, m], recv_sem=r_nrm.at[1, m],
            device_id=(base + chunk + 1 - 2 * lax.rem(chunk, 2), tp), device_id_type=MESH)

    def rs_copy(k):
        return pltpu.make_async_remote_copy(
            src_ref=part.at[peer(k)], dst_ref=rs_in.at[k - 1],
            send_sem=s_rs.at[k - 1], recv_sem=r_rs.at[k - 1],
            device_id=(base + peer(k), tp), device_id_type=MESH)

    def fin_copy(k):
        to = lax.rem(tp + k, ntp)
        return pltpu.make_async_remote_copy(
            src_ref=fin.at[to], dst_ref=fin_in.at[k - 1],
            send_sem=s_fin.at[k - 1], recv_sem=r_fin.at[k - 1],
            device_id=(sp, to), device_id_type=MESH)

    for m in range(1, H):
        nrm_across(m).start()
    nrm_pair(0).start()
    pair_copy(0, True).start()
    pass_on(0, nsp, False)
    pair_copy(0, False).start()
    for m in range(1, H):
        nrm_across(m).wait_recv()
        nrm_pair(H - m).start()
    for up in (True, False):
        for m in range(1, M):
            for k in range(nsp):
                across_copy(m, k, up).wait_recv()
            pair_copy(M - m, up).start()
        if up:
            for m in range(M):
                pair_copy(m, True).wait_recv()
            for m in range(H):
                nrm_pair(m).wait_recv()
            rows = nrm[...].reshape(q_all, D)

            def raise_step(t, _):
                upward = jnp.dot(rows, wup[t].reshape(D, F), preferred_element_type=F32)
                hid[t] = jnp.square(jnp.maximum(upward, 0.0)).astype(BF16)
                return 0

            lax.fori_loop(0, ntp, raise_step, 0)
    for m in range(M):
        pair_copy(m, False).wait_recv()
    Dc = D // nsp
    for j in range(nsp):
        total = jnp.dot(hid[0], wdn[0, j], preferred_element_type=F32)
        for t in range(1, ntp):
            total = total + jnp.dot(hid[t], wdn[t, j], preferred_element_type=F32)
        part[:, :, j * Dc : (j + 1) * Dc] = total.astype(BF16).reshape(c_ff, q, Dc)
    for k in range(1, c_ff):
        rs_copy(k).start()
    result = mid_out[...] + part[chunk].astype(F32)
    for k in range(1, c_ff):
        rs_copy(k).wait_recv()
        result = result + rs_in[k - 1].astype(F32)
    result = result.astype(BF16)
    for t in range(ntp):
        fin[t] = result[:, t * Dl : (t + 1) * Dl]
    for k in range(1, ntp):
        fin_copy(k).start()
    out_ref[pl.ds(pl.multiple_of(tp * q, q), q), :] = fin[tp]
    for k in range(1, ntp):
        fin_copy(k).wait_recv()
        src = lax.rem(tp - k + ntp, ntp)
        out_ref[pl.ds(pl.multiple_of(src * q, q), q), :] = fin_in[k - 1]
    for k in range(1, c_ff):
        rs_copy(k).wait_send()
    for m in range(H):
        if m > 0:
            nrm_across(m).wait_send()
        nrm_pair(m).wait_send()
    for k in range(1, ntp):
        fin_copy(k).wait_send()
    for up in (True, False):
        for k in range(1, nsp):
            spread_copy(k, up).wait_send()
        for m in range(1, M):
            for k in range(nsp):
                across_copy(m, k, up).wait_send()
        for m in range(M):
            pair_copy(m, up).wait_send()
    for k in range(1, nsp):
        ends_copy(k).wait_send()
    for k in range(1, ntp):
        res_copy(k).wait_send()
        row_copy(k).wait_send()


def mesh_split(nsp, ntp):
    Y = ntp // 2
    X = Y if Y > 0 and nsp % Y == 0 else 1
    return nsp // X, X, Y


def thirds(a):
    high = a.astype(BF16)
    rest = a - high.astype(F32)
    middle = rest.astype(BF16)
    low = (rest - middle.astype(F32)).astype(BF16)
    return jnp.concatenate([high, middle, low], axis=0)


def paired_body(cfg, x_hbm, dt_hbm, lf_hbm, long_rate_hbm, short_rate_hbm, long_freq_hbm, short_freq_hbm,
                skip_hbm, gain_hbm, resid_hbm, lead_hbm, long_hbm, short_hbm, emit_hbm, up_hbm, down_hbm,
                out_ref, x_ref, dt_ref, lf_ref, long_rate, short_rate, long_freq, short_freq,
                skip_ref, gain_ref, resid_ref, lead_ref, in_sem, lin_l, lin_s, lin_sem,
                pace, surge, pre, st, blk, ends, ends_all, cin, mg, rows_in, mrg, emit, resid_in,
                mid_out, wup, wdn, nrm, hid, loc, a_out, a_in, b_out, b_in, c_out, c_in, home_in,
                copy_sem, own_sem, s_ends, r_ends, s_rows, r_rows, s_res, r_res,
                s_z, r_z, s_x, r_x, s_d, r_d_up, r_d_down, s_t, r_t, s_y, r_y,
                s_a, r_a, s_b, r_b, s_c, r_c, s_last, s_home, r_home,
                o_out, s_own, r_own, r_tz, r_tx, r_td, r_ta):
    nsp, ntp, n, S, W, G, PL, PS, D, Fz = cfg
    Z, X, Y = mesh_split(nsp, ntp)
    L = n // SUB
    half = G // 2
    SL = half * PL
    sp = lax.axis_index("sp")
    tp = lax.axis_index("tp")
    q = n // ntp
    Dl = D // ntp
    Dh = D // nsp // 2
    Rh = D // nsp // 2
    MESH = pl.DeviceIdType.MESH
    z, x, y, c = sp // X, lax.rem(sp, X), tp // 2, lax.rem(tp, 2)
    side = z // 2
    half_in, half_out = 1 + side, 3 * side
    far_in, far_out = 2 - side, 3 - 3 * side
    far0 = 2 - 2 * side
    mate = z + 1 - 2 * lax.rem(z, 2)
    inner, outer = z == half_in, z == half_out
    kinds = (z, mate, far_in, far_out)
    as_seen = 2 + jnp.where(outer, 1, 0)

    def dev(z_, x_, y_, c_):
        return (z_ * X + x_, y_ * 2 + c_)

    x_mate, y_mate, c_mate = dev(z, 1 - x, y, c), dev(z, x, 1 - y, c), dev(z, x, y, 1 - c)

    def remote(src, dst, ssem, rsem, to):
        return pltpu.make_async_remote_copy(src_ref=src, dst_ref=dst, send_sem=ssem, recv_sem=rsem,
                                            device_id=to, device_id_type=MESH)

    in_copies = [pltpu.make_async_copy(src, dst, in_sem.at[at]) for at, (src, dst) in enumerate((
        (dt_hbm, dt_ref), (lf_hbm, lf_ref), (x_hbm, x_ref), (long_rate_hbm, long_rate), (short_rate_hbm, short_rate),
        (long_freq_hbm, long_freq), (short_freq_hbm, short_freq), (skip_hbm, skip_ref), (gain_hbm, gain_ref),
        (lead_hbm, lead_ref), (resid_hbm.at[pl.ds(pl.multiple_of(tp * q, q), q), :], resid_ref)))]
    emit_copy = pltpu.make_async_copy(emit_hbm, emit, copy_sem.at[0])
    lin_copies = []
    for at in range(8):
        for kind, (src, dst) in enumerate(((long_hbm, lin_l), (short_hbm, lin_s))):
            lin_copies.append(pltpu.make_async_copy(
                src.at[at // 4, at // 2 % 2, at % 2, pl.ds(tp * half, half)], dst.at[at], lin_sem.at[kind]))

    def sent(ref, sem):
        remote(ref, ref, sem, sem, c_mate).wait_send()

    def came(ref, sem):
        remote(ref, ref, sem, sem, c_mate).wait_recv()

    def bank(up):
        return wup if up else wdn

    def shard(up, h, to):
        part = pl.ds(pl.multiple_of(to * Fz, 128), Fz)
        if up:
            return up_hbm.at[pl.ds(h * Rh, Rh), part]
        return down_hbm.at[part, pl.ds(h * Dh, Dh)]

    def own_copy(up, h):
        return pltpu.make_async_copy(shard(up, h, z), bank(up).at[c, sp, h], own_sem.at[1 - up])

    def own_wait(up):
        pltpu.make_async_copy(bank(up).at[c, sp], bank(up).at[c, sp], own_sem.at[1 - up]).wait()

    def z_copy(up, h, k):
        to = kinds[k]
        return remote(shard(up, h, to), bank(up).at[c, sp, h], s_z.at[0],
                      r_z.at[1 - up, h, 0 if k == 1 else as_seen - 1], dev(to, x, y, c))

    def x_copy(up, h, k):
        piece = bank(up).at[c, kinds[k] * X + x, h]
        return remote(shard(up, h, z) if k == 0 else piece, piece, s_x.at[0], r_x.at[1 - up, h, k], x_mate)

    def d_copy(up, h, k, other):
        piece = bank(up).at[c, kinds[k] * X + (1 - x if other else x), h]
        return remote(shard(up, h, z) if k == 0 and not other else piece, piece, s_d.at[0],
                      r_d_up.at[0] if up else r_d_down.at[0 if k < 2 else 1 + (k - 2) * 2 + h], c_mate)

    def hop1(up, h, k):
        came(bank(up).at[c, kinds[k] * X + x, h], r_z.at[1 - up, h, k - 1])
        x_copy(up, h, k).start()
        d_copy(up, h, k, 0).start()

    def tail_rows(part):
        return pl.ds(part * (Fz // PARTS), Fz // PARTS)

    def tail_send(part, k):
        to = kinds[k]
        src = down_hbm.at[pl.ds(pl.multiple_of(to * Fz + part * (Fz // PARTS), 16), Fz // PARTS), pl.ds(Dh, Dh)]
        return remote(src, wdn.at[c, sp, 1, tail_rows(part)], s_z.at[0], r_tz.at[part], dev(to, x, y, c))

    def tail_x(part):
        piece = wdn.at[c, far_in * X + x, 1, tail_rows(part)]
        return remote(piece, piece, s_x.at[0], r_tx.at[part], x_mate)

    def tail_d(part, other):
        piece = wdn.at[c, far_in * X + (1 - x if other else x), 1, tail_rows(part)]
        return remote(piece, piece, s_d.at[0], r_td.at[other], c_mate)

    def tail1(part):
        came(wdn.at[c, far_in * X + x, 1, tail_rows(part)], r_tz.at[part])
        tail_x(part).start()
        tail_d(part, 0).start()

    def tail2(part):
        tail_x(part).wait_recv()
        tail_d(part, 1).start()

    def tail3(other):
        came(wdn.at[1 - c, far_in * X + (1 - x if other else x), 1], r_td.at[other])

    def hop2(up, h, k):
        x_copy(up, h, k).wait_recv()
        d_copy(up, h, k, 1).start()

    def hop3_up():
        came(wup.at[1 - c], r_d_up.at[0])

    def hop3_near():
        came(wdn.at[1 - c, pl.ds(side * 2 * X, 2 * X)], r_d_down.at[0])

    def hop3_far(h, k):
        came(wdn.at[1 - c, kinds[k] * X], r_d_down.at[1 + (k - 2) * 2 + h])

    def res_copy(k):
        to = lax.rem(tp + k, ntp)
        return remote(resid_hbm.at[pl.ds(pl.multiple_of(to * q, q), q), :], resid_in.at[k - 1], s_res.at[0],
                      r_res.at[0], (sp, to))

    barrier = pltpu.get_barrier_semaphore()
    for k in range(1, nsp):
        pl.semaphore_signal(barrier, inc=1, device_id=(lax.rem(sp + k, nsp), tp), device_id_type=MESH)
    for k in range(1, ntp):
        pl.semaphore_signal(barrier, inc=1, device_id=(sp, lax.rem(tp + k, ntp)), device_id_type=MESH)
    for copy in in_copies + lin_copies:
        copy.start()

    pl.semaphore_wait(barrier, nsp + ntp - 2)

    @pl.when(outer)
    def _():
        for k in (2, 3):
            z_copy(1, 0, k).start()

    @pl.when(inner)
    def _():
        z_copy(1, 0, 1).start()

    for h in range(2):
        x_copy(1, h, 0).start()
        d_copy(1, h, 0, 0).start()
    for k in range(1, ntp):
        res_copy(k).start()
    emit_copy.start()
    for up in (1, 0):
        for h in range(2):
            own_copy(up, h).start()

    lane = lax.broadcasted_iota(jnp.int32, (G, S), 1)
    group = jnp.where(lane < SL, 2 * (lane // PL), 2 * ((lane - SL) // PS) + 1)
    spread = (group == lax.broadcasted_iota(jnp.int32, (G, S), 0)).astype(BF16)
    r = lax.broadcasted_iota(jnp.int32, (n, n), 0)
    t = lax.broadcasted_iota(jnp.int32, (n, n), 1)
    mix = (t == (r % SUB) * L + r // SUB).astype(BF16)

    spread = jnp.concatenate([spread] * 3, axis=0)

    for copy in in_copies[:2]:
        copy.wait()
    moved = lax.dot_general(jnp.concatenate([thirds(dt_ref[...]), thirds(lf_ref[...])], axis=0), mix,
                            (((1,), (1,)), ((), ())), preferred_element_type=F32).astype(BF16)
    pace[...], surge[...] = (
        lax.dot_general(moved[3 * G * at : 3 * G * (at + 1)], spread, (((0,), (0,)), ((), ())),
                        preferred_element_type=F32) for at in range(2))
    def flat_kind(ref, e):
        states = ref.shape[2]
        width = half * states
        repeat = (lax.broadcasted_iota(jnp.int32, (states, width), 1) % states
                  == lax.broadcasted_iota(jnp.int32, (states, width), 0)).astype(BF16)
        own_rows = ref[e, pl.ds(pl.multiple_of(tp * half, half), half), :]
        wide = jnp.dot(thirds(own_rows), repeat, preferred_element_type=F32)
        mine = (lax.broadcasted_iota(jnp.int32, (3 * half, width), 0) % half
                == lax.broadcasted_iota(jnp.int32, (3 * half, width), 1) // states)
        return jnp.sum(jnp.where(mine, wide, 0.0), axis=0, keepdims=True)

    def flat(long_ref, short_ref, e):
        return jnp.concatenate([flat_kind(long_ref, e), flat_kind(short_ref, e)], axis=1)

    def widened(ref, index, states, sign):
        rows, width = half * CHAN, half * states
        repeat = (lax.broadcasted_iota(jnp.int32, (states, width), 1) % states
                  == lax.broadcasted_iota(jnp.int32, (states, width), 0)).astype(BF16)
        wide = jnp.dot(ref[index].reshape(rows, states).astype(BF16), repeat, preferred_element_type=F32)
        own_block = (lax.broadcasted_iota(jnp.int32, (rows, width), 0) // CHAN
                     == lax.broadcasted_iota(jnp.int32, (rows, width), 1) // states)
        return jnp.where(own_block, sign * wide, 0.0).astype(BF16)

    def block_map(index, sign=1.0):
        long_part = widened(lin_l, index, PL, sign)
        short_part = widened(lin_s, index, PS, sign)
        no_long, no_short = jnp.zeros((CHAN, SL), BF16), jnp.zeros((CHAN, S - SL), BF16)
        bands = []
        for g in range(half):
            band = slice(g * CHAN, (g + 1) * CHAN)
            bands.append(jnp.concatenate([long_part[band], no_short], axis=1))
            bands.append(jnp.concatenate([no_long, short_part[band]], axis=1))
        return jnp.concatenate(bands, axis=0)

    for copy in in_copies[2:]:
        copy.wait()
    xv = jnp.dot(mix, x_ref[...], preferred_element_type=F32).astype(BF16)
    for kind, ref in enumerate((lin_l, lin_s)):
        pltpu.make_async_copy(ref, ref, lin_sem.at[kind]).wait()
    for e in range(2):
        for part in range(2):
            st[:, pl.ds((2 * e + part) * S, S)] = jnp.dot(
                xv, block_map(4 * e + part), preferred_element_type=F32)

    for e in range(2):
        rate = flat(long_rate, short_rate, e)
        freq = flat(long_freq, short_freq, e)

        def step(i, carry):
            pr, pi, sr, si = carry
            at = i if e == 0 else L - 1 - i
            rows = pl.ds(pl.multiple_of(at * SUB, SUB), SUB)
            d = pace[rows, :]
            rd = rate * d
            m = jnp.exp(surge[rows, :] - rd)
            cos_v, sin_v = sincos(freq * d)
            w = jnp.sqrt(one_minus_exp_neg(2.0 * rd))
            ar, ai = m * cos_v, m * sin_v
            pr, pi = cmul(ar, ai, pr, pi)
            sr, si = cmul(ar, ai, sr, si)
            sr = sr + w * st[rows, pl.ds(2 * e * S, S)]
            si = si + w * st[rows, pl.ds((2 * e + 1) * S, S)]
            pre[rows, pl.ds(2 * e * S, S)] = pr
            pre[rows, pl.ds((2 * e + 1) * S, S)] = pi
            st[rows, pl.ds(2 * e * S, S)] = sr
            st[rows, pl.ds((2 * e + 1) * S, S)] = si
            return pr, pi, sr, si

        zero = jnp.zeros((SUB, S), F32)
        total = lax.fori_loop(0, L, step, (zero + 1.0, zero, zero, zero))
        for part in range(4):
            blk[4 * e + part] = total[part]
        order = range(SUB) if e == 0 else range(SUB - 1, -1, -1)
        run = None
        for b in order:
            now = tuple(blk[4 * e + part, b : b + 1, :] for part in range(4))
            if run is None:
                run = now
            else:
                p = cmul(now[0], now[1], run[0], run[1])
                s = cmul(now[0], now[1], run[2], run[3])
                run = (p[0], p[1], s[0] + now[2], s[1] + now[3])
        for part in range(4):
            ends[e, part : part + 1, :] = run[part]

    def ends_copy(e, k):
        return remote(ends.at[e], ends_all.at[e, k - 1], s_ends.at[0], r_ends.at[0],
                      (sp + k if e == 0 else sp - k, tp))

    def has_after(e, k):
        return sp + k < nsp if e == 0 else sp >= k

    def has_before(e, k):
        return has_after(1 - e, k)

    for k in range(1, nsp):
        for e in range(2):
            @pl.when(has_after(e, k))
            def _():
                ends_copy(e, k).start()

    @pl.when(inner)
    def _():
        for k in (2, 3):
            z_copy(1, 0, k).start()
        z_copy(1, 1, 1).start()

    @pl.when(outer)
    def _():
        for h in range(2):
            z_copy(1, h, 1).start()
        for k in (2, 3):
            z_copy(1, 1, k).start()
        hop1(1, 0, 1)

    read = jnp.concatenate(
        [block_map(2), block_map(3, -1.0), block_map(6), block_map(7, -1.0)], axis=1)

    came(ends_all.at[0], r_ends.at[0])
    blank = jnp.zeros((1, S), F32)

    def fold(j, carry, e):
        cr, ci = carry
        k = nsp - 1 - j
        got = ends_all[e, k - 1]
        nr, ni = cmul(got[0:1], got[1:2], cr, ci)
        reached = has_before(e, k)
        return jnp.where(reached, nr + got[2:3], cr), jnp.where(reached, ni + got[3:4], ci)

    for e in range(2):
        cr, ci = lax.fori_loop(0, nsp - 1, functools.partial(fold, e=e), (blank, blank))
        order = range(SUB) if e == 0 else range(SUB - 1, -1, -1)
        for b in order:
            cin[2 * e, b : b + 1, :] = cr
            cin[2 * e + 1, b : b + 1, :] = ci
            now = tuple(blk[4 * e + part, b : b + 1, :] for part in range(4))
            nr, ni = cmul(now[0], now[1], cr, ci)
            cr, ci = nr + now[2], ni + now[3]

        inr, ini = cin[2 * e], cin[2 * e + 1]

        def settle(i, _):
            rows = pl.ds(pl.multiple_of(i * SUB, SUB), SUB)
            re, im = pl.ds(2 * e * S, S), pl.ds((2 * e + 1) * S, S)
            ar, ai = cmul(pre[rows, re], pre[rows, im], inr, ini)
            st[rows, re] = st[rows, re] + ar
            st[rows, im] = st[rows, im] + ai
            return 0

        lax.fori_loop(0, L, settle, 0)

    v = lax.dot_general(st[...].astype(BF16), read, (((1,), (1,)), ((), ())),
                        preferred_element_type=F32)
    own = pl.ds(pl.multiple_of(tp * W, 128), W)
    skip_row, gain_row = skip_ref[:, own], gain_ref[:, own]
    v = v + skip_row * xv.astype(F32)
    v = 0.5 * v * (1.0 + jnp.tanh(0.7978845608028654 * (v + 0.044715 * v * v * v)))
    heads = []
    for h in range(W // NORM_W):
        head = v[:, h * NORM_W : (h + 1) * NORM_W]
        scale = lax.rsqrt(jnp.mean(head * head, axis=1, keepdims=True) + EPSILON)
        heads.append(head * scale * gain_row[:, h * NORM_W : (h + 1) * NORM_W])
    merged = jnp.concatenate(heads, axis=1).astype(BF16)
    t = lax.broadcasted_iota(jnp.int32, (n, n), 0)
    r = lax.broadcasted_iota(jnp.int32, (n, n), 1)
    unmix = (r == (t % L) * SUB + t // L).astype(BF16)
    mg[...] = jnp.dot(unmix, merged, preferred_element_type=F32).astype(BF16).reshape(ntp, q, W)

    def row_copy(k):
        to = lax.rem(tp + k, ntp)
        return remote(mg.at[to], rows_in.at[k - 1], s_rows.at[0], r_rows.at[0], (sp, to))

    for k in range(1, ntp):
        row_copy(k).start()

    @pl.when(inner)
    def _():
        for h in range(2):
            z_copy(0, h, 1).start()

    for h in range(2):
        hop2(1, h, 0)

    hop1(1, 0, 3)

    @pl.when(inner)
    def _():
        hop1(1, 0, 1)

    hop1(1, 1, 1)
    emit_copy.wait()
    mrg[:, pl.ds(pl.multiple_of(tp * W, 128), W)] = mg[tp]
    mid_out[:, pl.ds(pl.multiple_of(tp * Dl, 128), Dl)] = resid_ref[...].astype(F32)
    came(resid_in, r_res.at[0])
    came(rows_in, r_rows.at[0])
    for k in range(1, ntp):
        src = lax.rem(tp - k + ntp, ntp)
        mid_out[:, pl.ds(pl.multiple_of(src * Dl, 128), Dl)] = resid_in[k - 1].astype(F32)
        mrg[:, pl.ds(pl.multiple_of(src * W, 128), W)] = rows_in[k - 1]
    mid = mid_out[...] + jnp.dot(mrg[...], emit[...], preferred_element_type=F32)
    mid_out[...] = mid
    scale = lax.rsqrt(jnp.mean(mid * mid, axis=1, keepdims=True) + EPSILON)
    nrm[0, z] = (mid * scale * lead_ref[...]).astype(BF16)

    def t_far():
        return remote(nrm.at[0, z], nrm.at[0, z], s_t.at[0], r_t.at[as_seen - 1], dev(far_in, x, y, c))

    def t_mate(k):
        block = nrm.at[0, kinds[k]]
        return remote(block, block, s_t.at[0 if k == 0 else 1], r_t.at[max(k, 1) - 1], dev(mate, x, y, c))

    def t_wait(k):
        t_mate(k).wait_recv()

    def y_copy(k):
        return remote(nrm.at[0, kinds[k]], nrm.at[1, kinds[k]], s_y.at[0], r_y.at[0], y_mate)

    t_far().start()
    t_mate(0).start()
    y_copy(0).start()

    @pl.when(inner)
    def _():
        for k in (2, 3):
            z_copy(1, 1, k).start()

    @pl.when(outer)
    def _():
        for h in range(2):
            z_copy(0, h, 1).start()

    for h in range(2):
        x_copy(0, h, 0).start()
        d_copy(0, h, 0, 0).start()

    hop2(1, 0, 3)
    hop1(1, 1, 3)
    hop2(1, 0, 1)
    hop1(1, 0, 2)
    t_wait(1)
    y_copy(1).start()

    @pl.when(inner)
    def _():
        for k in (3, 2):
            t_wait(k)
            t_mate(k).start()
            y_copy(k).start()

    hop2(1, 1, 1)
    hop2(1, 1, 3)
    hop2(1, 0, 2)

    hop1(1, 1, 2)

    @pl.when(inner)
    def _():
        for k in (2, 3):
            z_copy(0, 0, k).start()

    @pl.when(outer)
    def _():
        z_copy(0, 0, 2).start()
        for k in (3, 2):
            t_wait(k)
            y_copy(k).start()
        z_copy(0, 0, 3).start()
        for k in (2, 3):
            z_copy(0, 1, k).start()

    for h in range(2):
        hop1(0, h, 1)
    for h in range(2):
        hop2(0, h, 0)
    hop2(1, 1, 2)
    came(nrm.at[1], r_y.at[0])
    own_wait(1)
    hop3_up()
    rows = nrm[...].reshape(2 * Z * q, D)
    for b in range(2):
        upward = jnp.dot(rows, wup[b].reshape(D, Fz), preferred_element_type=F32)
        hid[b] = jnp.square(jnp.maximum(upward, 0.0)).astype(BF16)

    def cols(zs, x_, h):
        return pl.ds(pl.multiple_of((zs * X + x_) * 2 * Dh + h * Dh, 128), Dh)

    def a_copy(zs, h):
        g = zs * 2 + h
        return remote(a_out.at[g], a_in.at[g], s_a.at[0], r_a.at[g], y_mate)

    def b_copy(zs, h):
        g = zs * 2 + h
        return remote(b_out.at[g, mate], b_in.at[g, mate], s_b.at[0], r_b.at[0, g], dev(mate, x, y, c))

    def b_far(zs, h):
        g = zs * 2 + h
        blocks = pl.ds(far0, 2)
        return remote(b_out.at[g, blocks], b_in.at[g, blocks], s_b.at[1], r_b.at[1, g], dev(mate, x, y, c))

    def c_copy(zs, h, i):
        g = zs * 2 + h
        return remote(c_out.at[g, i], c_in.at[tp, h], s_c.at[0], r_c.at[0], ((far0 + i) * X + x, zs))

    def stage_a(zs, h):
        g = zs * 2 + h
        for x_ in range(X):
            total = jnp.dot(hid[0], wdn[0, zs * X + x_, h], preferred_element_type=F32)
            total = total + jnp.dot(hid[1], wdn[1, zs * X + x_, h], preferred_element_type=F32)
            total = total.reshape(2, Z, q, Dh)
            a_out[g, :, x_] = total[1].astype(BF16)
            loc[g, :, x_] = total[0]
        a_copy(zs, h).start()

    def stage_b(zs, h):
        g = zs * 2 + h
        a_copy(zs, h).wait_recv()
        total = loc[g] + a_in[g].astype(F32)
        loc[g] = total
        b_out[g] = total.astype(BF16)

        @pl.when(outer)
        def _():
            b_far(zs, h).start()

        b_copy(zs, h).start()

    def keep(zs, src, dst):
        @pl.when(zs == tp)
        def _():
            dst[...] = src[...]

        @pl.when(zs != tp)
        def _():
            remote(src, dst, s_own.at[0], r_own.at[0], (sp, zs)).start()

    def stage_c(zs, h):
        g = zs * 2 + h

        @pl.when(inner)
        def _():
            b_far(zs, h).wait_recv()
            blocks = pl.ds(far0, 2)
            c_out[g] = (loc[g, blocks] + b_in[g, blocks].astype(F32)).astype(BF16)
            for i in range(2):
                c_copy(zs, h, i).start()

        b_copy(zs, h).wait_recv()
        o_out[g] = (loc[g, z] + b_in[g, z].astype(F32)).astype(BF16)
        keep(zs, o_out.at[g], c_in.at[tp, 3 + h])

    last = far_in * 2 + 1

    def tail_copy(xd, other):
        return remote(a_out.at[last, :, xd], a_in.at[last, :, xd], s_a.at[0], r_ta.at[other], y_mate)

    def tail_a(other):
        xd = 1 - x if other else x
        total = jnp.dot(hid[0], wdn[0, far_in * X + xd, 1], preferred_element_type=F32)
        total = total + jnp.dot(hid[1], wdn[1, far_in * X + xd, 1], preferred_element_type=F32)
        total = total.reshape(2, Z, q, Dh)
        a_out[last, :, xd] = total[1].astype(BF16)
        loc[last, :, xd] = total[0]
        tail_copy(xd, other).start()

    def tail_sums(other):
        xd = 1 - x if other else x
        tail_copy(xd, other).wait_recv()
        b_out[last, :, xd] = (loc[last, :, xd] + a_in[last, :, xd].astype(F32)).astype(BF16)
        for i in range(2):
            to = far0 + i
            remote(b_out.at[last, to, xd], c_in.at[tp, as_seen - 1, xd], s_last.at[0], r_c.at[as_seen - 2],
                   (to * X + x, far_in)).start()
        remote(b_out.at[last, mate, xd], c_in.at[tp, 2, xd], s_last.at[0], r_c.at[1], (mate * X + x, far_in)).start()
        keep(far_in, b_out.at[last, z, xd], c_in.at[tp, 4, xd])

    def home_copy(zs):
        return remote(mid_out.at[:, pl.ds(pl.multiple_of(zs * Dl, 128), Dl)], home_in.at[tp], s_home.at[0],
                      r_home.at[0], (sp, zs))

    turns = [(zs, h) for zs in (half_in, half_out, far_out, far_in) for h in range(2)]
    hop1(0, 0, 3)

    @pl.when(inner)
    def _():
        for part in range(PARTS):
            for k in (2, 3):
                tail_send(part, k).start()

    for zs in range(Z):
        @pl.when(zs == tp)
        def _():
            home_in[tp] = mid_out[:, zs * Dl : (zs + 1) * Dl]

        @pl.when(zs != tp)
        def _():
            home_copy(zs).start()

    own_wait(0)
    for h in range(2):
        hop2(0, h, 1)
    hop3_near()
    stage_a(*turns[0])
    stage_a(*turns[1])
    stage_a(*turns[2])
    stage_a(*turns[3])
    hop1(0, 1, 3)
    stage_b(*turns[0])
    hop2(0, 0, 3)
    stage_b(*turns[1])
    hop1(0, 0, 2)
    hop3_far(0, 3)
    stage_a(*turns[4])
    stage_b(*turns[2])
    hop2(0, 1, 3)
    tail1(0)
    stage_b(*turns[3])
    tail1(1)
    hop3_far(1, 3)
    stage_a(*turns[5])
    stage_b(*turns[4])
    hop2(0, 0, 2)
    tail1(2)
    stage_c(*turns[0])
    tail1(3)
    hop3_far(0, 2)
    stage_a(*turns[6])
    tail2(0)
    stage_c(*turns[1])
    stage_c(*turns[2])
    tail2(1)
    tail3(0)
    tail_a(0)
    stage_c(*turns[3])
    tail2(2)
    stage_b(*turns[5])
    tail2(3)
    tail3(1)
    tail_a(1)
    stage_b(*turns[6])
    tail_sums(0)
    stage_c(*turns[4])
    stage_c(*turns[5])
    tail_sums(1)
    stage_c(*turns[6])
    came(home_in.at[pl.ds(0, ntp - 1)], r_home.at[0])
    came(c_in.at[pl.ds(0, ntp - 1), pl.ds(3, 2)], r_own.at[0])
    came(c_in.at[:, pl.ds(0, 2)], r_c.at[0])

    @pl.when((tp == half_in) | (tp == far_in))
    def _():
        came(c_in.at[:, 2], r_c.at[1])
        for x_ in range(X):
            at = pl.ds((2 * x_ + 1) * Dh, Dh)
            home_in[:, :, at] = home_in[:, :, at] + c_in[:, 2, x_].astype(F32)

    for src in range(ntp):
        for x_ in range(X):
            for h in range(2):
                at = pl.ds((2 * x_ + h) * Dh, Dh)
                total = home_in[src, :, at] + c_in[src, h, x_].astype(F32) + c_in[src, 3 + h, x_].astype(F32)
                out_ref[pl.ds(src * q, q), at] = total.astype(BF16)

    sent(wup.at[0, pl.ds(0, 6)], s_z.at[0])
    sent(wup.at[0], s_x.at[0])
    sent(wup, s_d.at[0])
    sent(ends_all.at[0], s_ends.at[0])
    sent(nrm.at[0, pl.ds(0, 2)], s_t.at[0])
    sent(nrm.at[0], s_y.at[0])
    sent(a_out, s_a.at[0])
    sent(b_out.at[pl.ds(0, 2 * Z - 1), 0], s_b.at[0])
    sent(b_out.at[0, pl.ds(0, 3)], s_last.at[0])
    sent(c_in.at[pl.ds(0, ntp - 1), pl.ds(3, 2)], s_own.at[0])
    sent(home_in.at[pl.ds(0, ntp - 1)], s_home.at[0])
    sent(resid_in, s_res.at[0])
    sent(rows_in, s_rows.at[0])

    @pl.when(inner)
    def _():
        sent(nrm.at[0, pl.ds(0, 2)], s_t.at[1])
        sent(c_out.at[pl.ds(0, 2 * Z - 1)], s_c.at[0])

    @pl.when(outer)
    def _():
        sent(b_out.at[pl.ds(0, 2 * Z - 1), pl.ds(0, 2)], s_b.at[1])


def paired_call(nsp, ntp, residual, lifted, dts, long_rate, short_rate, emitted, raising):
    n, W = lifted.shape
    G = dts.shape[0]
    half = G // 2
    PL, PS = long_rate.shape[2], short_rate.shape[2]
    S = half * (PL + PS)
    D = emitted.shape[1]
    Dl = residual.shape[1]
    q = n // ntp
    Z, X, Y = mesh_split(nsp, ntp)
    Fz = raising.shape[1] // Z
    Dh = D // nsp // 2
    groups = 2 * Z
    cfg = (nsp, ntp, n, S, W, G, PL, PS, D, Fz)
    vm = pl.BlockSpec(memory_space=pltpu.VMEM)
    dma = pltpu.SemaphoreType.DMA
    return pl.pallas_call(
        functools.partial(paired_body, cfg),
        out_shape=jax.ShapeDtypeStruct((n, Dl), BF16),
        in_specs=[pl.BlockSpec(memory_space=pl.ANY)] * 16,
        out_specs=vm,
        scratch_shapes=[
            pltpu.VMEM(lifted.shape, BF16), pltpu.VMEM(dts.shape, F32), pltpu.VMEM(dts.shape, F32),
            *[pltpu.VMEM(long_rate.shape, F32), pltpu.VMEM(short_rate.shape, F32)] * 2,
            pltpu.VMEM((1, ntp * W), F32), pltpu.VMEM((1, ntp * W), F32), pltpu.VMEM((q, Dl), BF16),
            pltpu.VMEM((1, D), F32), dma((11,)),
            pltpu.VMEM((8, half, CHAN, PL), F32), pltpu.VMEM((8, half, CHAN, PS), F32), dma((2,)),
            pltpu.VMEM((n, S), F32), pltpu.VMEM((n, S), F32),
            pltpu.VMEM((n, 4 * S), F32), pltpu.VMEM((n, 4 * S), F32),
            pltpu.VMEM((8, SUB, S), F32), pltpu.VMEM((2, 4, S), F32), pltpu.VMEM((2, nsp - 1, 4, S), F32),
            pltpu.VMEM((4, SUB, S), F32),
            pltpu.VMEM((ntp, q, W), BF16), pltpu.VMEM((ntp - 1, q, W), BF16),
            pltpu.VMEM((q, ntp * W), BF16), pltpu.VMEM(emitted.shape, BF16),
            pltpu.VMEM((ntp - 1, q, Dl), BF16),
            pltpu.VMEM((q, D), F32),
            pltpu.VMEM((2, nsp, 2, D // nsp // 2, Fz), BF16), pltpu.VMEM((2, nsp, 2, Fz, Dh), BF16),
            pltpu.VMEM((2, Z, q, D), BF16), pltpu.VMEM((2, 2 * Z * q, Fz), BF16),
            pltpu.VMEM((groups, Z, X, q, Dh), F32),
            *[pltpu.VMEM((groups, Z, X, q, Dh), BF16)] * 4,
            pltpu.VMEM((groups, 2, X, q, Dh), BF16), pltpu.VMEM((ntp, 5, X, q, Dh), BF16),
            pltpu.VMEM((ntp, q, Dl), F32),
            dma((1,)), dma((2,)), *[dma((1,))] * 6,
            dma((1,)), dma((2, 2, 3)), dma((1,)), dma((2, 2, 4)), dma((1,)), dma((1,)), dma((5,)),
            dma((2,)), dma((3,)), dma((1,)), dma((1,)),
            dma((1,)), dma((groups,)), dma((2,)), dma((2, groups)), dma((1,)), dma((2,)), *[dma((1,))] * 3,
            pltpu.VMEM((groups, X, q, Dh), BF16), dma((1,)), dma((1,)), dma((PARTS,)), dma((PARTS,)), dma((2,)), dma((2,)),
        ],
        compiler_params=pltpu.CompilerParams(collective_id=0, has_side_effects=True),
        cost_estimate=pl.CostEstimate(flops=10**9, bytes_accessed=3 * 10**7, transcendentals=10**6),
    )


def on_device(residual, lifted, dts, fades, long_rate, short_rate, long_freq, short_freq,
              long_lin, short_lin, skip, closing, emitted, leading, raising, lowering):
    nsp, ntp = lax.axis_size("sp"), lax.axis_size("tp")
    operands = (lifted, dts, fades, long_rate, short_rate, long_freq, short_freq, skip[None], closing[None],
                residual, leading[None], long_lin.swapaxes(4, 5), short_lin.swapaxes(4, 5), emitted, raising, lowering)
    Z, X, Y = mesh_split(nsp, ntp)
    if X == 2 and Y == 2 and Z == ntp:
        return paired_call(nsp, ntp, residual, lifted, dts, long_rate, short_rate, emitted, raising)(*operands)
    n, W = lifted.shape
    G = dts.shape[0]
    half = G // 2
    PL, PS = long_rate.shape[2], short_rate.shape[2]
    S = half * (PL + PS)
    D = emitted.shape[1]
    Dl = residual.shape[1]
    q = n // ntp
    c_ff = min(nsp, raising.shape[1] // 128)
    F = raising.shape[1] // c_ff
    q_all, M = c_ff * q, ntp // 2
    cfg = (nsp, ntp, n, S, W, G, PL, PS, D, c_ff, F)
    vm = pl.BlockSpec(memory_space=pltpu.VMEM)
    dma = pltpu.SemaphoreType.DMA
    return pl.pallas_call(
        functools.partial(mixer_body, cfg),
        out_shape=jax.ShapeDtypeStruct((n, Dl), BF16),
        in_specs=[vm] * 11 + [pl.BlockSpec(memory_space=pl.ANY)] * 5,
        out_specs=vm,
        scratch_shapes=[
            pltpu.VMEM((8, half, CHAN, PL), F32), pltpu.VMEM((8, half, CHAN, PS), F32), dma((2, 8)),
            pltpu.VMEM((n, S), F32), pltpu.VMEM((n, S), F32),
            pltpu.VMEM((n, 4 * S), F32), pltpu.VMEM((n, 4 * S), F32),
            pltpu.VMEM((8, SUB, S), F32), pltpu.VMEM((8, S), F32), pltpu.VMEM((nsp - 1, 8, S), F32),
            pltpu.VMEM((4, SUB, S), F32),
            pltpu.VMEM((ntp, q, W), BF16), pltpu.VMEM((ntp - 1, q, W), BF16),
            pltpu.VMEM((q, ntp * W), BF16), pltpu.VMEM(emitted.shape, BF16),
            pltpu.VMEM((ntp - 1, q, Dl), BF16),
            pltpu.VMEM((q, D), F32),
            pltpu.VMEM((ntp, nsp, D // nsp, F), BF16), pltpu.VMEM((ntp, nsp, F, D // nsp), BF16),
            pltpu.VMEM((c_ff, q, D), BF16), pltpu.VMEM((ntp, q_all, F), BF16),
            pltpu.VMEM((c_ff, q, D), BF16), pltpu.VMEM((c_ff - 1, q, D), BF16),
            pltpu.VMEM((ntp, q, Dl), BF16), pltpu.VMEM((ntp - 1, q, Dl), BF16),
            dma((3,)), dma((nsp - 1,)), dma((nsp - 1,)), dma((ntp - 1,)), dma((ntp - 1,)),
            dma((ntp - 1,)), dma((ntp - 1,)),
            *[dma((nsp - 1,))] * 4, *[dma((M - 1, nsp))] * 4, *[dma((M,))] * 4,
            *[dma((2, c_ff // 2))] * 2, *[dma((c_ff - 1,))] * 2, *[dma((ntp - 1,))] * 2,
        ],
        compiler_params=pltpu.CompilerParams(collective_id=0, has_side_effects=True),
        cost_estimate=pl.CostEstimate(flops=10**9, bytes_accessed=3 * 10**7, transcendentals=10**6),
    )(*operands)


def solution(mesh):
    both, swapped = P("sp", "tp"), P("tp", "sp")
    in_specs = (both, both, swapped, swapped) + (P(),) * 10 + (both, swapped)
    return jax.shard_map(on_device, mesh=mesh, in_specs=in_specs, out_specs=both, check_vma=False)
```
